32 devices in a mesh: grp: 2 (over y), sp: 4 (over z), tp: 4 (over x, core).
Axes of the slice: x: 2, y: 2, z: 4, core: 2. Of those that a mesh axis runs over, the one named last changes fastest.
Arguments:
- resid_in: bfloat16 [2048, 2048], P(('grp', 'sp', 'tp')), parts along dimension 0, may hold values from -3 to 3
- queries: bfloat16 [2048, 1024], P(('grp', 'sp'), 'tp'), parts along dimension 0, may hold values from -39 to 39
- keys: bfloat16 [2048, 1024], P(('grp', 'sp'), 'tp'), parts along dimension 0, may hold values from -6 to 6
- values: bfloat16 [2048, 1024], P(('grp', 'sp'), 'tp'), parts along dimension 0, may hold values from -12 to 12
- cum_gate: float32 [2048, 16], P('grp', 'tp'), parts along dimension 0, may hold values from -105 to 0, as said below
- w_out: bfloat16 [1024, 2048], replicated, may hold values from -0.1875 to 0.1875
- norm_gain: float32 [2048], replicated, may hold values from 0.1 to 1.9
- w_gate: bfloat16 [2048, 5632], P('sp', 'tp'), may hold values from -0.125 to 0.125
- w_up: bfloat16 [2048, 5632], P('sp', 'tp'), may hold values from -0.125 to 0.125
- w_down: bfloat16 [5632, 2048], P('tp', 'sp'), may hold values from -0.078125 to 0.078125
Outputs:
- resid_out: bfloat16 [2048, 2048], P(('grp', 'sp', 'tp')), parts along dimension 0
The draws below stay inside these ranges and needn't reach their ends.
There are 2 independent parts, one for each index of `grp`. The reference program is written for one: setup_inputs(seed, part) draws one part's arguments, and reference() takes and returns one part's arrays. A program takes and returns all parts, laid end to end along the dimension named above; an argument that names none is the same for every part. Nothing has to cross between parts.
Inputs may be any that keep to these rules, and one draw needn't show every extreme that they name: `cum_gate`: in every head the values never rise from one position to the next, and the first is at most 0.
All inputs are finite; a program needn't handle non-finite values.
Results may differ from the reference program's by a relative error of at most 0.018.
Values may be sent and summed in bfloat16 or wider, within the bound.
A program may use at most 128 MiB of HBM per device.

```python
import math
import jax
import jax.numpy as jnp
from jax import lax

D = 2048
HEADS = 16
HEAD_DIM = 64
FF = 5632
TOK_DEV = 256
SEQUENCE_TOKENS = 1024
ATT_WIDTH = 1024


def attention_pair(key):
    key_q, key_k = jax.random.split(key, 2)
    width = HEADS * HEAD_DIM
    queries = 2.0 * jnp.clip(jax.random.normal(key_q, (SEQUENCE_TOKENS, width), jnp.float32), -6.0, 6.0)
    keys = jnp.clip(jax.random.normal(key_k, (SEQUENCE_TOKENS, width), jnp.float32), -6.0, 6.0)
    return (queries, keys)


def draw_queries(key, part):
    return attention_pair(jax.random.fold_in(key, 11))[0].astype(jnp.bfloat16)


def draw_keys(key, part):
    return attention_pair(jax.random.fold_in(key, 11))[1].astype(jnp.bfloat16)


def draw_cum_gate(key, part):
    every_key_row = jax.random.split(jax.random.fold_in(key, 23), 6)
    sluggish_path = jax.random.permutation(every_key_row[0], HEADS) < HEADS // 2
    fast_rate = jnp.exp(jax.random.uniform(every_key_row[1], (HEADS,), jnp.float32, jnp.log(1.0 / 100.0), jnp.log(1.0 / 30.0)))
    rate = jnp.where(sluggish_path, 0.4 / SEQUENCE_TOKENS, fast_rate)
    factor = jnp.exp(jax.random.uniform(every_key_row[2], (SEQUENCE_TOKENS // TOK_DEV, 1), jnp.float32, jnp.log(0.5), jnp.log(2.0)))
    factor = jnp.repeat(factor, TOK_DEV, axis=0)
    rough = jax.random.uniform(every_key_row[3], (SEQUENCE_TOKENS, HEADS), jnp.float32, 0.5, 1.5)
    step_count = -rate[None, :] * factor * rough
    spike_position = jax.random.randint(every_key_row[4], (3,), 1, SEQUENCE_TOKENS, dtype=jnp.int32)
    training_loss = jax.random.uniform(every_key_row[5], (3, HEADS), jnp.float32, 0.2, 0.5)
    step_count = step_count.at[spike_position].add(jnp.log(1.0 - training_loss) * sluggish_path.astype(jnp.float32)[None, :])
    return jnp.cumsum(step_count, axis=0)


def levels(key, shape, cuts, low, top_value):
    factor_of, own = 1.0, jax.random.fold_in(key, 6)
    for position, shards_of in cuts:
        draws = jnp.exp(jax.random.uniform(jax.random.fold_in(own, position), (shards_of,), jnp.float32, low / len(cuts), top_value / len(cuts)))
        factor_of = factor_of * jnp.repeat(draws, shape[position] // shards_of).reshape([-1 if axis == position else 1 for axis in range(len(shape))])
    return factor_of


def scatter_about(key, shape, spread, reach, pieces=(), held_as=jnp.bfloat16):
    gain = levels(key, shape, pieces, -0.22, 0.18) if pieces else 1.0
    drawn = jax.random.normal(key, shape, jnp.float32) * spread * gain
    return jnp.minimum(jnp.maximum(drawn, -reach), reach).astype(held_as)


def setup_inputs(seed: int = 0, part: int = 0) -> dict:
    splits = jax.random.split(jax.random.key(seed), 11)
    part_splits = jax.random.split(jax.random.fold_in(splits[10], part), 11)
    return {
        "resid_in": scatter_about(part_splits[0], (SEQUENCE_TOKENS, D), 0.5, 3.0, ((0, 16),)),
        "queries": draw_queries(jax.random.fold_in(jax.random.fold_in(splits[10], part), 71), part),
        "keys": draw_keys(jax.random.fold_in(jax.random.fold_in(splits[10], part), 71), part),
        "values": scatter_about(part_splits[3], (SEQUENCE_TOKENS, ATT_WIDTH), 2.0, 12.0, ((0, 4), (1, 4))),
        "cum_gate": draw_cum_gate(jax.random.fold_in(jax.random.fold_in(splits[10], part), 71), part),
        "w_out": scatter_about(splits[5], (ATT_WIDTH, D), ATT_WIDTH ** -0.5, 0.1875),
        "norm_gain": jnp.clip(1.0 + 0.18 * jax.random.normal(splits[6], (D,), jnp.float32), 0.1, 1.9),
        "w_gate": scatter_about(splits[7], (D, FF), D ** -0.5, 0.125, ((0, 4), (1, 4))),
        "w_up": scatter_about(splits[8], (D, FF), D ** -0.5, 0.125, ((0, 4), (1, 4))),
        "w_down": scatter_about(splits[9], (FF, D), FF ** -0.5, 0.078125, ((0, 4), (1, 4))),
    }


def attention(queries, keys, values, cum_gate):
    total = queries.shape[0]
    span = math.gcd(total, 256)
    scale = HEAD_DIM ** (-0.5)
    query_heads = queries.astype(jnp.float32).reshape(total, HEADS, HEAD_DIM)
    key_heads = keys.astype(jnp.float32).reshape(total, HEADS, HEAD_DIM)
    value_heads = values.astype(jnp.float32).reshape(total, HEADS, HEAD_DIM)
    positions = jnp.arange(total, dtype=jnp.int32)

    def block(first):
        query_block = lax.dynamic_slice_in_dim(query_heads, first, span, 0)
        gate_block_rows = lax.dynamic_slice_in_dim(cum_gate, first, span, 0)
        scores = jnp.einsum('qhd,khd->hqk', query_block, key_heads) * scale
        scores = scores + gate_block_rows.T[:, :, None] - cum_gate.T[:, None, :]
        mask = positions[None, :] <= (first + jnp.arange(span, dtype=jnp.int32))[:, None]
        scores = jnp.where(mask[None], scores, -1e+30)
        top = lax.optimization_barrier(jnp.max(scores, axis=-1, keepdims=True))
        weights = jnp.where(mask[None], jnp.exp(scores - top), 0.0)
        totals = lax.optimization_barrier(jnp.sum(weights, axis=-1))
        rounded = lax.optimization_barrier(weights.astype(jnp.bfloat16)).astype(jnp.float32)
        attended = jnp.einsum('hqk,khd->qhd', rounded, value_heads) / totals.T[:, :, None]
        return attended.reshape(span, HEADS * HEAD_DIM).astype(jnp.bfloat16)
    starts = jnp.arange(total // span, dtype=jnp.int32) * span
    return lax.map(block, starts).reshape(total, HEADS * HEAD_DIM)

def reference(resid_in, queries, keys, values, cum_gate, w_out, norm_gain, w_gate, w_up, w_down):
    attended = attention(queries, keys, values, cum_gate)
    mixed = jnp.dot(attended, w_out, preferred_element_type=jnp.float32)
    resid = resid_in.astype(jnp.float32) + mixed
    normed = resid * lax.rsqrt(lax.optimization_barrier(jnp.mean(resid * resid, axis=-1, keepdims=True)) + 1e-06)
    normed = (normed * norm_gain).astype(jnp.bfloat16)
    gate = jnp.dot(normed, w_gate, preferred_element_type=jnp.float32)
    up = jnp.dot(normed, w_up, preferred_element_type=jnp.float32)
    hidden = (jax.nn.silu(gate) * up).astype(jnp.bfloat16)
    down = jnp.dot(hidden, w_down, preferred_element_type=jnp.float32)
    return (resid + down).astype(jnp.bfloat16)
```

```python
import functools
import math

import jax
import jax.numpy as jnp
from jax import lax
from jax.experimental import pallas as pl
from jax.experimental.pallas import tpu as pltpu
from jax.sharding import PartitionSpec as P

HEAD_DIM = 64


def on_device(resid_in, queries, keys, values, cum_gate, w_out, norm_gain, w_gate, w_up, w_down):
    tok_rows = queries.shape[0]
    local_heads = queries.shape[1] // HEAD_DIM
    scale = HEAD_DIM ** (-0.5)
    offset = lax.axis_index("sp") * tok_rows
    query_heads = queries.reshape(tok_rows, local_heads, HEAD_DIM)
    own_gate = lax.dynamic_slice_in_dim(cum_gate, offset, tok_rows, 0).T
    query_pos = offset + jnp.arange(tok_rows, dtype=jnp.int32)
    last_pos = offset + tok_rows - 1
    initial = (
        jnp.full((local_heads, tok_rows), -1e30, jnp.float32),
        jnp.zeros((local_heads, tok_rows), jnp.float32),
        jnp.zeros((tok_rows, local_heads, HEAD_DIM), jnp.float32),
    )
    pair = lax.all_gather(jnp.stack([keys, values]), "sp", axis=1, tiled=True)
    key_piece, value_piece = pair[0], pair[1]
    length = key_piece.shape[0]
    span = math.gcd(length, 512)

    def block(index, state):
        begin = index * span

        def work(inner):
            maxima, totals, summed = inner
            key_block = lax.dynamic_slice_in_dim(key_piece, index * span, span, 0).reshape(
                span, local_heads, HEAD_DIM
            )
            value_block_rows = lax.dynamic_slice_in_dim(value_piece, index * span, span, 0).reshape(
                span, local_heads, HEAD_DIM
            )
            key_gate = lax.dynamic_slice_in_dim(cum_gate, begin, span, 0).T
            scores = (
                jnp.einsum(
                    "qhd,khd->hqk", query_heads, key_block, preferred_element_type=jnp.float32
                )
                * scale
            )
            scores = scores + own_gate[:, :, None] - key_gate[:, None, :]
            key_pos = begin + jnp.arange(span, dtype=jnp.int32)
            mask = (key_pos[None, :] <= query_pos[:, None])[None]
            scores = jnp.where(mask, scores, -1e30)
            new_max = jnp.maximum(maxima, jnp.max(scores, axis=-1))
            weights = jnp.where(mask, jnp.exp(scores - new_max[:, :, None]), 0.0)
            rescale = jnp.exp(maxima - new_max)
            totals = totals * rescale + jnp.sum(weights, axis=-1)
            product = jnp.einsum(
                "hqk,khd->qhd",
                weights.astype(jnp.bfloat16),
                value_block_rows,
                preferred_element_type=jnp.float32,
            )
            summed = summed * rescale.T[:, :, None] + product
            return (new_max, totals, summed)

        return lax.cond(begin <= last_pos, work, lambda inner: inner, state)

    maxima, totals, summed = lax.fori_loop(0, length // span, block, initial)
    attended = (
        (summed / totals.T[:, :, None])
        .reshape(tok_rows, local_heads * HEAD_DIM)
        .astype(jnp.bfloat16)
    )
    head_rows = lax.all_to_all(attended, "tp", split_axis=0, concat_axis=1, tiled=True)
    mixed = jnp.dot(head_rows, w_out, preferred_element_type=jnp.float32)
    resid = resid_in.astype(jnp.float32) + mixed
    normed = resid * lax.rsqrt(jnp.mean(resid * resid, axis=-1, keepdims=True) + 1e-06)
    normed = (normed * norm_gain).astype(jnp.bfloat16)
    all_rows = lax.all_gather(normed, ("sp", "tp"), axis=0, tiled=True)
    full_gate, full_up, full_down = (
        lax.all_to_all(w_gate, "sp", split_axis=1, concat_axis=0, tiled=True),
        lax.all_to_all(w_up, "sp", split_axis=1, concat_axis=0, tiled=True),
        lax.all_to_all(w_down, "sp", split_axis=0, concat_axis=1, tiled=True),
    )
    gate = jnp.dot(all_rows, full_gate, preferred_element_type=jnp.float32)
    up = jnp.dot(all_rows, full_up, preferred_element_type=jnp.float32)
    hidden = (jax.nn.silu(gate) * up).astype(jnp.bfloat16)
    terms = jnp.dot(hidden, full_down, preferred_element_type=jnp.float32)
    back = lax.psum_scatter(
        terms.astype(jnp.bfloat16), ("sp", "tp"), scatter_dimension=0, tiled=True
    ).astype(jnp.float32)
    return (resid + back).astype(jnp.bfloat16)


MESH = pl.DeviceIdType.MESH
F32 = jnp.float32
BF16 = jnp.bfloat16
UNIT = 128
PIECES = 4


def layer_kernel(
    dims, resid_ref, q_ref, k_ref, v_ref, gate_t_ref, gain_ref, w_out_ref, w_gate_ref,
    w_up_ref, w_down_ref, out_ref, kbuf, vbuf, top, tot, acc, att, heads, w_out, resid, nall, wgu,
    wd, hidden, part, crecv, csend, keep, xrecv, zsend, zrecv, loc_sem, kv_send, kv_recv, wz_send,
    wz_recv, wy_send, wy_recv, dz_send, dz_recv, dy_send, dy_recv, h_send, h_recv, az_send, az_recv,
    ax_send, ax_recv, ac_send, ac_recv, rc_send, rc_recv, rx_send, rx_recv, rz_send, rz_recv,
):
    ns, nt, chunk, nj = dims
    g, s, t = lax.axis_index("grp"), lax.axis_index("sp"), lax.axis_index("tp")
    rows, width = resid_ref.shape
    tok, att_w = q_ref.shape
    depth, units = w_gate_ref.shape
    nheads = att_w // HEAD_DIM
    half_depth = depth // 2
    dup = ns * chunk - units
    nu, dj = chunk // UNIT, depth // nj
    wide = ns * dj
    x, c = t // 2, t % 2
    tx = (t + 2) % 4
    tc = t + 1 - 2 * c
    scale = HEAD_DIM ** (-0.5)
    sc = jax.named_scope

    def start_of(i):
        return min(i * chunk, units - chunk)

    def first_unit(i):
        return dup // UNIT if i == ns - 1 else 0

    def remote(src, dst, send, recv, **where):
        return pltpu.make_async_remote_copy(
            src_ref=src, dst_ref=dst, send_sem=send, recv_sem=recv, device_id=where,
            device_id_type=MESH,
        )

    def xor(a, b):
        hi, lo, bh, bl = a // 2, a % 2, b // 2, b % 2
        return 2 * (hi + bh - 2 * hi * bh) + lo + bl - 2 * lo * bl

    def on_each_s(body):
        for k in range(ns):
            pl.when(s == k)(lambda k=k: (body(k), None)[1])

    def each(low, high, body):
        lax.fori_loop(low, high, lambda i, z: (body(i), z)[1], 0)

    def unit_band(src, half):
        return pl.ds(pl.multiple_of(src * depth + half * half_depth, half_depth), half_depth)

    def unit_z(mat, u, me, dst):
        src = (w_gate_ref, w_up_ref)[mat].at[
            pl.ds(pl.multiple_of(g * half_depth, half_depth), half_depth),
            pl.ds(start_of(dst) + u * UNIT, UNIT),
        ]
        return remote(
            src, wgu.at[u, unit_band(me, g), pl.ds(mat * UNIT, UNIT)],
            wz_send.at[2 * u + mat, dst], wz_recv.at[2 * u + mat, me], sp=dst,
        )

    def unit_in(mat, u, src):
        block = wgu.at[u, unit_band(src, g), pl.ds(mat * UNIT, UNIT)]
        return remote(block, block, wz_send.at[2 * u + mat, src], wz_recv.at[2 * u + mat, src], sp=src)

    def unit_y(u, src, half):
        block = wgu.at[u, unit_band(src, half)]
        return remote(block, block, wy_send.at[u, src], wy_recv.at[u, src], grp=1 - g)

    def send_units(me, dst, us):
        for u in us:
            if u >= first_unit(dst):
                for mat in range(2):
                    unit_z(mat, u, me, dst).start()

    def pass_units(me, u, *srcs):
        if u >= first_unit(me):
            for src in srcs:
                for mat in range(2):
                    unit_in(mat, u, src).wait_recv()
                unit_y(u, src, g).start()

    def down_band(j, src, half, me):
        skip = first_unit(me) * UNIT
        size = (chunk - skip) // 2
        return wd.at[
            j, pl.ds(pl.multiple_of(skip + half * size, math.gcd(128, size)), size),
            pl.ds(src * dj, dj),
        ]

    def down_z(j, me, dst):
        skip = first_unit(dst) * UNIT
        size = (chunk - skip) // 2
        src = w_down_ref.at[
            pl.ds(pl.multiple_of(start_of(dst) + skip + g * size, math.gcd(128, size)), size),
            pl.ds(j * dj, dj),
        ]
        return remote(
            src, down_band(j, me, g, dst), dz_send.at[j, dst], dz_recv.at[j, me], sp=dst
        )

    def down_y(j, src, half, me):
        block = down_band(j, src, half, me)
        return remote(block, block, dy_send.at[j, src], dy_recv.at[j, src], grp=1 - g)

    def send_down(me, j, *dsts):
        for dst in dsts:
            down_z(j, me, dst).start()

    def pass_down(me, j, *srcs):
        for src in srcs:
            block = down_band(j, src, g, me)
            with sc(f"d{j}.{src}"):
                remote(block, block, dz_send.at[j, src], dz_recv.at[j, src], sp=src).wait_recv()
            down_y(j, src, g, me).start()

    barrier = pltpu.get_barrier_semaphore()

    def greet(i):
        pl.semaphore_signal(barrier, inc=1, device_id={"sp": i}, device_id_type=MESH)

    each(0, s, greet)
    each(s + 1, ns, greet)
    pl.semaphore_signal(barrier, inc=1, device_id={"grp": 1 - g}, device_id_type=MESH)
    for j in range(1, nt):
        pl.semaphore_signal(barrier, inc=1, device_id={"tp": (t + j) % nt}, device_id_type=MESH)
    with sc("bar"):
        pl.semaphore_wait(barrier, ns + nt - 1)

    def kv_out(i, kk, vv):
        return (
            remote(kk, kbuf.at[i], kv_send.at[0, i], kv_recv.at[0, i], sp=s + 1),
            remote(vv, vbuf.at[i], kv_send.at[1, i], kv_recv.at[1, i], sp=s + 1),
        )

    def kv_in(i):
        return (
            remote(kbuf.at[i], kbuf.at[i], kv_send.at[0, i], kv_recv.at[0, i], sp=s - 1),
            remote(vbuf.at[i], vbuf.at[i], kv_send.at[1, i], kv_recv.at[1, i], sp=s - 1),
        )

    @pl.when(s + 1 < ns)
    def _():
        for copy in kv_out(0, k_ref, v_ref):
            copy.start()

    w_out_copy = pltpu.make_async_copy(w_out_ref, w_out, loc_sem.at[0])
    w_out_copy.start()

    def locals_(me):
        own = pl.ds(me * depth, depth)
        copies = []
        for mat in range(2):
            for u in range(nu):
                copies.append(
                    pltpu.make_async_copy(
                        (w_gate_ref, w_up_ref)[mat].at[:, pl.ds(start_of(me) + u * UNIT, UNIT)],
                        wgu.at[u, own, pl.ds(mat * UNIT, UNIT)], loc_sem.at[1 + 2 * u + mat],
                    )
                )
        for j in range(nj):
            copies.append(
                pltpu.make_async_copy(
                    w_down_ref.at[pl.ds(start_of(me), chunk), pl.ds(j * dj, dj)],
                    wd.at[j, :, pl.ds(me * dj, dj)], loc_sem.at[1 + 2 * nu + j],
                )
            )
        return copies

    early = range(nu - 1)
    late = range(nu - 1, nu)

    def opening(me):
        for u in early:
            for dst in range(me - 1, -1, -1):
                send_units(me, dst, (u,))
        if me == 0:
            send_units(0, 1, range(nu))
        for copy in locals_(me):
            copy.start()

    on_each_s(opening)

    if dup:

        @pl.when(s == ns - 1)
        def _():
            for j in range(nj):
                wd[j, :dup, : (ns - 1) * dj] = jnp.zeros((dup, (ns - 1) * dj), BF16)
            for k in range(ns):
                hidden[k, :, :dup] = jnp.zeros((tok, dup), BF16)

    gate_own = gate_t_ref[:, pl.ds(pl.multiple_of(s * tok, tok), tok)].T

    def attend(src, kk, vv, first):
        for h in range(nheads):
            lanes = slice(h * HEAD_DIM, (h + 1) * HEAD_DIM)
            scores = lax.dot_general(
                q_ref[:, lanes], kk[:, lanes], (((1,), (1,)), ((), ())), preferred_element_type=F32
            )
            key_gate = gate_t_ref[h : h + 1, pl.ds(pl.multiple_of(src * tok, tok), tok)]
            scores = scores * scale + gate_own[:, h : h + 1] - key_gate
            if first:
                row = lax.broadcasted_iota(jnp.int32, (tok, tok), 0)
                col = lax.broadcasted_iota(jnp.int32, (tok, tok), 1)
                scores = jnp.where(col <= row, scores, -1e30)
                new = jnp.max(scores, axis=-1, keepdims=True)
                w = jnp.where(col <= row, jnp.exp(scores - new), 0.0)
                tot[h] = jnp.sum(w, axis=-1, keepdims=True)
                acc[h] = jnp.dot(w.astype(BF16), vv[:, lanes], preferred_element_type=F32)
            else:
                old = top[h]
                new = jnp.maximum(old, jnp.max(scores, axis=-1, keepdims=True))
                w = jnp.exp(scores - new)
                shrink = jnp.exp(old - new)
                tot[h] = tot[h] * shrink + jnp.sum(w, axis=-1, keepdims=True)
                acc[h] = acc[h] * shrink + jnp.dot(
                    w.astype(BF16), vv[:, lanes], preferred_element_type=F32
                )
            top[h] = new

    with sc("att0"):
        attend(s, k_ref, v_ref, True)

    def earlier(i):
        for copy in kv_in(i - 1):
            copy.wait_recv()

        @pl.when(s + 1 < ns)
        def _():
            for copy in kv_out(i, kbuf.at[i - 1], vbuf.at[i - 1]):
                copy.start()

        attend(s - i, kbuf.at[i - 1], vbuf.at[i - 1], False)

    with sc("earlier"):
        each(1, s + 1, earlier)

    for h in range(nheads):
        att[:, h * HEAD_DIM : (h + 1) * HEAD_DIM] = (acc[h] / tot[h]).astype(BF16)

    def head_copy(j):
        dst = (t + j) % nt
        return remote(
            att.at[pl.ds(pl.multiple_of(dst * rows, rows), rows)], heads.at[j - 1],
            h_send.at[j - 1], h_recv.at[j - 1], tp=dst,
        )

    for j in range(1, nt):
        head_copy(j).start()

    with sc("mix"):
        w_out_copy.wait()
        resid[...] = resid_ref[...].astype(F32) + jnp.dot(
            att[pl.ds(pl.multiple_of(t * rows, rows), rows), :],
            w_out[pl.ds(pl.multiple_of(t * att_w, att_w), att_w), :], preferred_element_type=F32,
        )

        def mix(j):
            head_copy(j).wait_recv()
            src = (t + nt - j) % nt
            resid[...] += jnp.dot(
                heads[j - 1], w_out[pl.ds(pl.multiple_of(src * att_w, att_w), att_w), :],
                preferred_element_type=F32,
            )

        each(1, nt, mix)
        full = resid[...]
        normed = full * lax.rsqrt(jnp.mean(full * full, axis=-1, keepdims=True) + 1e-06)
        nall[s, t] = (normed * gain_ref[...]).astype(BF16)

    def row_z(kind, src, to):
        block = nall.at[src, t]
        return remote(block, block, az_send.at[kind, src], az_recv.at[src], sp=to)

    def row_x(src, who):
        block = nall.at[src, who]
        return remote(block, block, ax_send.at[src], ax_recv.at[src], tp=tx)

    def row_c(kind, src, who):
        block = nall.at[src, who]
        return remote(block, block, ac_send.at[kind, src], ac_recv.at[kind, src], tp=tc)

    def spread(src):
        row_x(src, t).start()
        row_c(0, src, t).start()

    def relay(src):
        row_x(src, tx).wait_recv()
        row_c(1, src, tx).start()

    def take(me, src):
        row_z(0, src, me).wait_recv()
        if (me, src // 2) in ((1, 1), (2, 0)):
            row_z(0, src, me ^ 1).start()
        spread(src)

    def gather(me):
        near, mid = me ^ 1, 2 if me < 2 else 1
        row_z(1, me, mid).start()
        row_z(0, me, near).start()
        spread(me)
        last = nu - 1
        if me < 2:
            for u in range(nu):
                send_units(me, 2, (u,))
                send_units(me, 3, (u,))
        if me == 0:
            relay(0)
            for u in early:
                pass_units(0, u, 1, 2, 3)
            for u in late:
                pass_units(0, u, 1)
            take(0, 1)
            relay(1)
            for j in range(nj):
                send_down(0, j, 1)
            take(0, 2)
            take(0, 3)
            relay(2)
            for u in late:
                pass_units(0, u, 2, 3)
            relay(3)
            send_down(0, 0, 2, 3)
        elif me == 1:
            send_units(1, 0, late)
            for j in range(nj):
                send_down(1, j, 0)
            for u in range(nu):
                pass_units(1, u, 0)
            relay(1)
            for u in early:
                pass_units(1, u, 2, 3)
            take(1, 0)
            take(1, 2)
            take(1, 3)
            relay(0)
            pass_units(1, last, 2)
            relay(2)
            pass_units(1, last, 3)
            for j in range(nj):
                send_down(1, j, 2, 3)
            relay(3)
        elif me == 2:
            send_units(2, 1, late)
            send_units(2, 3, range(last))
            for u in early:
                pass_units(2, u, 3)
            relay(2)
            take(2, 0)
            take(2, 1)
            send_units(2, 3, late)
            pass_units(2, 0, 0)
            relay(0)
            pass_units(2, 1, 0)
            relay(1)
            for u in late:
                pass_units(2, u, 0, 3)
            send_units(2, 0, late)
            pass_units(2, 0, 1)
            take(2, 3)
            send_down(2, 0, 1)
            pass_units(2, 1, 1)
            relay(3)
            send_down(2, 0, 0, 3)
            for j in range(1, nj):
                send_down(2, j, 3)
        else:
            send_units(3, 2, late)
            send_units(3, 1, late)
            relay(3)
            take(3, 2)
            pass_units(3, 0, 2, 0)
            pass_units(3, 1, 2, 0)
            relay(2)
            take(3, 0)
            send_units(3, 0, late)
            pass_units(3, last, 0)
            for j in range(nj):
                send_down(3, j, 2)
            take(3, 1)
            relay(0)
            pass_units(3, 0, 1)
            pass_units(3, 1, 1)
            pass_units(3, last, 2)
            relay(1)
            send_down(3, 0, 1, 0)

    with sc("gather"):
        on_each_s(gather)

    def between(me, u):
        if u == 0:
            if me >= 2:
                for i in late:
                    pass_units(me, i, 1)
            elif me == 1:
                pass_down(1, 0, 0, 2)
            else:
                pass_down(0, 0, 1)
        elif u == 1:
            if me in (0, 2, 3):
                for j in range(1, nj):
                    send_down(me, j, *((2, 3) if me == 0 else (1, 0)))
            if me >= 2:
                pass_down(me, 0, me ^ 1, 1)
            else:
                pass_down(me, 0, 2 if me == 0 else 3)
        elif u == nu - 1:
            if me < 2:
                if me == 0:
                    pass_down(0, 0, 3)
            else:
                pass_down(me, 0, 0)

    def own_units(u):
        def body(me):
            copies = locals_(me)
            for mat in range(2):
                copies[mat * nu + u].wait()

        on_each_s(body)

    def own_down(j):
        on_each_s(lambda me: locals_(me)[2 * nu + j].wait())

    def twin_units(u):
        def body(me):
            if u >= first_unit(me):
                for src in range(ns):
                    if src != me:
                        unit_y(u, src, 1 - g).wait_recv()

        on_each_s(body)

    def twin_down(j):
        def body(me):
            for src in range(ns):
                if src != me:
                    down_y(j, src, 1 - g, me).wait_recv()

        on_each_s(body)

    def hide(u):
        def block(k):
            y = jnp.dot(nall[k].reshape(tok, width), wgu[u], preferred_element_type=F32)
            gate, up = y[:, :UNIT], y[:, UNIT:]
            hidden[k, :, u * UNIT : (u + 1) * UNIT] = (gate / (1.0 + jnp.exp(-gate)) * up).astype(BF16)

        def run():
            each(0, ns, block)

        if (u + 1) * UNIT <= dup:
            pl.when(s < ns - 1)(run)
        else:
            run()

    with sc("rows"):

        def rows_in(k):
            row_c(0, k, tc).wait_recv()
            row_c(1, k, (tc + 2) % 4).wait_recv()

        each(0, ns, rows_in)
    for u in range(nu):
        with sc(f"tw{u}"):
            own_units(u)
            twin_units(u)
        with sc(f"hide{u}"):
            hide(u)
        with sc(f"bt{u}"):
            on_each_s(lambda me, u=u: between(me, u))

    def pass_down_all(j):
        on_each_s(lambda me: pass_down(me, j, me ^ 1, me ^ 2, me ^ 3))

    steps = [(j, m) for j in range(nj) for m in (3, 1, 2, 0)]
    nd = len(steps)

    def sum_c(d):
        return remote(part.at[d, :, 1 - c], crecv.at[d], rc_send.at[d], rc_recv.at[d], tp=tc)

    def sum_x(d):
        return remote(csend.at[d], xrecv.at[d], rx_send.at[d], rx_recv.at[d], tp=tx)

    def sum_z(d):
        far = steps[d][1] == 2
        return remote(
            zsend.at[d], zrecv.at[d], rz_send.at[d], rz_recv.at[d], sp=xor(s, 2 if far else 1)
        )

    def stage_x(d):
        sum_c(d).wait_recv()
        csend[d] = (part[d, 1 - x, c].astype(F32) + crecv[d, 1 - x].astype(F32)).astype(BF16)
        sum_x(d).start()
        keep[d] = part[d, x, c].astype(F32) + crecv[d, x].astype(F32)

    def stage_z(d):
        m = steps[d][1]
        if m == 0:
            return
        sum_x(d).wait_recv()
        total = keep[d] + xrecv[d].astype(F32)
        if m == 2:
            sum_z(d - 2).wait_recv()
            total = total + zrecv[d - 2].astype(F32)
        zsend[d] = total.astype(BF16)
        sum_z(d).start()

    def feed(d):
        j, m = steps[d]
        src = hidden[xor(s, m)]
        piece = math.gcd(wide, 512)

        def down(p):
            cols = pl.ds(pl.multiple_of(p * piece, piece), piece)
            y = jnp.dot(src, wd[j, :, cols], preferred_element_type=F32).astype(BF16)
            part[d, :, :, :, cols] = y.reshape(2, 2, rows, piece)

        each(0, wide // piece, down)
        sum_c(d).start()

    def finish(j):
        d = 4 * j + 3
        sum_x(d).wait_recv()
        sum_z(d - 1).wait_recv()
        sum_z(d - 2).wait_recv()
        total = (
            keep[d] + xrecv[d].astype(F32) + zrecv[d - 1].astype(F32) + zrecv[d - 2].astype(F32)
        )
        for p in range(ns):
            cols = slice(p * depth + j * dj, p * depth + (j + 1) * dj)
            out_ref[:, cols] = (resid[:, cols] + total[:, p * dj : (p + 1) * dj]).astype(BF16)

    for d in range(nd):
        j, k = d // 4, d % 4
        if k == 0:
            with sc(f"td{j}"):
                own_down(j)
                twin_down(j)
        for ahead in range(1, nj):
            if d == 1 + (ahead - 1) * 5 // 2:
                with sc(f"pd{ahead}"):
                    pass_down_all(ahead)
        with sc(f"f{d}"):
            feed(d)
            if d >= 1:
                stage_x(d - 1)
            if d >= 3:
                stage_z(d - 3)
    with sc("st"):
        stage_x(nd - 1)
        for d in range(nd - 3, nd):
            stage_z(d)
    for j in range(nj):
        with sc(f"fin{j}"):
            finish(j)

    @pl.when(s + 1 < ns)
    def _():
        def sent(i):
            for copy in kv_out(i, kbuf.at[0], vbuf.at[0]):
                copy.wait_send()

        each(0, s + 1, sent)

    def drain(me):
        row_z(0, me, me ^ 1).wait_send()
        row_z(1, me, me ^ 1).wait_send()
        for src in range(ns):
            if (me, src // 2) in ((1, 1), (2, 0)):
                row_z(0, src, me ^ 1).wait_send()
            if src != me:
                for u in range(nu):
                    if u >= first_unit(src):
                        for mat in range(2):
                            unit_z(mat, u, me, src).wait_send()
                    if u >= first_unit(me):
                        unit_y(u, src, g).wait_send()
                for j in range(nj):
                    down_z(j, me, src).wait_send()
                    down_y(j, src, g, me).wait_send()

    with sc("drain"):
        on_each_s(drain)
        for j in range(1, nt):
            head_copy(j).wait_send()

        def spread_done(i):
            row_x(i, t).wait_send()
            row_c(0, i, t).wait_send()
            row_c(1, i, tx).wait_send()

        each(0, ns, spread_done)
        for d in range(nd):
            sum_c(d).wait_send()
            sum_x(d).wait_send()
            if steps[d][1]:
                sum_z(d).wait_send()


def fused(ns, nt, chunk, nj, resid_in, queries, keys, values, cum_gate, w_out, norm_gain, w_gate, w_up, w_down):
    rows, width = resid_in.shape
    tok, att_w = queries.shape
    depth, units = w_gate.shape
    nheads = att_w // HEAD_DIM
    nu, nd, wide = chunk // UNIT, 4 * nj, width // nj
    vm = pl.BlockSpec(memory_space=pltpu.VMEM)
    hbm = pl.BlockSpec(memory_space=pltpu.HBM)
    dma = pltpu.SemaphoreType.DMA
    return pl.pallas_call(
        functools.partial(layer_kernel, (ns, nt, chunk, nj)),
        out_shape=jax.ShapeDtypeStruct((rows, width), BF16),
        in_specs=[vm] * 6 + [hbm] * 4,
        out_specs=vm,
        scratch_shapes=[
            pltpu.VMEM((ns - 1, tok, att_w), BF16),
            pltpu.VMEM((ns - 1, tok, att_w), BF16),
            pltpu.VMEM((nheads, tok, 1), F32),
            pltpu.VMEM((nheads, tok, 1), F32),
            pltpu.VMEM((nheads, tok, HEAD_DIM), F32),
            pltpu.VMEM((tok, att_w), BF16),
            pltpu.VMEM((nt - 1, rows, att_w), BF16),
            pltpu.VMEM(w_out.shape, BF16),
            pltpu.VMEM((rows, width), F32),
            pltpu.VMEM((ns, nt, rows, width), BF16),
            pltpu.VMEM((nu, width, 2 * UNIT), BF16),
            pltpu.VMEM((nj, chunk, wide), BF16),
            pltpu.VMEM((ns, tok, chunk), BF16),
            pltpu.VMEM((nd, 2, 2, rows, wide), BF16),
            pltpu.VMEM((nd, 2, rows, wide), BF16),
            pltpu.VMEM((nd, rows, wide), BF16),
            pltpu.VMEM((nd, rows, wide), F32),
            pltpu.VMEM((nd, rows, wide), BF16),
            pltpu.VMEM((nd, rows, wide), BF16),
            pltpu.VMEM((nd, rows, wide), BF16),
            dma((1 + 2 * nu + nj,)),
            dma((2, ns)), dma((2, ns)),
            dma((2 * nu, ns)), dma((2 * nu, ns)),
            dma((nu, ns)), dma((nu, ns)),
            dma((nj, ns)), dma((nj, ns)),
            dma((nj, ns)), dma((nj, ns)),
            dma((nt - 1,)), dma((nt - 1,)),
            dma((2, ns)), dma((ns,)),
            dma((ns,)), dma((ns,)),
            dma((2, ns)), dma((2, ns)),
            dma((nd,)), dma((nd,)),
            dma((nd,)), dma((nd,)),
            dma((nd,)), dma((nd,)),
        ],
        compiler_params=pltpu.CompilerParams(
            collective_id=0, has_side_effects=True, vmem_limit_bytes=60 * 2**20
        ),
        name="layer",
    )(
        resid_in, queries, keys, values, cum_gate.T, norm_gain[None, :], w_out, w_gate,
        w_up, w_down,
    )


def pick(mesh):
    ng, ns, nt = (mesh.shape[a] for a in ("grp", "sp", "tp"))

    def step(*args):
        resid_in, queries, cum_gate, w_gate = args[0], args[1], args[4], args[7]
        rows, width = resid_in.shape
        depth, units = w_gate.shape
        chunk = -(-units // (128 * ns)) * 128
        need = 2 * ns * nt * rows * width * 4 + 6 * width * chunk + 2 * args[5].size
        fits = (
            ng == 2 and nt == 4 and ns == 4 and units % UNIT == 0 and chunk >= 2 * UNIT and depth % (128 * PIECES) == 0 and (ns - 1) * chunk < units
            and depth % 256 == 0 and width % 256 == 0 and (chunk - ns * chunk + units) % 32 == 0 and width == ns * depth and rows % 16 == 0
            and queries.shape[0] == rows * nt and queries.shape[0] % 128 == 0
            and cum_gate.shape[0] == ns * nt * rows and queries.shape[1] % 128 == 0
            and need < 40 * 2**20
        )
        if fits:
            return fused(ns, nt, chunk, PIECES, *args)
        return on_device(*args)

    return step


def solution(mesh):
    return jax.shard_map(
        pick(mesh),
        mesh=mesh,
        in_specs=(
            P(("grp", "sp", "tp"), None),
            P(("grp", "sp"), "tp"),
            P(("grp", "sp"), "tp"),
            P(("grp", "sp"), "tp"),
            P("grp", "tp"),
            P(),
            P(),
            P("sp", "tp"),
            P("sp", "tp"),
            P("tp", "sp"),
        ),
        out_specs=P(("grp", "sp", "tp"), None),
        check_vma=False,
    )
```

```python
import functools
import math

import jax
import jax.numpy as jnp
from jax import lax
from jax.experimental import pallas as pl
from jax.experimental.pallas import tpu as pltpu
from jax.sharding import PartitionSpec as P

HEAD_DIM = 64


def on_device(resid_in, queries, keys, values, cum_gate, w_out, norm_gain, w_gate, w_up, w_down):
    tok_rows = queries.shape[0]
    local_heads = queries.shape[1] // HEAD_DIM
    scale = HEAD_DIM ** (-0.5)
    offset = lax.axis_index("sp") * tok_rows
    query_heads = queries.reshape(tok_rows, local_heads, HEAD_DIM)
    own_gate = lax.dynamic_slice_in_dim(cum_gate, offset, tok_rows, 0).T
    query_pos = offset + jnp.arange(tok_rows, dtype=jnp.int32)
    last_pos = offset + tok_rows - 1
    initial = (
        jnp.full((local_heads, tok_rows), -1e30, jnp.float32),
        jnp.zeros((local_heads, tok_rows), jnp.float32),
        jnp.zeros((tok_rows, local_heads, HEAD_DIM), jnp.float32),
    )
    pair = lax.all_gather(jnp.stack([keys, values]), "sp", axis=1, tiled=True)
    key_piece, value_piece = pair[0], pair[1]
    length = key_piece.shape[0]
    span = math.gcd(length, 512)

    def block(index, state):
        begin = index * span

        def work(inner):
            maxima, totals, summed = inner
            key_block = lax.dynamic_slice_in_dim(key_piece, index * span, span, 0).reshape(
                span, local_heads, HEAD_DIM
            )
            value_block_rows = lax.dynamic_slice_in_dim(value_piece, index * span, span, 0).reshape(
                span, local_heads, HEAD_DIM
            )
            key_gate = lax.dynamic_slice_in_dim(cum_gate, begin, span, 0).T
            scores = (
                jnp.einsum(
                    "qhd,khd->hqk", query_heads, key_block, preferred_element_type=jnp.float32
                )
                * scale
            )
            scores = scores + own_gate[:, :, None] - key_gate[:, None, :]
            key_pos = begin + jnp.arange(span, dtype=jnp.int32)
            mask = (key_pos[None, :] <= query_pos[:, None])[None]
            scores = jnp.where(mask, scores, -1e30)
            new_max = jnp.maximum(maxima, jnp.max(scores, axis=-1))
            weights = jnp.where(mask, jnp.exp(scores - new_max[:, :, None]), 0.0)
            rescale = jnp.exp(maxima - new_max)
            totals = totals * rescale + jnp.sum(weights, axis=-1)
            product = jnp.einsum(
                "hqk,khd->qhd",
                weights.astype(jnp.bfloat16),
                value_block_rows,
                preferred_element_type=jnp.float32,
            )
            summed = summed * rescale.T[:, :, None] + product
            return (new_max, totals, summed)

        return lax.cond(begin <= last_pos, work, lambda inner: inner, state)

    maxima, totals, summed = lax.fori_loop(0, length // span, block, initial)
    attended = (
        (summed / totals.T[:, :, None])
        .reshape(tok_rows, local_heads * HEAD_DIM)
        .astype(jnp.bfloat16)
    )
    head_rows = lax.all_to_all(attended, "tp", split_axis=0, concat_axis=1, tiled=True)
    mixed = jnp.dot(head_rows, w_out, preferred_element_type=jnp.float32)
    resid = resid_in.astype(jnp.float32) + mixed
    normed = resid * lax.rsqrt(jnp.mean(resid * resid, axis=-1, keepdims=True) + 1e-06)
    normed = (normed * norm_gain).astype(jnp.bfloat16)
    all_rows = lax.all_gather(normed, ("sp", "tp"), axis=0, tiled=True)
    full_gate, full_up, full_down = (
        lax.all_to_all(w_gate, "sp", split_axis=1, concat_axis=0, tiled=True),
        lax.all_to_all(w_up, "sp", split_axis=1, concat_axis=0, tiled=True),
        lax.all_to_all(w_down, "sp", split_axis=0, concat_axis=1, tiled=True),
    )
    gate = jnp.dot(all_rows, full_gate, preferred_element_type=jnp.float32)
    up = jnp.dot(all_rows, full_up, preferred_element_type=jnp.float32)
    hidden = (jax.nn.silu(gate) * up).astype(jnp.bfloat16)
    terms = jnp.dot(hidden, full_down, preferred_element_type=jnp.float32)
    back = lax.psum_scatter(
        terms.astype(jnp.bfloat16), ("sp", "tp"), scatter_dimension=0, tiled=True
    ).astype(jnp.float32)
    return (resid + back).astype(jnp.bfloat16)


MESH = pl.DeviceIdType.MESH
F32 = jnp.float32
BF16 = jnp.bfloat16
UNIT = 128
PIECES = 4


def layer_kernel(
    dims, resid_ref, q_ref, k_ref, v_ref, gate_t_ref, gain_ref, w_out_ref, w_gate_ref,
    w_up_ref, w_down_ref, out_ref, kbuf, vbuf, top, tot, acc, att, heads, w_out, resid, nall, wgu,
    wd, hidden, part, crecv, csend, keep, xrecv, zsend, zrecv, loc_sem, kv_send, kv_recv, wz_send,
    wz_recv, wy_send, wy_recv, dz_send, dz_recv, dy_send, dy_recv, h_send, h_recv, az_send, az_recv,
    ax_send, ax_recv, ac_send, ac_recv, rc_send, rc_recv, rx_send, rx_recv, rz_send, rz_recv,
):
    ns, nt, chunk, nj = dims
    g, s, t = lax.axis_index("grp"), lax.axis_index("sp"), lax.axis_index("tp")
    rows, width = resid_ref.shape
    tok, att_w = q_ref.shape
    depth, units = w_gate_ref.shape
    nheads = att_w // HEAD_DIM
    half_depth = depth // 2
    dup = ns * chunk - units
    nu, dj = chunk // UNIT, depth // nj
    wide = ns * dj
    x, c = t // 2, t % 2
    tx = (t + 2) % 4
    tc = t + 1 - 2 * c
    scale = HEAD_DIM ** (-0.5)
    sc = jax.named_scope

    def start_of(i):
        return min(i * chunk, units - chunk)

    def first_unit(i):
        return dup // UNIT if i == ns - 1 else 0

    def remote(src, dst, send, recv, **where):
        return pltpu.make_async_remote_copy(
            src_ref=src, dst_ref=dst, send_sem=send, recv_sem=recv, device_id=where,
            device_id_type=MESH,
        )

    def xor(a, b):
        hi, lo, bh, bl = a // 2, a % 2, b // 2, b % 2
        return 2 * (hi + bh - 2 * hi * bh) + lo + bl - 2 * lo * bl

    def on_each_s(body):
        for k in range(ns):
            pl.when(s == k)(lambda k=k: (body(k), None)[1])

    def each(low, high, body):
        lax.fori_loop(low, high, lambda i, z: (body(i), z)[1], 0)

    def unit_band(src, half):
        return pl.ds(pl.multiple_of(src * depth + half * half_depth, half_depth), half_depth)

    def unit_z(mat, u, me, dst):
        src = (w_gate_ref, w_up_ref)[mat].at[
            pl.ds(pl.multiple_of(g * half_depth, half_depth), half_depth),
            pl.ds(start_of(dst) + u * UNIT, UNIT),
        ]
        return remote(
            src, wgu.at[u, unit_band(me, g), pl.ds(mat * UNIT, UNIT)],
            wz_send, wz_recv.at[2 * u + mat, me], sp=dst,
        )

    def unit_in(mat, u, src):
        block = wgu.at[u, unit_band(src, g), pl.ds(mat * UNIT, UNIT)]
        return remote(block, block, wz_send, wz_recv.at[2 * u + mat, src], sp=src)

    def unit_y(u, src, half):
        block = wgu.at[u, unit_band(src, half)]
        return remote(block, block, wy_send, wy_recv.at[u, src], grp=1 - g)

    def send_units(me, dst, us):
        for u in us:
            if u >= first_unit(dst):
                for mat in range(2):
                    unit_z(mat, u, me, dst).start()

    def pass_units(me, u, *srcs):
        if u >= first_unit(me):
            for src in srcs:
                for mat in range(2):
                    unit_in(mat, u, src).wait_recv()
                unit_y(u, src, g).start()

    def down_band(j, src, half, me):
        skip = first_unit(me) * UNIT
        size = (chunk - skip) // 2
        return wd.at[
            j, pl.ds(pl.multiple_of(skip + half * size, math.gcd(128, size)), size),
            pl.ds(src * dj, dj),
        ]

    def down_z(j, me, dst):
        skip = first_unit(dst) * UNIT
        size = (chunk - skip) // 2
        src = w_down_ref.at[
            pl.ds(pl.multiple_of(start_of(dst) + skip + g * size, math.gcd(128, size)), size),
            pl.ds(j * dj, dj),
        ]
        return remote(
            src, down_band(j, me, g, dst), dz_send, dz_recv.at[j, me], sp=dst
        )

    def down_y(j, src, half, me):
        block = down_band(j, src, half, me)
        return remote(block, block, dy_send, dy_recv.at[j, src], grp=1 - g)

    def send_down(me, j, *dsts):
        for dst in dsts:
            down_z(j, me, dst).start()

    def pass_down(me, j, *srcs):
        for src in srcs:
            block = down_band(j, src, g, me)
            with sc(f"d{j}.{src}"):
                remote(block, block, dz_send, dz_recv.at[j, src], sp=src).wait_recv()
            down_y(j, src, g, me).start()

    barrier = pltpu.get_barrier_semaphore()

    def greet(i):
        pl.semaphore_signal(barrier, inc=1, device_id={"sp": i}, device_id_type=MESH)

    each(0, s, greet)
    each(s + 1, ns, greet)
    pl.semaphore_signal(barrier, inc=1, device_id={"grp": 1 - g}, device_id_type=MESH)
    for j in range(1, nt):
        pl.semaphore_signal(barrier, inc=1, device_id={"tp": (t + j) % nt}, device_id_type=MESH)
    with sc("bar"):
        pl.semaphore_wait(barrier, ns + nt - 1)

    def kv_out(i, kk, vv):
        return (
            remote(kk, kbuf.at[i], kv_send.at[0, i], kv_recv.at[0, i], sp=s + 1),
            remote(vv, vbuf.at[i], kv_send.at[1, i], kv_recv.at[1, i], sp=s + 1),
        )

    def kv_in(i):
        return (
            remote(kbuf.at[i], kbuf.at[i], kv_send.at[0, i], kv_recv.at[0, i], sp=s - 1),
            remote(vbuf.at[i], vbuf.at[i], kv_send.at[1, i], kv_recv.at[1, i], sp=s - 1),
        )

    @pl.when(s + 1 < ns)
    def _():
        for copy in kv_out(0, k_ref, v_ref):
            copy.start()

    w_out_copy = pltpu.make_async_copy(w_out_ref, w_out, loc_sem.at[0])
    w_out_copy.start()

    def locals_(me):
        own = pl.ds(me * depth, depth)
        copies = []
        for mat in range(2):
            for u in range(nu):
                copies.append(
                    pltpu.make_async_copy(
                        (w_gate_ref, w_up_ref)[mat].at[:, pl.ds(start_of(me) + u * UNIT, UNIT)],
                        wgu.at[u, own, pl.ds(mat * UNIT, UNIT)], loc_sem.at[1 + 2 * u + mat],
                    )
                )
        for j in range(nj):
            copies.append(
                pltpu.make_async_copy(
                    w_down_ref.at[pl.ds(start_of(me), chunk), pl.ds(j * dj, dj)],
                    wd.at[j, :, pl.ds(me * dj, dj)], loc_sem.at[1 + 2 * nu + j],
                )
            )
        return copies

    early = range(nu - 1)
    late = range(nu - 1, nu)

    def opening(me):
        for u in early:
            for dst in range(me - 1, -1, -1):
                send_units(me, dst, (u,))
        if me == 0:
            send_units(0, 1, range(nu))
        for copy in locals_(me):
            copy.start()

    on_each_s(opening)

    if dup:

        @pl.when(s == ns - 1)
        def _():
            for j in range(nj):
                wd[j, :dup, : (ns - 1) * dj] = jnp.zeros((dup, (ns - 1) * dj), BF16)
            for k in range(ns):
                hidden[k, :, :dup] = jnp.zeros((tok, dup), BF16)

    gate_own = gate_t_ref[:, pl.ds(pl.multiple_of(s * tok, tok), tok)].T

    def attend(src, kk, vv, first):
        for h in range(nheads):
            lanes = slice(h * HEAD_DIM, (h + 1) * HEAD_DIM)
            scores = lax.dot_general(
                q_ref[:, lanes], kk[:, lanes], (((1,), (1,)), ((), ())), preferred_element_type=F32
            )
            key_gate = gate_t_ref[h : h + 1, pl.ds(pl.multiple_of(src * tok, tok), tok)]
            scores = scores * scale + gate_own[:, h : h + 1] - key_gate
            if first:
                row = lax.broadcasted_iota(jnp.int32, (tok, tok), 0)
                col = lax.broadcasted_iota(jnp.int32, (tok, tok), 1)
                scores = jnp.where(col <= row, scores, -1e30)
                new = jnp.max(scores, axis=-1, keepdims=True)
                w = jnp.where(col <= row, jnp.exp(scores - new), 0.0)
                tot[h] = jnp.sum(w, axis=-1, keepdims=True)
                acc[h] = jnp.dot(w.astype(BF16), vv[:, lanes], preferred_element_type=F32)
            else:
                old = top[h]
                new = jnp.maximum(old, jnp.max(scores, axis=-1, keepdims=True))
                w = jnp.exp(scores - new)
                shrink = jnp.exp(old - new)
                tot[h] = tot[h] * shrink + jnp.sum(w, axis=-1, keepdims=True)
                acc[h] = acc[h] * shrink + jnp.dot(
                    w.astype(BF16), vv[:, lanes], preferred_element_type=F32
                )
            top[h] = new

    with sc("att0"):
        attend(s, k_ref, v_ref, True)

    def earlier(i):
        for copy in kv_in(i - 1):
            copy.wait_recv()

        @pl.when(s + 1 < ns)
        def _():
            for copy in kv_out(i, kbuf.at[i - 1], vbuf.at[i - 1]):
                copy.start()

        attend(s - i, kbuf.at[i - 1], vbuf.at[i - 1], False)

    with sc("earlier"):
        each(1, s + 1, earlier)

    for h in range(nheads):
        att[:, h * HEAD_DIM : (h + 1) * HEAD_DIM] = (acc[h] / tot[h]).astype(BF16)

    def head_copy(j):
        dst = (t + j) % nt
        return remote(
            att.at[pl.ds(pl.multiple_of(dst * rows, rows), rows)], heads.at[j - 1],
            h_send.at[j - 1], h_recv.at[j - 1], tp=dst,
        )

    for j in range(1, nt):
        head_copy(j).start()

    with sc("mix"):
        w_out_copy.wait()
        resid[...] = resid_ref[...].astype(F32) + jnp.dot(
            att[pl.ds(pl.multiple_of(t * rows, rows), rows), :],
            w_out[pl.ds(pl.multiple_of(t * att_w, att_w), att_w), :], preferred_element_type=F32,
        )

        def mix(j):
            head_copy(j).wait_recv()
            src = (t + nt - j) % nt
            resid[...] += jnp.dot(
                heads[j - 1], w_out[pl.ds(pl.multiple_of(src * att_w, att_w), att_w), :],
                preferred_element_type=F32,
            )

        each(1, nt, mix)
        full = resid[...]
        normed = full * lax.rsqrt(jnp.mean(full * full, axis=-1, keepdims=True) + 1e-06)
        nall[s, t] = (normed * gain_ref[...]).astype(BF16)

    def row_z(kind, src, to):
        block = nall.at[src, t]
        return remote(block, block, az_send.at[kind, src], az_recv.at[src], sp=to)

    def row_x(src, who):
        block = nall.at[src, who]
        return remote(block, block, ax_send.at[src], ax_recv.at[src], tp=tx)

    def row_c(kind, src, who):
        block = nall.at[src, who]
        return remote(block, block, ac_send.at[kind, src], ac_recv.at[kind, src], tp=tc)

    def spread(src):
        row_x(src, t).start()
        row_c(0, src, t).start()

    def relay(src):
        row_x(src, tx).wait_recv()
        row_c(1, src, tx).start()

    def take(me, src):
        row_z(0, src, me).wait_recv()
        if (me, src // 2) in ((1, 1), (2, 0)):
            row_z(0, src, me ^ 1).start()
        spread(src)

    def gather(me):
        near, mid = me ^ 1, 2 if me < 2 else 1
        row_z(1, me, mid).start()
        row_z(0, me, near).start()
        spread(me)
        last = nu - 1
        if me < 2:
            for u in range(nu):
                send_units(me, 2, (u,))
                send_units(me, 3, (u,))
        if me == 0:
            relay(0)
            for u in early:
                pass_units(0, u, 1, 2, 3)
            for u in late:
                pass_units(0, u, 1)
            take(0, 1)
            relay(1)
            for j in range(nj):
                send_down(0, j, 1)
            take(0, 2)
            take(0, 3)
            relay(2)
            for u in late:
                pass_units(0, u, 2)
            send_down(0, 0, 2, 3)
            pass_down(0, 0, 1)
            relay(3)
        elif me == 1:
            send_units(1, 0, late)
            for j in range(nj):
                send_down(1, j, 0)
            for u in range(nu):
                pass_units(1, u, 0)
            relay(1)
            for u in early:
                pass_units(1, u, 2, 3)
            take(1, 0)
            take(1, 2)
            take(1, 3)
            relay(0)
            pass_units(1, last, 2)
            relay(2)
            pass_units(1, last, 3)
            for j in range(nj):
                send_down(1, j, 2, 3)
            relay(3)
        elif me == 2:
            send_units(2, 1, late)
            send_units(2, 3, range(last))
            for u in early:
                pass_units(2, u, 3)
            relay(2)
            take(2, 0)
            send_units(2, 3, late)
            take(2, 1)
            pass_units(2, 0, 0)
            relay(0)
            pass_units(2, 1, 0)
            relay(1)
            for u in late:
                pass_units(2, u, 0, 3)
            pass_units(2, 0, 1)
            take(2, 3)
            send_down(2, 0, 1)
            pass_units(2, 1, 1)
            send_units(2, 0, late)
            relay(3)
            send_down(2, 0, 0, 3)
            for j in range(1, nj):
                send_down(2, j, 3)
        else:
            send_units(3, 2, late)
            send_units(3, 1, late)
            relay(3)
            take(3, 2)
            pass_units(3, 0, 2, 0)
            pass_units(3, 1, 2, 0)
            relay(2)
            take(3, 0)
            send_down(3, 0, 1)
            pass_units(3, last, 0)
            for j in range(nj):
                send_down(3, j, 2)
            relay(0)
            pass_units(3, 0, 1)
            pass_units(3, 1, 1)
            send_units(3, 0, late)
            send_down(3, 0, 0)
            pass_units(3, last, 2)
            take(3, 1)
            pass_units(3, last, 1)
            relay(1)
            for j in range(1, nj):
                send_down(3, j, 1, 0)

    with sc("gather"):
        on_each_s(gather)

    def between(me, u):
        if u == 0:
            if me == 2:
                for i in late:
                    pass_units(2, i, 1)
                pass_down(2, 0, 3)
            elif me == 3:
                pass_down(3, 0, 2, 1)
            elif me == 1:
                pass_down(1, 0, 0, 2)
            else:
                for i in late:
                    pass_units(0, i, 3)
                pass_down(0, 0, 2)
        elif u == 1:
            if me in (0, 2):
                for j in range(1, nj):
                    send_down(me, j, *((2, 3) if me == 0 else (1, 0)))
            if me == 2:
                pass_down(2, 0, 1, 0)
            elif me == 3:
                pass_down(3, 0, 0)
            else:
                pass_down(me, 0, 3)

    def own_units(u):
        def body(me):
            copies = locals_(me)
            for mat in range(2):
                copies[mat * nu + u].wait()

        on_each_s(body)

    def own_down(j):
        on_each_s(lambda me: locals_(me)[2 * nu + j].wait())

    def twin_units(u):
        def body(me):
            if u >= first_unit(me):
                for src in range(ns):
                    if src != me:
                        unit_y(u, src, 1 - g).wait_recv()

        on_each_s(body)

    def twin_down(j):
        def body(me):
            for src in range(ns):
                if src != me:
                    down_y(j, src, 1 - g, me).wait_recv()

        on_each_s(body)

    def hide(u):
        def block(k):
            y = jnp.dot(nall[k].reshape(tok, width), wgu[u], preferred_element_type=F32)
            gate, up = y[:, :UNIT], y[:, UNIT:]
            hidden[k, :, u * UNIT : (u + 1) * UNIT] = (gate / (1.0 + jnp.exp(-gate)) * up).astype(BF16)

        def run():
            each(0, ns, block)

        if (u + 1) * UNIT <= dup:
            pl.when(s < ns - 1)(run)
        else:
            run()

    with sc("rows"):

        def rows_in(k):
            row_c(0, k, tc).wait_recv()
            row_c(1, k, (tc + 2) % 4).wait_recv()

        each(0, ns, rows_in)
    for u in range(nu):
        with sc(f"tw{u}"):
            own_units(u)
            twin_units(u)
        with sc(f"hide{u}"):
            hide(u)
        with sc(f"bt{u}"):
            on_each_s(lambda me, u=u: between(me, u))

    def pass_down_all(j):
        on_each_s(lambda me: pass_down(me, j, me ^ 1, me ^ 2, me ^ 3))

    steps = [(0, m) for m in (3, 1, 2, 0)]
    steps += [(j, m) for j in range(1, nj - 2) for m in (3, 1, 2)]
    steps += [(j, m) for ms in ((3, 1), (2,)) for j in (nj - 2, nj - 1) for m in ms]
    steps += [(j, 0) for j in range(1, nj)]
    nd = len(steps)
    at = {step: d for d, step in enumerate(steps)}
    slot = {d: i for i, d in enumerate(d for d in range(nd) if steps[d][1])}

    def sum_c(d):
        return remote(part.at[d, :, 1 - c], crecv.at[d], rc_send, rc_recv.at[d], tp=tc)

    def sum_x(d):
        return remote(csend.at[d], xrecv.at[d], rx_send, rx_recv.at[d], tp=tx)

    def sum_z(d):
        i = slot[d]
        to = xor(s, 2 if steps[d][1] == 2 else 1)
        return remote(zsend.at[i], zrecv.at[i], rz_send, rz_recv.at[i], sp=to)

    def stage_x(d):
        sum_c(d).wait_recv()
        csend[d] = (part[d, 1 - x, c].astype(F32) + crecv[d, 1 - x].astype(F32)).astype(BF16)
        sum_x(d).start()
        keep[d] = part[d, x, c].astype(F32) + crecv[d, x].astype(F32)

    def stage_z(d):
        j, m = steps[d]
        if m == 0:
            return
        sum_x(d).wait_recv()
        total = keep[d] + xrecv[d].astype(F32)
        if m == 2:
            from_near = at[j, 3]
            sum_z(from_near).wait_recv()
            total = total + zrecv[slot[from_near]].astype(F32)
        zsend[slot[d]] = total.astype(BF16)
        sum_z(d).start()

    def feed(d):
        j, m = steps[d]
        src = hidden[xor(s, m)]
        piece = math.gcd(wide, 512)

        def down(p):
            cols = pl.ds(pl.multiple_of(p * piece, piece), piece)
            y = jnp.dot(src, wd[j, :, cols], preferred_element_type=F32).astype(BF16)
            part[d, :, :, :, cols] = y.reshape(2, 2, rows, piece)

        each(0, wide // piece, down)
        sum_c(d).start()

    def finish(j):
        d, near, far = at[j, 0], at[j, 1], at[j, 2]
        sum_x(d).wait_recv()
        sum_z(near).wait_recv()
        sum_z(far).wait_recv()
        total = (
            keep[d] + xrecv[d].astype(F32) + zrecv[slot[near]].astype(F32)
            + zrecv[slot[far]].astype(F32)
        )
        for p in range(ns):
            cols = slice(p * depth + j * dj, p * depth + (j + 1) * dj)
            out_ref[:, cols] = (resid[:, cols] + total[:, p * dj : (p + 1) * dj]).astype(BF16)

    ready = set()
    for d in range(nd):
        j = steps[d][0]
        if j not in ready:
            ready.add(j)
            with sc(f"td{j}"):
                own_down(j)
                twin_down(j)
        with sc(f"f{d}"):
            feed(d)
            if d >= 1:
                stage_x(d - 1)
            if d >= 3:
                stage_z(d - 3)
        for ahead in range(1, nj):
            if d == 2 * ahead - 1:
                with sc(f"pd{ahead}"):
                    pass_down_all(ahead)
    with sc("st"):
        stage_x(nd - 1)
        for d in range(nd - 3, nd):
            stage_z(d)
    for j in range(nj):
        with sc(f"fin{j}"):
            finish(j)

    @pl.when(s + 1 < ns)
    def _():
        def sent(i):
            for copy in kv_out(i, kbuf.at[0], vbuf.at[0]):
                copy.wait_send()

        each(0, s + 1, sent)

    def drain(me):
        row_z(0, me, me ^ 1).wait_send()
        row_z(1, me, me ^ 1).wait_send()
        for src in range(ns):
            if (me, src // 2) in ((1, 1), (2, 0)):
                row_z(0, src, me ^ 1).wait_send()
        others = [i for i in range(ns) if i != me]
        for count, sem in (
            (sum(nu - first_unit(i) for i in others), wz_send),
            ((ns - 1) * (nu - first_unit(me)), wy_send),
        ):
            high = count * half_depth
            all_of = wgu.at[0, :high] if high <= width else wgu.at[:, : high // nu]
            remote(all_of, all_of, sem, wz_recv.at[0, me], grp=1 - g).wait_send()
        halves = [(chunk - first_unit(i) * UNIT) // 2 for i in range(ns)]
        for count, sem in (
            (sum(halves[i] for i in others), dz_send), ((ns - 1) * halves[me], dy_send)
        ):
            all_of = wd.at[:, : count // ns]
            remote(all_of, all_of, sem, dz_recv.at[0, me], grp=1 - g).wait_send()

    with sc("drain"):
        on_each_s(drain)
        for j in range(1, nt):
            head_copy(j).wait_send()

        def spread_done(i):
            row_x(i, t).wait_send()
            row_c(0, i, t).wait_send()
            row_c(1, i, tx).wait_send()

        each(0, ns, spread_done)
        remote(crecv, crecv, rc_send, rc_recv.at[0], tp=tc).wait_send()
        remote(xrecv, xrecv, rx_send, rx_recv.at[0], tp=tx).wait_send()
        remote(zrecv, zrecv, rz_send, rz_recv.at[0], tp=tx).wait_send()


def fused(ns, nt, chunk, nj, resid_in, queries, keys, values, cum_gate, w_out, norm_gain, w_gate, w_up, w_down):
    rows, width = resid_in.shape
    tok, att_w = queries.shape
    depth, units = w_gate.shape
    nheads = att_w // HEAD_DIM
    nu, nd, wide = chunk // UNIT, 4 * nj, width // nj
    vm = pl.BlockSpec(memory_space=pltpu.VMEM)
    hbm = pl.BlockSpec(memory_space=pltpu.HBM)
    dma = pltpu.SemaphoreType.DMA
    return pl.pallas_call(
        functools.partial(layer_kernel, (ns, nt, chunk, nj)),
        out_shape=jax.ShapeDtypeStruct((rows, width), BF16),
        in_specs=[vm] * 6 + [hbm] * 4,
        out_specs=vm,
        scratch_shapes=[
            pltpu.VMEM((ns - 1, tok, att_w), BF16),
            pltpu.VMEM((ns - 1, tok, att_w), BF16),
            pltpu.VMEM((nheads, tok, 1), F32),
            pltpu.VMEM((nheads, tok, 1), F32),
            pltpu.VMEM((nheads, tok, HEAD_DIM), F32),
            pltpu.VMEM((tok, att_w), BF16),
            pltpu.VMEM((nt - 1, rows, att_w), BF16),
            pltpu.VMEM(w_out.shape, BF16),
            pltpu.VMEM((rows, width), F32),
            pltpu.VMEM((ns, nt, rows, width), BF16),
            pltpu.VMEM((nu, width, 2 * UNIT), BF16),
            pltpu.VMEM((nj, chunk, wide), BF16),
            pltpu.VMEM((ns, tok, chunk), BF16),
            pltpu.VMEM((nd, 2, 2, rows, wide), BF16),
            pltpu.VMEM((nd, 2, rows, wide), BF16),
            pltpu.VMEM((nd, rows, wide), BF16),
            pltpu.VMEM((nd, rows, wide), F32),
            pltpu.VMEM((nd, rows, wide), BF16),
            pltpu.VMEM((3 * nj, rows, wide), BF16),
            pltpu.VMEM((3 * nj, rows, wide), BF16),
            dma((1 + 2 * nu + nj,)),
            dma((2, ns)), dma((2, ns)),
            dma, dma((2 * nu, ns)),
            dma, dma((nu, ns)),
            dma, dma((nj, ns)),
            dma, dma((nj, ns)),
            dma((nt - 1,)), dma((nt - 1,)),
            dma((2, ns)), dma((ns,)),
            dma((ns,)), dma((ns,)),
            dma((2, ns)), dma((2, ns)),
            dma, dma((nd,)),
            dma, dma((nd,)),
            dma, dma((3 * nj,)),
        ],
        compiler_params=pltpu.CompilerParams(
            collective_id=0, has_side_effects=True, vmem_limit_bytes=60 * 2**20
        ),
        name="layer",
    )(
        resid_in, queries, keys, values, cum_gate.T, norm_gain[None, :], w_out, w_gate,
        w_up, w_down,
    )


def pick(mesh):
    ng, ns, nt = (mesh.shape[a] for a in ("grp", "sp", "tp"))

    def step(*args):
        resid_in, queries, cum_gate, w_gate = args[0], args[1], args[4], args[7]
        rows, width = resid_in.shape
        depth, units = w_gate.shape
        chunk = -(-units // (128 * ns)) * 128
        need = 2 * ns * nt * rows * width * 4 + 6 * width * chunk + 2 * args[5].size
        fits = (
            ng == 2 and nt == 4 and ns == 4 and units % UNIT == 0 and chunk >= 2 * UNIT and depth % (128 * PIECES) == 0 and (ns - 1) * chunk < units
            and depth % 256 == 0 and width % 256 == 0 and (chunk - ns * chunk + units) % 32 == 0 and width == ns * depth and rows % 16 == 0
            and queries.shape[0] == rows * nt and queries.shape[0] % 128 == 0
            and cum_gate.shape[0] == ns * nt * rows and queries.shape[1] % 128 == 0
            and need < 40 * 2**20
        )
        if fits:
            return fused(ns, nt, chunk, PIECES, *args)
        return on_device(*args)

    return step


def solution(mesh):
    return jax.shard_map(
        pick(mesh),
        mesh=mesh,
        in_specs=(
            P(("grp", "sp", "tp"), None),
            P(("grp", "sp"), "tp"),
            P(("grp", "sp"), "tp"),
            P(("grp", "sp"), "tp"),
            P("grp", "tp"),
            P(),
            P(),
            P("sp", "tp"),
            P("sp", "tp"),
            P("tp", "sp"),
        ),
        out_specs=P(("grp", "sp", "tp"), None),
        check_vma=False,
    )
```

```python
import functools
import math

import jax
import jax.numpy as jnp
from jax import lax
from jax.experimental import pallas as pl
from jax.experimental.pallas import tpu as pltpu
from jax.sharding import PartitionSpec as P

HEAD_DIM = 64


def on_device(resid_in, queries, keys, values, cum_gate, w_out, norm_gain, w_gate, w_up, w_down):
    tok_rows = queries.shape[0]
    local_heads = queries.shape[1] // HEAD_DIM
    scale = HEAD_DIM ** (-0.5)
    offset = lax.axis_index("sp") * tok_rows
    query_heads = queries.reshape(tok_rows, local_heads, HEAD_DIM)
    own_gate = lax.dynamic_slice_in_dim(cum_gate, offset, tok_rows, 0).T
    query_pos = offset + jnp.arange(tok_rows, dtype=jnp.int32)
    last_pos = offset + tok_rows - 1
    initial = (
        jnp.full((local_heads, tok_rows), -1e30, jnp.float32),
        jnp.zeros((local_heads, tok_rows), jnp.float32),
        jnp.zeros((tok_rows, local_heads, HEAD_DIM), jnp.float32),
    )
    pair = lax.all_gather(jnp.stack([keys, values]), "sp", axis=1, tiled=True)
    key_piece, value_piece = pair[0], pair[1]
    length = key_piece.shape[0]
    span = math.gcd(length, 512)

    def block(index, state):
        begin = index * span

        def work(inner):
            maxima, totals, summed = inner
            key_block = lax.dynamic_slice_in_dim(key_piece, index * span, span, 0).reshape(
                span, local_heads, HEAD_DIM
            )
            value_block_rows = lax.dynamic_slice_in_dim(value_piece, index * span, span, 0).reshape(
                span, local_heads, HEAD_DIM
            )
            key_gate = lax.dynamic_slice_in_dim(cum_gate, begin, span, 0).T
            scores = (
                jnp.einsum(
                    "qhd,khd->hqk", query_heads, key_block, preferred_element_type=jnp.float32
                )
                * scale
            )
            scores = scores + own_gate[:, :, None] - key_gate[:, None, :]
            key_pos = begin + jnp.arange(span, dtype=jnp.int32)
            mask = (key_pos[None, :] <= query_pos[:, None])[None]
            scores = jnp.where(mask, scores, -1e30)
            new_max = jnp.maximum(maxima, jnp.max(scores, axis=-1))
            weights = jnp.where(mask, jnp.exp(scores - new_max[:, :, None]), 0.0)
            rescale = jnp.exp(maxima - new_max)
            totals = totals * rescale + jnp.sum(weights, axis=-1)
            product = jnp.einsum(
                "hqk,khd->qhd",
                weights.astype(jnp.bfloat16),
                value_block_rows,
                preferred_element_type=jnp.float32,
            )
            summed = summed * rescale.T[:, :, None] + product
            return (new_max, totals, summed)

        return lax.cond(begin <= last_pos, work, lambda inner: inner, state)

    maxima, totals, summed = lax.fori_loop(0, length // span, block, initial)
    attended = (
        (summed / totals.T[:, :, None])
        .reshape(tok_rows, local_heads * HEAD_DIM)
        .astype(jnp.bfloat16)
    )
    head_rows = lax.all_to_all(attended, "tp", split_axis=0, concat_axis=1, tiled=True)
    mixed = jnp.dot(head_rows, w_out, preferred_element_type=jnp.float32)
    resid = resid_in.astype(jnp.float32) + mixed
    normed = resid * lax.rsqrt(jnp.mean(resid * resid, axis=-1, keepdims=True) + 1e-06)
    normed = (normed * norm_gain).astype(jnp.bfloat16)
    all_rows = lax.all_gather(normed, ("sp", "tp"), axis=0, tiled=True)
    full_gate, full_up, full_down = (
        lax.all_to_all(w_gate, "sp", split_axis=1, concat_axis=0, tiled=True),
        lax.all_to_all(w_up, "sp", split_axis=1, concat_axis=0, tiled=True),
        lax.all_to_all(w_down, "sp", split_axis=0, concat_axis=1, tiled=True),
    )
    gate = jnp.dot(all_rows, full_gate, preferred_element_type=jnp.float32)
    up = jnp.dot(all_rows, full_up, preferred_element_type=jnp.float32)
    hidden = (jax.nn.silu(gate) * up).astype(jnp.bfloat16)
    terms = jnp.dot(hidden, full_down, preferred_element_type=jnp.float32)
    back = lax.psum_scatter(
        terms.astype(jnp.bfloat16), ("sp", "tp"), scatter_dimension=0, tiled=True
    ).astype(jnp.float32)
    return (resid + back).astype(jnp.bfloat16)


MESH = pl.DeviceIdType.MESH
F32 = jnp.float32
BF16 = jnp.bfloat16
UNIT = 128
PIECES = 4


def layer_kernel(
    dims, resid_ref, q_ref, k_ref, v_ref, gate_t_ref, gain_ref, w_out_ref, w_gate_ref,
    w_up_ref, w_down_ref, out_ref, kbuf, vbuf, top, tot, acc, att, heads, w_out, resid, nall, wgu,
    wd, hidden, part, crecv, csend, keep, xrecv, zsend, zrecv, loc_sem, kv_send, kv_recv, wz_send,
    wz_recv, wy_send, wy_recv, dz_send, dz_recv, dy_send, dy_recv, h_send, h_recv, az_send, az_recv,
    ax_send, ax_recv, ac_send, ac_recv, rc_send, rc_recv, rx_send, rx_recv, rz_send, rz_recv,
):
    ns, nt, chunk, nj = dims
    g, s, t = lax.axis_index("grp"), lax.axis_index("sp"), lax.axis_index("tp")
    rows, width = resid_ref.shape
    tok, att_w = q_ref.shape
    depth, units = w_gate_ref.shape
    nheads = att_w // HEAD_DIM
    half_depth = depth // 2
    dup = ns * chunk - units
    nu, dj = chunk // UNIT, depth // nj
    wide = ns * dj
    x, c = t // 2, t % 2
    tx = (t + 2) % 4
    tc = t + 1 - 2 * c
    scale = HEAD_DIM ** (-0.5)
    sc = jax.named_scope

    def start_of(i):
        return min(i * chunk, units - chunk)

    def first_unit(i):
        return dup // UNIT if i == ns - 1 else 0

    def remote(src, dst, send, recv, **where):
        return pltpu.make_async_remote_copy(
            src_ref=src, dst_ref=dst, send_sem=send, recv_sem=recv, device_id=where,
            device_id_type=MESH,
        )

    def xor(a, b):
        hi, lo, bh, bl = a // 2, a % 2, b // 2, b % 2
        return 2 * (hi + bh - 2 * hi * bh) + lo + bl - 2 * lo * bl

    def on_each_s(body):
        for k in range(ns):
            pl.when(s == k)(lambda k=k: (body(k), None)[1])

    def each(low, high, body):
        lax.fori_loop(low, high, lambda i, z: (body(i), z)[1], 0)

    def unit_band(src, half):
        return pl.ds(pl.multiple_of(src * depth + half * half_depth, half_depth), half_depth)

    def unit_z(mat, u, me, dst):
        src = (w_gate_ref, w_up_ref)[mat].at[
            pl.ds(pl.multiple_of(g * half_depth, half_depth), half_depth),
            pl.ds(start_of(dst) + u * UNIT, UNIT),
        ]
        return remote(
            src, wgu.at[u, unit_band(me, g), pl.ds(mat * UNIT, UNIT)],
            wz_send, wz_recv.at[u, me], sp=dst,
        )

    def unit_in(u, src):
        block = wgu.at[u, unit_band(src, g)]
        return remote(block, block, wz_send, wz_recv.at[u, src], sp=src)

    def unit_y(u, src, half):
        block = wgu.at[u, unit_band(src, half)]
        return remote(block, block, wy_send, wy_recv.at[u], grp=1 - g)

    def send_units(me, dst, us):
        for u in us:
            if u >= first_unit(dst):
                for mat in range(2):
                    unit_z(mat, u, me, dst).start()

    def pass_units(me, u, *srcs):
        if u >= first_unit(me):
            for src in srcs:
                with sc(f"y{u}.{src}"):
                    unit_in(u, src).wait_recv()
                unit_y(u, src, g).start()

    def down_band(j, src, half, me):
        skip = first_unit(me) * UNIT
        size = (chunk - skip) // 2
        return wd.at[
            j, pl.ds(pl.multiple_of(skip + half * size, math.gcd(128, size)), size),
            pl.ds(src * dj, dj),
        ]

    def down_z(j, me, dst):
        skip = first_unit(dst) * UNIT
        size = (chunk - skip) // 2
        src = w_down_ref.at[
            pl.ds(pl.multiple_of(start_of(dst) + skip + g * size, math.gcd(128, size)), size),
            pl.ds(j * dj, dj),
        ]
        return remote(
            src, down_band(j, me, g, dst), dz_send, dz_recv.at[j, me], sp=dst
        )

    def down_y(j, src, half, me):
        block = down_band(j, src, half, me)
        return remote(block, block, dy_send, dy_recv.at[j], grp=1 - g)

    def send_down(me, j, *dsts):
        for dst in dsts:
            down_z(j, me, dst).start()

    def pass_down(me, j, *srcs):
        for src in srcs:
            block = down_band(j, src, g, me)
            with sc(f"d{j}.{src}"):
                remote(block, block, dz_send, dz_recv.at[j, src], sp=src).wait_recv()
            down_y(j, src, g, me).start()

    barrier = pltpu.get_barrier_semaphore()

    def greet(i):
        pl.semaphore_signal(barrier, inc=1, device_id={"sp": i}, device_id_type=MESH)

    each(0, s, greet)
    each(s + 1, ns, greet)
    pl.semaphore_signal(barrier, inc=1, device_id={"grp": 1 - g}, device_id_type=MESH)
    for j in range(1, nt):
        pl.semaphore_signal(barrier, inc=1, device_id={"tp": (t + j) % nt}, device_id_type=MESH)
    with sc("bar"):
        pl.semaphore_wait(barrier, ns + nt - 1)

    def kv_out(i, kk, vv):
        return (
            remote(kk, kbuf.at[i], kv_send.at[0], kv_recv.at[0, i], sp=s + 1),
            remote(vv, vbuf.at[i], kv_send.at[1], kv_recv.at[1, i], sp=s + 1),
        )

    def kv_in(i):
        return (
            remote(kbuf.at[i], kbuf.at[i], kv_send.at[0], kv_recv.at[0, i], sp=s - 1),
            remote(vbuf.at[i], vbuf.at[i], kv_send.at[1], kv_recv.at[1, i], sp=s - 1),
        )

    @pl.when(s + 1 < ns)
    def _():
        for copy in kv_out(0, k_ref, v_ref):
            copy.start()

    w_out_copy = pltpu.make_async_copy(w_out_ref, w_out, loc_sem.at[0])
    w_out_copy.start()

    def locals_(me):
        own = pl.ds(me * depth, depth)
        copies = []
        for mat in range(2):
            for u in range(nu):
                copies.append(
                    pltpu.make_async_copy(
                        (w_gate_ref, w_up_ref)[mat].at[:, pl.ds(start_of(me) + u * UNIT, UNIT)],
                        wgu.at[u, own, pl.ds(mat * UNIT, UNIT)], loc_sem.at[1 + 2 * u + mat],
                    )
                )
        for j in range(nj):
            copies.append(
                pltpu.make_async_copy(
                    w_down_ref.at[pl.ds(start_of(me), chunk), pl.ds(j * dj, dj)],
                    wd.at[j, :, pl.ds(me * dj, dj)], loc_sem.at[1 + 2 * nu + j],
                )
            )
        return copies

    early = range(nu - 1)
    late = range(nu - 1, nu)

    def opening(me):
        for u in early:
            for dst in range(me - 1, -1, -1):
                if u == 0 or dst != 1:
                    send_units(me, dst, (u,))
        if me == 0:
            send_units(0, 1, range(nu))
        for copy in locals_(me):
            copy.start()

    on_each_s(opening)

    if dup:

        @pl.when(s == ns - 1)
        def _():
            for j in range(nj):
                wd[j, :dup, : (ns - 1) * dj] = jnp.zeros((dup, (ns - 1) * dj), BF16)
            for k in range(ns):
                hidden[k, :, :dup] = jnp.zeros((tok, dup), BF16)

    gate_own = gate_t_ref[:, pl.ds(pl.multiple_of(s * tok, tok), tok)].T

    def attend(src, kk, vv, first):
        for h in range(nheads):
            lanes = slice(h * HEAD_DIM, (h + 1) * HEAD_DIM)
            scores = lax.dot_general(
                q_ref[:, lanes], kk[:, lanes], (((1,), (1,)), ((), ())), preferred_element_type=F32
            )
            key_gate = gate_t_ref[h : h + 1, pl.ds(pl.multiple_of(src * tok, tok), tok)]
            scores = scores * scale + gate_own[:, h : h + 1] - key_gate
            if first:
                row = lax.broadcasted_iota(jnp.int32, (tok, tok), 0)
                col = lax.broadcasted_iota(jnp.int32, (tok, tok), 1)
                scores = jnp.where(col <= row, scores, -1e30)
                new = jnp.max(scores, axis=-1, keepdims=True)
                w = jnp.where(col <= row, jnp.exp(scores - new), 0.0)
                tot[h] = jnp.sum(w, axis=-1, keepdims=True)
                acc[h] = jnp.dot(w.astype(BF16), vv[:, lanes], preferred_element_type=F32)
            else:
                old = top[h]
                new = jnp.maximum(old, jnp.max(scores, axis=-1, keepdims=True))
                w = jnp.exp(scores - new)
                shrink = jnp.exp(old - new)
                tot[h] = tot[h] * shrink + jnp.sum(w, axis=-1, keepdims=True)
                acc[h] = acc[h] * shrink + jnp.dot(
                    w.astype(BF16), vv[:, lanes], preferred_element_type=F32
                )
            top[h] = new

    with sc("att0"):
        attend(s, k_ref, v_ref, True)

    def earlier(i):
        for copy in kv_in(i - 1):
            copy.wait_recv()

        @pl.when(s + 1 < ns)
        def _():
            for copy in kv_out(i, kbuf.at[i - 1], vbuf.at[i - 1]):
                copy.start()

        attend(s - i, kbuf.at[i - 1], vbuf.at[i - 1], False)

    with sc("earlier"):
        each(1, s + 1, earlier)

    for h in range(nheads):
        att[:, h * HEAD_DIM : (h + 1) * HEAD_DIM] = (acc[h] / tot[h]).astype(BF16)

    def head_copy(j):
        dst = (t + j) % nt
        return remote(
            att.at[pl.ds(pl.multiple_of(dst * rows, rows), rows)], heads.at[j - 1],
            h_send, h_recv.at[j - 1], tp=dst,
        )

    for j in range(1, nt):
        head_copy(j).start()

    with sc("mix"):
        w_out_copy.wait()
        resid[...] = resid_ref[...].astype(F32) + jnp.dot(
            att[pl.ds(pl.multiple_of(t * rows, rows), rows), :],
            w_out[pl.ds(pl.multiple_of(t * att_w, att_w), att_w), :], preferred_element_type=F32,
        )

        def mix(j):
            head_copy(j).wait_recv()
            src = (t + nt - j) % nt
            resid[...] += jnp.dot(
                heads[j - 1], w_out[pl.ds(pl.multiple_of(src * att_w, att_w), att_w), :],
                preferred_element_type=F32,
            )

        each(1, nt, mix)
        full = resid[...]
        normed = full * lax.rsqrt(jnp.mean(full * full, axis=-1, keepdims=True) + 1e-06)
        nall[s, t] = (normed * gain_ref[...]).astype(BF16)

    part_rows = rows // 2

    def half_of(src, who, h):
        return nall.at[src, who, pl.ds(h * part_rows, part_rows)]

    def row_z(src, to, h):
        block = half_of(src, t, h)
        return remote(block, block, az_send, az_recv.at[src, h], sp=to)

    def row_x(src, who, h):
        block = half_of(src, who, h)
        return remote(block, block, ax_send, ax_recv.at[src, h], tp=tx)

    def row_c(kind, src, who, h):
        block = half_of(src, who, h)
        return remote(block, block, ac_send, ac_recv.at[kind, src, h], tp=tc)

    def spread(src, h):
        row_x(src, t, h).start()
        row_c(0, src, t, h).start()

    def relay(src):
        for h in range(2):
            row_x(src, tx, h).wait_recv()
            row_c(1, src, tx, h).start()

    def take(me, src):
        for h in range(2):
            with sc(f"take{src}.{h}"):
                row_z(src, me, h).wait_recv()
            if (me, src // 2) in ((1, 1), (2, 0)):
                row_z(src, me ^ 1, h).start()
            spread(src, h)

    def gather(me):
        near, mid = me ^ 1, 2 if me < 2 else 1
        for h in range(2):
            row_z(me, mid, h).start()
        for h in range(2):
            row_z(me, near, h).start()
            spread(me, h)
        last = nu - 1
        if me < 2:
            for u in range(nu):
                send_units(me, 2, (u,))
                send_units(me, 3, (u,))
        if me == 0:
            relay(0)
            for u in early:
                pass_units(0, u, 1, 2, 3)
            for u in late:
                pass_units(0, u, 1)
            take(0, 1)
            relay(1)
            for j in range(nj):
                send_down(0, j, 1)
            take(0, 2)
            for u in late:
                pass_units(0, u, 2, 3)
            take(0, 3)
            relay(2)
            pass_down(0, 0, 1)
            relay(3)
            send_down(0, 0, 2, 3)
        elif me == 1:
            send_units(1, 0, late)
            for j in range(nj):
                send_down(1, j, 0)
            for u in range(nu):
                pass_units(1, u, 0)
            relay(1)
            pass_units(1, 0, 2, 3)
            take(1, 0)
            take(1, 2)
            relay(0)
            take(1, 3)
            relay(2)
            for j in range(nj):
                send_down(1, j, 2, 3)
            pass_units(1, 1, 2)
            relay(3)
            pass_units(1, 1, 3)
            for u in range(2, nu):
                pass_units(1, u, 2, 3)
        elif me == 2:
            send_units(2, 0, late)
            send_units(2, 3, range(last))
            for u in early:
                pass_units(2, u, 3)
            relay(2)
            take(2, 0)
            send_units(2, 3, late)
            take(2, 1)
            pass_units(2, 0, 0)
            relay(0)
            send_units(2, 1, range(1, nu))
            pass_units(2, 1, 0)
            relay(1)
            for u in late:
                pass_units(2, u, 0, 3)
            pass_units(2, 0, 1)
            take(2, 3)
            send_down(2, 0, 0, 1)
            pass_units(2, 1, 1)
            relay(3)
            send_down(2, 0, 3)
            for j in range(1, nj):
                send_down(2, j, 3)
        else:
            send_units(3, 2, late)
            send_units(3, 0, late)
            relay(3)
            take(3, 2)
            pass_units(3, 0, 2, 0)
            pass_units(3, 1, 2, 0)
            relay(2)
            send_units(3, 1, range(1, nu))
            take(3, 0)
            pass_units(3, last, 0)
            send_down(3, 0, 0, 1)
            for j in range(nj):
                send_down(3, j, 2)
            relay(0)
            pass_units(3, 0, 1)
            pass_units(3, 1, 1)
            pass_units(3, last, 2)
            take(3, 1)
            pass_units(3, last, 1)
            relay(1)
            for j in range(1, nj):
                send_down(3, j, 0, 1)

    with sc("gather"):
        on_each_s(gather)

    def between(me, u):
        if u == 0:
            if me == 2:
                for i in late:
                    pass_units(2, i, 1)
                pass_down(2, 0, 3)
            elif me == 3:
                pass_down(3, 0, 2, 1)
            elif me == 1:
                pass_down(1, 0, 0)
            else:
                pass_down(0, 0, 2)
        elif u == 1:
            if me == 2:
                for j in range(1, nj):
                    send_down(2, j, 0, 1)
                pass_down(2, 0, 1, 0)
            elif me == 3:
                pass_down(3, 0, 0)
            elif me == 1:
                pass_down(1, 0, 2, 3)
            else:
                pass_down(0, 0, 3)
        elif u == nu - 1 and me == 0:
            for j in range(1, nj):
                send_down(0, j, 2, 3)

    def own_units(u):
        def body(me):
            copies = locals_(me)
            for mat in range(2):
                copies[mat * nu + u].wait()

        on_each_s(body)

    def own_down(j):
        on_each_s(lambda me: locals_(me)[2 * nu + j].wait())

    def twin_units(u):
        def body(me):
            if u >= first_unit(me):
                all_of = wgu.at[u, : (ns - 1) * half_depth]
                remote(all_of, all_of, wy_send, wy_recv.at[u], grp=1 - g).wait_recv()

        on_each_s(body)

    def twin_down(j):
        def body(me):
            all_of = wd.at[j, : (ns - 1) * ((chunk - first_unit(me) * UNIT) // 2) // ns]
            remote(all_of, all_of, dy_send, dy_recv.at[j], grp=1 - g).wait_recv()

        on_each_s(body)

    final = ns - 1 - 2 * (s // (ns - 1))

    def hide(u, low, high):
        def block(i):
            k = jnp.where(i == ns - 1, final, i + jnp.where(i >= final, 1, 0))
            y = jnp.dot(nall[k].reshape(tok, width), wgu[u], preferred_element_type=F32)
            gate, up = y[:, :UNIT], y[:, UNIT:]
            hidden[k, :, u * UNIT : (u + 1) * UNIT] = (gate / (1.0 + jnp.exp(-gate)) * up).astype(BF16)

        def run():
            each(low, high, block)

        if (u + 1) * UNIT <= dup:
            pl.when(s < ns - 1)(run)
        else:
            run()

    def rows_in(i):
        k = jnp.where(i == ns - 1, final, i + jnp.where(i >= final, 1, 0))
        for h in range(2):
            row_c(0, k, tc, h).wait_recv()
            row_c(1, k, (tc + 2) % 4, h).wait_recv()

    with sc("rows"):
        each(0, ns - 1, rows_in)
    for u in range(nu):
        with sc(f"tw{u}"):
            own_units(u)
            twin_units(u)
        with sc(f"hide{u}"):
            hide(u, 0, ns - 1)
        with sc(f"bt{u}"):
            on_each_s(lambda me, u=u: between(me, u))
    with sc("rowl"):
        rows_in(ns - 1)
    with sc("hidel"):
        for u in range(nu):
            hide(u, ns - 1, ns)

    def pass_down_all(j):
        on_each_s(lambda me: pass_down(me, j, me ^ 1, me ^ 2, me ^ 3))

    steps = [(0, m) for m in (3, 1, 2, 0)]
    steps += [(j, m) for j in range(1, nj - 2) for m in (3, 1, 2)]
    steps += [(j, m) for m in (3, 2, 1) for j in (nj - 2, nj - 1)]
    steps += [(j, 0) for j in range(1, nj)]
    nd = len(steps)
    at = {step: d for d, step in enumerate(steps)}
    slot = {d: i for i, d in enumerate(d for d in range(nd) if steps[d][1])}

    def sum_c(d):
        return remote(part.at[d, :, 1 - c], crecv.at[d], rc_send, rc_recv.at[d], tp=tc)

    def sum_x(d):
        return remote(csend.at[d], xrecv.at[d], rx_send, rx_recv.at[d], tp=tx)

    def sum_z(d):
        i = slot[d]
        to = xor(s, 2 if steps[d][1] == 2 else 1)
        return remote(zsend.at[i], zrecv.at[i], rz_send, rz_recv.at[i], sp=to)

    def stage_x(d):
        sum_c(d).wait_recv()
        csend[d] = (part[d, 1 - x, c].astype(F32) + crecv[d, 1 - x].astype(F32)).astype(BF16)
        sum_x(d).start()
        keep[d] = part[d, x, c].astype(F32) + crecv[d, x].astype(F32)

    def stage_z(d):
        j, m = steps[d]
        if m == 0:
            return
        sum_x(d).wait_recv()
        total = keep[d] + xrecv[d].astype(F32)
        if m == 2:
            from_near = at[j, 3]
            sum_z(from_near).wait_recv()
            total = total + zrecv[slot[from_near]].astype(F32)
        zsend[slot[d]] = total.astype(BF16)
        sum_z(d).start()

    def feed(d):
        j, m = steps[d]
        src = hidden[xor(s, m)]
        piece = math.gcd(wide, 512)

        def down(p):
            cols = pl.ds(pl.multiple_of(p * piece, piece), piece)
            y = jnp.dot(src, wd[j, :, cols], preferred_element_type=F32).astype(BF16)
            part[d, :, :, :, cols] = y.reshape(2, 2, rows, piece)

        each(0, wide // piece, down)
        sum_c(d).start()

    def finish(j):
        d, near, far = at[j, 0], at[j, 1], at[j, 2]
        sum_x(d).wait_recv()
        sum_z(near).wait_recv()
        sum_z(far).wait_recv()
        total = (
            keep[d] + xrecv[d].astype(F32) + zrecv[slot[near]].astype(F32)
            + zrecv[slot[far]].astype(F32)
        )
        for p in range(ns):
            cols = slice(p * depth + j * dj, p * depth + (j + 1) * dj)
            out_ref[:, cols] = (resid[:, cols] + total[:, p * dj : (p + 1) * dj]).astype(BF16)

    ready = set()
    for d in range(nd):
        j = steps[d][0]
        if j not in ready:
            ready.add(j)
            with sc(f"td{j}"):
                own_down(j)
                twin_down(j)
        with sc(f"f{d}"):
            feed(d)
            if d >= 1:
                stage_x(d - 1)
        if 2 <= d <= nj:
            with sc(f"pd{d - 1}"):
                pass_down_all(d - 1)
        if d >= 3:
            with sc(f"z{d}"):
                stage_z(d - 3)
    with sc("st"):
        stage_x(nd - 1)
        for d in range(nd - 3, nd):
            stage_z(d)
    for j in range(nj):
        with sc(f"fin{j}"):
            finish(j)

    def drain(me):
        if me + 1 < ns:
            for kind, buf in enumerate((kbuf, vbuf)):
                sent = buf.at[: me + 1]
                remote(sent, sent, kv_send.at[kind], kv_recv.at[kind, 0], tp=tx).wait_send()
        sent = nall.at[0, : 2 if me in (0, ns - 1) else 4]
        remote(sent, sent, az_send, az_recv.at[0, 0], tp=tx).wait_send()
        others = [i for i in range(ns) if i != me]
        for count, sem in (
            (sum(nu - first_unit(i) for i in others), wz_send),
            ((ns - 1) * (nu - first_unit(me)), wy_send),
        ):
            high = count * half_depth
            all_of = wgu.at[0, :high] if high <= width else wgu.at[:, : high // nu]
            remote(all_of, all_of, sem, wz_recv.at[0, me], grp=1 - g).wait_send()
        halves = [(chunk - first_unit(i) * UNIT) // 2 for i in range(ns)]
        for count, sem in (
            (sum(halves[i] for i in others), dz_send), ((ns - 1) * halves[me], dy_send)
        ):
            all_of = wd.at[:, : count // ns]
            remote(all_of, all_of, sem, dz_recv.at[0, me], grp=1 - g).wait_send()

    with sc("drain"):
        on_each_s(drain)
        remote(heads, heads, h_send, h_recv.at[0], tp=tx).wait_send()

        remote(nall.at[0], nall.at[0], ax_send, ax_recv.at[0, 0], tp=tx).wait_send()
        sent = nall.at[pl.ds(0, 2)]
        remote(sent, sent, ac_send, ac_recv.at[0, 0, 0], tp=tx).wait_send()
        remote(crecv, crecv, rc_send, rc_recv.at[0], tp=tc).wait_send()
        remote(xrecv, xrecv, rx_send, rx_recv.at[0], tp=tx).wait_send()
        remote(zrecv, zrecv, rz_send, rz_recv.at[0], tp=tx).wait_send()


def fused(ns, nt, chunk, nj, resid_in, queries, keys, values, cum_gate, w_out, norm_gain, w_gate, w_up, w_down):
    rows, width = resid_in.shape
    tok, att_w = queries.shape
    depth, units = w_gate.shape
    nheads = att_w // HEAD_DIM
    nu, nd, wide = chunk // UNIT, 4 * nj, width // nj
    vm = pl.BlockSpec(memory_space=pltpu.VMEM)
    hbm = pl.BlockSpec(memory_space=pltpu.HBM)
    dma = pltpu.SemaphoreType.DMA
    return pl.pallas_call(
        functools.partial(layer_kernel, (ns, nt, chunk, nj)),
        out_shape=jax.ShapeDtypeStruct((rows, width), BF16),
        in_specs=[vm] * 6 + [hbm] * 4,
        out_specs=vm,
        scratch_shapes=[
            pltpu.VMEM((ns - 1, tok, att_w), BF16),
            pltpu.VMEM((ns - 1, tok, att_w), BF16),
            pltpu.VMEM((nheads, tok, 1), F32),
            pltpu.VMEM((nheads, tok, 1), F32),
            pltpu.VMEM((nheads, tok, HEAD_DIM), F32),
            pltpu.VMEM((tok, att_w), BF16),
            pltpu.VMEM((nt - 1, rows, att_w), BF16),
            pltpu.VMEM(w_out.shape, BF16),
            pltpu.VMEM((rows, width), F32),
            pltpu.VMEM((ns, nt, rows, width), BF16),
            pltpu.VMEM((nu, width, 2 * UNIT), BF16),
            pltpu.VMEM((nj, chunk, wide), BF16),
            pltpu.VMEM((ns, tok, chunk), BF16),
            pltpu.VMEM((nd, 2, 2, rows, wide), BF16),
            pltpu.VMEM((nd, 2, rows, wide), BF16),
            pltpu.VMEM((nd, rows, wide), BF16),
            pltpu.VMEM((nd, rows, wide), F32),
            pltpu.VMEM((nd, rows, wide), BF16),
            pltpu.VMEM((3 * nj, rows, wide), BF16),
            pltpu.VMEM((3 * nj, rows, wide), BF16),
            dma((1 + 2 * nu + nj,)),
            dma((2,)), dma((2, ns - 1)),
            dma, dma((nu, ns)),
            dma, dma((nu,)),
            dma, dma((nj, ns)),
            dma, dma((nj,)),
            dma, dma((nt - 1,)),
            dma, dma((ns, 2)),
            dma, dma((ns, 2)),
            dma, dma((2, ns, 2)),
            dma, dma((nd,)),
            dma, dma((nd,)),
            dma, dma((3 * nj,)),
        ],
        compiler_params=pltpu.CompilerParams(
            collective_id=0, has_side_effects=True, vmem_limit_bytes=60 * 2**20
        ),
        name="layer",
    )(
        resid_in, queries, keys, values, cum_gate.T, norm_gain[None, :], w_out, w_gate,
        w_up, w_down,
    )


def pick(mesh):
    ng, ns, nt = (mesh.shape[a] for a in ("grp", "sp", "tp"))

    def step(*args):
        resid_in, queries, cum_gate, w_gate = args[0], args[1], args[4], args[7]
        rows, width = resid_in.shape
        depth, units = w_gate.shape
        chunk = -(-units // (128 * ns)) * 128
        need = 2 * ns * nt * rows * width * 4 + 6 * width * chunk + 2 * args[5].size
        fits = (
            ng == 2 and nt == 4 and ns == 4 and units % UNIT == 0 and chunk >= 2 * UNIT and depth % (128 * PIECES) == 0 and (ns - 1) * chunk < units
            and depth % 256 == 0 and width % 256 == 0 and (chunk - ns * chunk + units) % 32 == 0 and width == ns * depth and rows % 32 == 0
            and queries.shape[0] == rows * nt and queries.shape[0] % 128 == 0
            and cum_gate.shape[0] == ns * nt * rows and queries.shape[1] % 128 == 0
            and need < 40 * 2**20
        )
        if fits:
            return fused(ns, nt, chunk, PIECES, *args)
        return on_device(*args)

    return step


def solution(mesh):
    return jax.shard_map(
        pick(mesh),
        mesh=mesh,
        in_specs=(
            P(("grp", "sp", "tp"), None),
            P(("grp", "sp"), "tp"),
            P(("grp", "sp"), "tp"),
            P(("grp", "sp"), "tp"),
            P("grp", "tp"),
            P(),
            P(),
            P("sp", "tp"),
            P("sp", "tp"),
            P("tp", "sp"),
        ),
        out_specs=P(("grp", "sp", "tp"), None),
        check_vma=False,
    )
```

```python
import functools
import math

import jax
import jax.numpy as jnp
from jax import lax
from jax.experimental import pallas as pl
from jax.experimental.pallas import tpu as pltpu
from jax.sharding import PartitionSpec as P

HEAD_DIM = 64


def on_device(resid_in, queries, keys, values, cum_gate, w_out, norm_gain, w_gate, w_up, w_down):
    tok_rows = queries.shape[0]
    local_heads = queries.shape[1] // HEAD_DIM
    scale = HEAD_DIM ** (-0.5)
    offset = lax.axis_index("sp") * tok_rows
    query_heads = queries.reshape(tok_rows, local_heads, HEAD_DIM)
    own_gate = lax.dynamic_slice_in_dim(cum_gate, offset, tok_rows, 0).T
    query_pos = offset + jnp.arange(tok_rows, dtype=jnp.int32)
    last_pos = offset + tok_rows - 1
    initial = (
        jnp.full((local_heads, tok_rows), -1e30, jnp.float32),
        jnp.zeros((local_heads, tok_rows), jnp.float32),
        jnp.zeros((tok_rows, local_heads, HEAD_DIM), jnp.float32),
    )
    pair = lax.all_gather(jnp.stack([keys, values]), "sp", axis=1, tiled=True)
    key_piece, value_piece = pair[0], pair[1]
    length = key_piece.shape[0]
    span = math.gcd(length, 512)

    def block(index, state):
        begin = index * span

        def work(inner):
            maxima, totals, summed = inner
            key_block = lax.dynamic_slice_in_dim(key_piece, index * span, span, 0).reshape(
                span, local_heads, HEAD_DIM
            )
            value_block_rows = lax.dynamic_slice_in_dim(value_piece, index * span, span, 0).reshape(
                span, local_heads, HEAD_DIM
            )
            key_gate = lax.dynamic_slice_in_dim(cum_gate, begin, span, 0).T
            scores = (
                jnp.einsum(
                    "qhd,khd->hqk", query_heads, key_block, preferred_element_type=jnp.float32
                )
                * scale
            )
            scores = scores + own_gate[:, :, None] - key_gate[:, None, :]
            key_pos = begin + jnp.arange(span, dtype=jnp.int32)
            mask = (key_pos[None, :] <= query_pos[:, None])[None]
            scores = jnp.where(mask, scores, -1e30)
            new_max = jnp.maximum(maxima, jnp.max(scores, axis=-1))
            weights = jnp.where(mask, jnp.exp(scores - new_max[:, :, None]), 0.0)
            rescale = jnp.exp(maxima - new_max)
            totals = totals * rescale + jnp.sum(weights, axis=-1)
            product = jnp.einsum(
                "hqk,khd->qhd",
                weights.astype(jnp.bfloat16),
                value_block_rows,
                preferred_element_type=jnp.float32,
            )
            summed = summed * rescale.T[:, :, None] + product
            return (new_max, totals, summed)

        return lax.cond(begin <= last_pos, work, lambda inner: inner, state)

    maxima, totals, summed = lax.fori_loop(0, length // span, block, initial)
    attended = (
        (summed / totals.T[:, :, None])
        .reshape(tok_rows, local_heads * HEAD_DIM)
        .astype(jnp.bfloat16)
    )
    head_rows = lax.all_to_all(attended, "tp", split_axis=0, concat_axis=1, tiled=True)
    mixed = jnp.dot(head_rows, w_out, preferred_element_type=jnp.float32)
    resid = resid_in.astype(jnp.float32) + mixed
    normed = resid * lax.rsqrt(jnp.mean(resid * resid, axis=-1, keepdims=True) + 1e-06)
    normed = (normed * norm_gain).astype(jnp.bfloat16)
    all_rows = lax.all_gather(normed, ("sp", "tp"), axis=0, tiled=True)
    full_gate, full_up, full_down = (
        lax.all_to_all(w_gate, "sp", split_axis=1, concat_axis=0, tiled=True),
        lax.all_to_all(w_up, "sp", split_axis=1, concat_axis=0, tiled=True),
        lax.all_to_all(w_down, "sp", split_axis=0, concat_axis=1, tiled=True),
    )
    gate = jnp.dot(all_rows, full_gate, preferred_element_type=jnp.float32)
    up = jnp.dot(all_rows, full_up, preferred_element_type=jnp.float32)
    hidden = (jax.nn.silu(gate) * up).astype(jnp.bfloat16)
    terms = jnp.dot(hidden, full_down, preferred_element_type=jnp.float32)
    back = lax.psum_scatter(
        terms.astype(jnp.bfloat16), ("sp", "tp"), scatter_dimension=0, tiled=True
    ).astype(jnp.float32)
    return (resid + back).astype(jnp.bfloat16)


MESH = pl.DeviceIdType.MESH
F32 = jnp.float32
BF16 = jnp.bfloat16
UNIT = 128
PIECES = 4


def layer_kernel(
    dims, resid_hbm, q_hbm, k_hbm, v_hbm, gate_t_hbm, gain_hbm, w_out_ref, w_gate_ref,
    w_up_ref, w_down_ref, out_ref, resid_ref, q_ref, k_ref, v_ref, gate_t_ref, gain_ref, kbuf, vbuf, top, tot, acc, att, heads, w_out, resid, nall, wgu,
    wd, hidden, part, crecv, csend, keep, xrecv, zsend, zrecv, frecv, in_sem, loc_sem, kv_send, kv_recv, wz_send,
    wz_recv, wy_send, wy_recv, dz_send, dz_recv, dy_send, dy_recv, h_send, h_recv, az_send, az_recv,
    ax_send, ax_recv, ac_send, ac_recv, rc_send, rc_recv, rx_send, rx_recv, rz_send, rz_recv,
    rf_recv,
):
    ns, nt, chunk, nj = dims
    g, s, t = lax.axis_index("grp"), lax.axis_index("sp"), lax.axis_index("tp")
    rows, width = resid_hbm.shape
    tok, att_w = q_hbm.shape
    depth, units = w_gate_ref.shape
    nheads = att_w // HEAD_DIM
    half_depth = depth // 2
    dup = ns * chunk - units
    nu, dj = chunk // UNIT, depth // nj
    wide = ns * dj
    x, c = t // 2, t % 2
    tx = (t + 2) % 4
    tc = t + 1 - 2 * c
    scale = HEAD_DIM ** (-0.5)
    sc = jax.named_scope

    def start_of(i):
        return min(i * chunk, units - chunk)

    def first_unit(i):
        return dup // UNIT if i == ns - 1 else 0

    def remote(src, dst, send, recv, **where):
        return pltpu.make_async_remote_copy(
            src_ref=src, dst_ref=dst, send_sem=send, recv_sem=recv, device_id=where,
            device_id_type=MESH,
        )

    def xor(a, b):
        hi, lo, bh, bl = a // 2, a % 2, b // 2, b % 2
        return 2 * (hi + bh - 2 * hi * bh) + lo + bl - 2 * lo * bl

    def on_each_s(body):
        for k in range(ns):
            pl.when(s == k)(lambda k=k: (body(k), None)[1])

    def each(low, high, body):
        lax.fori_loop(low, high, lambda i, z: (body(i), z)[1], 0)

    def unit_band(src, half):
        return pl.ds(pl.multiple_of(src * depth + half * half_depth, half_depth), half_depth)

    def unit_z(mat, u, me, dst):
        src = (w_gate_ref, w_up_ref)[mat].at[
            pl.ds(pl.multiple_of(g * half_depth, half_depth), half_depth),
            pl.ds(start_of(dst) + u * UNIT, UNIT),
        ]
        return remote(
            src, wgu.at[u, unit_band(me, g), pl.ds(mat * UNIT, UNIT)],
            wz_send, wz_recv.at[u + (mat if u == nu - 1 else 0), me], sp=dst,
        )

    def unit_parts(u):
        return ((0, 0, UNIT), (1, UNIT, UNIT)) if u == nu - 1 else ((0, 0, 2 * UNIT),)

    def unit_in(u, src, part):
        i, low, size = part
        block = wgu.at[u, unit_band(src, g), pl.ds(low, size)]
        return remote(block, block, wz_send, wz_recv.at[u + i, src], sp=src)

    def unit_y(u, src, part):
        _, low, size = part
        block = wgu.at[u, unit_band(src, g), pl.ds(low, size)]
        return remote(block, block, wy_send, wy_recv.at[u], grp=1 - g)

    def send_units(me, dst, us):
        for u in us:
            if u >= first_unit(dst):
                for mat in range(2):
                    unit_z(mat, u, me, dst).start()

    def pass_units(me, u, *srcs):
        if u >= first_unit(me):
            for src in srcs:
                with sc(f"y{u}.{src}"):
                    for part in unit_parts(u):
                        unit_in(u, src, part).wait_recv()
                        unit_y(u, src, part).start()

    def down_band(j, src, half, me):
        skip = first_unit(me) * UNIT
        size = (chunk - skip) // 2
        return wd.at[
            j, pl.ds(pl.multiple_of(skip + half * size, math.gcd(128, size)), size),
            pl.ds(src * dj, dj),
        ]

    def down_z(j, me, dst):
        skip = first_unit(dst) * UNIT
        size = (chunk - skip) // 2
        src = w_down_ref.at[
            pl.ds(pl.multiple_of(start_of(dst) + skip + g * size, math.gcd(128, size)), size),
            pl.ds(j * dj, dj),
        ]
        return remote(
            src, down_band(j, me, g, dst), dz_send, dz_recv.at[j, me], sp=dst
        )

    def down_y(j, src, half, me):
        block = down_band(j, src, half, me)
        return remote(block, block, dy_send, dy_recv.at[j], grp=1 - g)

    def send_down(me, j, *dsts):
        for dst in dsts:
            down_z(j, me, dst).start()

    def pass_down(me, j, *srcs):
        for src in srcs:
            block = down_band(j, src, g, me)
            with sc(f"d{j}.{src}"):
                remote(block, block, dz_send, dz_recv.at[j, src], sp=src).wait_recv()
            down_y(j, src, g, me).start()

    inputs = [
        pltpu.make_async_copy(src, dst, in_sem.at[i])
        for i, (src, dst) in enumerate((
            (k_hbm, k_ref), (v_hbm, v_ref), (q_hbm, q_ref), (gate_t_hbm, gate_t_ref),
            (gain_hbm, gain_ref), (resid_hbm, resid_ref),
        ))
    ]
    for copy in inputs:
        copy.start()
    barrier = pltpu.get_barrier_semaphore()

    def greet(i):
        pl.semaphore_signal(barrier, inc=1, device_id={"sp": i}, device_id_type=MESH)

    each(0, s, greet)
    each(s + 1, ns, greet)
    pl.semaphore_signal(barrier, inc=1, device_id={"grp": 1 - g}, device_id_type=MESH)
    for j in range(1, nt):
        pl.semaphore_signal(barrier, inc=1, device_id={"tp": (t + j) % nt}, device_id_type=MESH)
    with sc("bar"):
        pl.semaphore_wait(barrier, ns + nt - 1)
        for copy in inputs[:4]:
            copy.wait()

    def kv_out(i, kk, vv):
        return (
            remote(kk, kbuf.at[i], kv_send.at[0], kv_recv.at[0, i], sp=s + 1),
            remote(vv, vbuf.at[i], kv_send.at[1], kv_recv.at[1, i], sp=s + 1),
        )

    def kv_in(i):
        return (
            remote(kbuf.at[i], kbuf.at[i], kv_send.at[0], kv_recv.at[0, i], sp=s - 1),
            remote(vbuf.at[i], vbuf.at[i], kv_send.at[1], kv_recv.at[1, i], sp=s - 1),
        )

    @pl.when(s + 1 < ns)
    def _():
        for copy in kv_out(0, k_ref, v_ref):
            copy.start()

    w_out_copy = pltpu.make_async_copy(w_out_ref, w_out, loc_sem.at[0])
    w_out_copy.start()

    def locals_(me):
        own = pl.ds(me * depth, depth)
        copies = []
        for mat in range(2):
            for u in range(nu):
                copies.append(
                    pltpu.make_async_copy(
                        (w_gate_ref, w_up_ref)[mat].at[:, pl.ds(start_of(me) + u * UNIT, UNIT)],
                        wgu.at[u, own, pl.ds(mat * UNIT, UNIT)], loc_sem.at[1 + 2 * u + mat],
                    )
                )
        for j in range(nj):
            copies.append(
                pltpu.make_async_copy(
                    w_down_ref.at[pl.ds(start_of(me), chunk), pl.ds(j * dj, dj)],
                    wd.at[j, :, pl.ds(me * dj, dj)], loc_sem.at[1 + 2 * nu + j],
                )
            )
        return copies

    early = range(nu - 1)
    late = range(nu - 1, nu)

    def opening(me):
        for u in early:
            for dst in range(me - 1, -1, -1):
                if u == 0 or dst != 1:
                    send_units(me, dst, (u,))
        if me == 0:
            send_units(0, 1, range(nu))
        for copy in locals_(me):
            copy.start()

    on_each_s(opening)

    if dup:

        @pl.when(s == ns - 1)
        def _():
            for j in range(nj):
                wd[j, :dup, : (ns - 1) * dj] = jnp.zeros((dup, (ns - 1) * dj), BF16)
            for k in range(ns):
                hidden[k, :, :dup] = jnp.zeros((tok, dup), BF16)

    gate_own = gate_t_ref[:, pl.ds(pl.multiple_of(s * tok, tok), tok)].T

    def attend(src, kk, vv, first):
        for h in range(nheads):
            lanes = slice(h * HEAD_DIM, (h + 1) * HEAD_DIM)
            scores = lax.dot_general(
                q_ref[:, lanes], kk[:, lanes], (((1,), (1,)), ((), ())), preferred_element_type=F32
            )
            key_gate = gate_t_ref[h : h + 1, pl.ds(pl.multiple_of(src * tok, tok), tok)]
            scores = scores * scale + gate_own[:, h : h + 1] - key_gate
            if first:
                row = lax.broadcasted_iota(jnp.int32, (tok, tok), 0)
                col = lax.broadcasted_iota(jnp.int32, (tok, tok), 1)
                scores = jnp.where(col <= row, scores, -1e30)
                new = jnp.max(scores, axis=-1, keepdims=True)
                w = jnp.where(col <= row, jnp.exp(scores - new), 0.0)
                tot[h] = jnp.sum(w, axis=-1, keepdims=True)
                acc[h] = jnp.dot(w.astype(BF16), vv[:, lanes], preferred_element_type=F32)
            else:
                old = top[h]
                new = jnp.maximum(old, jnp.max(scores, axis=-1, keepdims=True))
                w = jnp.exp(scores - new)
                shrink = jnp.exp(old - new)
                tot[h] = tot[h] * shrink + jnp.sum(w, axis=-1, keepdims=True)
                acc[h] = acc[h] * shrink + jnp.dot(
                    w.astype(BF16), vv[:, lanes], preferred_element_type=F32
                )
            top[h] = new

    with sc("att0"):
        attend(s, k_ref, v_ref, True)

    def earlier(i):
        for copy in kv_in(i - 1):
            copy.wait_recv()

        @pl.when(s + 1 < ns)
        def _():
            for copy in kv_out(i, kbuf.at[i - 1], vbuf.at[i - 1]):
                copy.start()

        attend(s - i, kbuf.at[i - 1], vbuf.at[i - 1], False)

    with sc("earlier"):
        each(1, s + 1, earlier)

    for h in range(nheads):
        att[:, h * HEAD_DIM : (h + 1) * HEAD_DIM] = (acc[h] / tot[h]).astype(BF16)

    def head_copy(j):
        dst = (t + j) % nt
        return remote(
            att.at[pl.ds(pl.multiple_of(dst * rows, rows), rows)], heads.at[j - 1],
            h_send, h_recv.at[j - 1], tp=dst,
        )

    for j in range(1, nt):
        head_copy(j).start()

    with sc("mix"):
        w_out_copy.wait()
        for copy in inputs[4:]:
            copy.wait()
        resid[...] = resid_ref[...].astype(F32) + jnp.dot(
            att[pl.ds(pl.multiple_of(t * rows, rows), rows), :],
            w_out[pl.ds(pl.multiple_of(t * att_w, att_w), att_w), :], preferred_element_type=F32,
        )

        def mix(j):
            head_copy(j).wait_recv()
            src = (t + nt - j) % nt
            resid[...] += jnp.dot(
                heads[j - 1], w_out[pl.ds(pl.multiple_of(src * att_w, att_w), att_w), :],
                preferred_element_type=F32,
            )

        each(1, nt, mix)
        full = resid[...]
        normed = full * lax.rsqrt(jnp.mean(full * full, axis=-1, keepdims=True) + 1e-06)
        nall[s, t] = (normed * gain_ref[...]).astype(BF16)

    part_rows = rows // 2

    def half_of(src, who, h):
        return nall.at[src, who, pl.ds(h * part_rows, part_rows)]

    def row_z(src, to, h):
        block = half_of(src, t, h)
        return remote(block, block, az_send, az_recv.at[src, h], sp=to)

    def row_x(src, who, h):
        block = half_of(src, who, h)
        return remote(block, block, ax_send, ax_recv.at[src, h], tp=tx)

    def row_c(kind, src, who, h):
        block = half_of(src, who, h)
        return remote(block, block, ac_send, ac_recv.at[kind, src, h], tp=tc)

    def spread(src, h):
        row_x(src, t, h).start()
        row_c(0, src, t, h).start()

    def relay(src):
        for h in range(2):
            row_x(src, tx, h).wait_recv()
            row_c(1, src, tx, h).start()

    def take(me, src):
        for h in range(2):
            with sc(f"take{src}.{h}"):
                row_z(src, me, h).wait_recv()
            if (me, src // 2) in ((1, 1), (2, 0)):
                row_z(src, me ^ 1, h).start()
            spread(src, h)

    def gather(me):
        near, mid = me ^ 1, 2 if me < 2 else 1
        for h in range(2):
            row_z(me, mid, h).start()
        for h in range(2):
            row_z(me, near, h).start()
            spread(me, h)
        last = nu - 1
        if me < 2:
            for u in range(nu):
                send_units(me, 2, (u,))
                send_units(me, 3, (u,))
        if me == 0:
            relay(0)
            for u in early:
                pass_units(0, u, 1, 2, 3)
            for u in late:
                pass_units(0, u, 1)
            take(0, 1)
            relay(1)
            for j in range(nj):
                send_down(0, j, 1)
            take(0, 2)
            for u in late:
                pass_units(0, u, 2, 3)
            take(0, 3)
            relay(2)
            pass_down(0, 0, 1)
            relay(3)
            send_down(0, 0, 2, 3)
        elif me == 1:
            send_units(1, 0, late)
            for j in range(nj):
                send_down(1, j, 0)
            for u in range(nu):
                pass_units(1, u, 0)
            relay(1)
            pass_units(1, 0, 2, 3)
            take(1, 0)
            take(1, 2)
            relay(0)
            take(1, 3)
            relay(2)
            for j in range(nj):
                send_down(1, j, 2, 3)
            pass_units(1, 1, 2)
            relay(3)
            pass_units(1, 1, 3)
            for u in range(2, nu):
                pass_units(1, u, 2, 3)
        elif me == 2:
            send_units(2, 0, late)
            send_units(2, 3, range(last))
            for u in early:
                pass_units(2, u, 3)
            relay(2)
            take(2, 0)
            send_units(2, 3, late)
            take(2, 1)
            pass_units(2, 0, 0)
            relay(0)
            send_units(2, 1, range(1, nu))
            pass_units(2, 1, 0)
            relay(1)
            for u in late:
                pass_units(2, u, 0, 3)
            pass_units(2, 0, 1)
            take(2, 3)
            send_down(2, 0, 0, 1)
            pass_units(2, 1, 1)
            relay(3)
            send_down(2, 0, 3)
            for j in range(1, nj):
                send_down(2, j, 3)
        else:
            send_units(3, 2, late)
            send_units(3, 0, late)
            relay(3)
            take(3, 2)
            pass_units(3, 0, 2, 0)
            pass_units(3, 1, 2, 0)
            relay(2)
            send_units(3, 1, range(1, nu))
            take(3, 0)
            pass_units(3, last, 0)
            send_down(3, 0, 0, 1)
            for j in range(nj):
                send_down(3, j, 2)
            relay(0)
            pass_units(3, 0, 1)
            pass_units(3, 1, 1)
            pass_units(3, last, 2)
            take(3, 1)
            pass_units(3, last, 1)
            relay(1)
            for j in range(1, nj):
                send_down(3, j, 0, 1)

    with sc("gather"):
        on_each_s(gather)

    def between(me, u):
        if u == 0:
            if me == 2:
                for i in late:
                    pass_units(2, i, 1)
                pass_down(2, 0, 3)
            elif me == 3:
                pass_down(3, 0, 2, 1)
            elif me == 1:
                pass_down(1, 0, 0)
            else:
                pass_down(0, 0, 2)
        elif u == 1:
            if me == 2:
                for j in range(1, nj):
                    send_down(2, j, 0, 1)
                pass_down(2, 0, 1, 0)
            elif me == 3:
                pass_down(3, 0, 0)
            elif me == 1:
                pass_down(1, 0, 2, 3)
            else:
                pass_down(0, 0, 3)
        elif u == nu - 1 and me == 0:
            for j in range(1, nj):
                send_down(0, j, 2, 3)
        if (me, u) in ((0, nu - 1), (1, nu - 1), (2, nu - 1), (3, 1)):
            for j in range(1, nj):
                pass_down(me, j, me ^ 1)

    def own_units(u):
        def body(me):
            copies = locals_(me)
            for mat in range(2):
                copies[mat * nu + u].wait()

        on_each_s(body)

    def own_down(j):
        on_each_s(lambda me: locals_(me)[2 * nu + j].wait())

    def twin_units(u):
        def body(me):
            if u >= first_unit(me):
                all_of = wgu.at[u, : (ns - 1) * half_depth]
                remote(all_of, all_of, wy_send, wy_recv.at[u], grp=1 - g).wait_recv()

        on_each_s(body)

    def twin_down(j):
        def body(me):
            all_of = wd.at[j, : (ns - 1) * ((chunk - first_unit(me) * UNIT) // 2) // ns]
            remote(all_of, all_of, dy_send, dy_recv.at[j], grp=1 - g).wait_recv()

        on_each_s(body)

    final = ns - 1 - 2 * (s // (ns - 1))

    def hide(u, low, high):
        def block(i):
            k = jnp.where(i == ns - 1, final, i + jnp.where(i >= final, 1, 0))
            y = jnp.dot(nall[k].reshape(tok, width), wgu[u], preferred_element_type=F32)
            gate, up = y[:, :UNIT], y[:, UNIT:]
            hidden[k, :, u * UNIT : (u + 1) * UNIT] = (gate / (1.0 + jnp.exp(-gate)) * up).astype(BF16)

        def run():
            each(low, high, block)

        if (u + 1) * UNIT <= dup:
            pl.when(s < ns - 1)(run)
        else:
            run()

    def rows_in(i):
        k = jnp.where(i == ns - 1, final, i + jnp.where(i >= final, 1, 0))
        for h in range(2):
            row_c(0, k, tc, h).wait_recv()
            row_c(1, k, (tc + 2) % 4, h).wait_recv()

    with sc("rows"):
        each(0, ns - 1, rows_in)
    for u in range(nu):
        with sc(f"tw{u}"):
            own_units(u)
            twin_units(u)
        with sc(f"hide{u}"):
            hide(u, 0, ns - 1)
        with sc(f"bt{u}"):
            on_each_s(lambda me, u=u: between(me, u))
    with sc("rowl"):
        rows_in(ns - 1)
    with sc("hidel"):
        for u in range(nu):
            hide(u, ns - 1, ns)

    def pass_down_all(j):
        on_each_s(lambda me: pass_down(me, j, me ^ 2, me ^ 3))

    steps = [(0, m) for m in (3, 1, 2, 0)]
    steps += [(j, m) for j in range(1, nj - 2) for m in (3, 1, 2)]
    steps += [(j, m) for m in (3, 2, 1) for j in (nj - 2, nj - 1)]
    steps += [(j, 0) for j in range(1, nj)]
    nd = len(steps)
    at = {step: d for d, step in enumerate(steps)}
    slot = {d: i for i, d in enumerate(d for d in range(nd) if steps[d][1])}

    def sum_c(d):
        return remote(part.at[d, :, 1 - c], crecv.at[d], rc_send, rc_recv.at[d], tp=tc)

    def sum_x(d):
        return remote(csend.at[d], xrecv.at[d], rx_send, rx_recv.at[d], tp=tx)

    def sum_near(d):
        i = slot[d]
        return remote(zsend.at[i], zrecv.at[i], rz_send, rz_recv.at[i], sp=xor(s, 1))

    def sum_on(d):
        j, m = steps[d]
        return remote(zsend.at[slot[d]], frecv.at[j], rz_send, rf_recv.at[j], sp=xor(s, m))

    middle = (s > 0) & (s < ns - 1)

    def stage_x(d):
        sum_c(d).wait_recv()
        csend[d] = (part[d, 1 - x, c].astype(F32) + crecv[d, 1 - x].astype(F32)).astype(BF16)
        sum_x(d).start()
        keep[d] = part[d, x, c].astype(F32) + crecv[d, x].astype(F32)

    def stage_z(d):
        m = steps[d][1]
        if m == 0:
            return
        sum_x(d).wait_recv()
        keep[d] = keep[d] + xrecv[d].astype(F32)

        @pl.when((m == 1) | ~middle)
        def _():
            zsend[slot[d]] = keep[d].astype(BF16)
            sum_near(d).start()

    def stage_on(d):
        j, m = steps[d]

        @pl.when(middle)
        def _():
            other = at[j, 5 - m]
            sum_near(other).wait_recv()
            zsend[slot[d]] = (keep[d] + zrecv[slot[other]].astype(F32)).astype(BF16)
            sum_on(d).start()

    def feed(d):
        j, m = steps[d]
        src = hidden[xor(s, m)]
        piece = math.gcd(wide, 512)

        def down(p):
            cols = pl.ds(pl.multiple_of(p * piece, piece), piece)
            y = jnp.dot(src, wd[j, :, cols], preferred_element_type=F32).astype(BF16)
            part[d, :, :, :, cols] = y.reshape(2, 2, rows, piece)

        each(0, wide // piece, down)
        sum_c(d).start()

    def finish(j):
        d, near = at[j, 0], at[j, 1]
        sum_x(d).wait_recv()
        sum_near(near).wait_recv()
        remote(frecv.at[j], frecv.at[j], rz_send, rf_recv.at[j], sp=xor(s, 1)).wait_recv()
        total = (
            keep[d] + xrecv[d].astype(F32) + zrecv[slot[near]].astype(F32) + frecv[j].astype(F32)
        )
        for p in range(ns):
            cols = slice(p * depth + j * dj, p * depth + (j + 1) * dj)
            out_ref[:, cols] = (resid[:, cols] + total[:, p * dj : (p + 1) * dj]).astype(BF16)

    def on_time(i):
        j, m = steps[i]
        return {2: at[j, 2] + 4, 3: at[j, 2] + 7}.get(m, -1)

    ready = set()
    for d in range(nd):
        j = steps[d][0]
        if j not in ready:
            ready.add(j)
            with sc(f"td{j}"):
                own_down(j)
                twin_down(j)
        with sc(f"f{d}"):
            feed(d)
            if d >= 1:
                stage_x(d - 1)
        ahead = d - 1 if 2 <= d <= nj else nj
        if ahead < nj:
            with sc(f"pd{ahead}"):
                pass_down_all(ahead)
        for i in range(nd):
            if d == i + 4:
                with sc(f"z{i}"):
                    stage_z(i)
        for i in range(nd):
            if d == on_time(i):
                with sc(f"o{i}"):
                    stage_on(i)
    with sc("st"):
        stage_x(nd - 1)
        for d in range(nd, nd + 4):
            stage_z(d - 4)
            for i in range(nd):
                if d == on_time(i):
                    stage_on(i)
    for j in range(nj):
        with sc(f"fin{j}"):
            finish(j)

    def drain(me):
        if me + 1 < ns:
            for kind, buf in enumerate((kbuf, vbuf)):
                sent = buf.at[: me + 1]
                remote(sent, sent, kv_send.at[kind], kv_recv.at[kind, 0], tp=tx).wait_send()
        sent = nall.at[0, : 2 if me in (0, ns - 1) else 4]
        remote(sent, sent, az_send, az_recv.at[0, 0], tp=tx).wait_send()
        others = [i for i in range(ns) if i != me]
        for count, sem in (
            (sum(nu - first_unit(i) for i in others), wz_send),
            ((ns - 1) * (nu - first_unit(me)), wy_send),
        ):
            high = count * half_depth
            all_of = wgu.at[0, :high] if high <= width else wgu.at[:, : high // nu]
            remote(all_of, all_of, sem, wz_recv.at[0, me], grp=1 - g).wait_send()
        halves = [(chunk - first_unit(i) * UNIT) // 2 for i in range(ns)]
        for count, sem in (
            (sum(halves[i] for i in others), dz_send), ((ns - 1) * halves[me], dy_send)
        ):
            all_of = wd.at[:, : count // ns]
            remote(all_of, all_of, sem, dz_recv.at[0, me], grp=1 - g).wait_send()

    with sc("drain"):
        on_each_s(drain)
        remote(heads, heads, h_send, h_recv.at[0], tp=tx).wait_send()

        remote(nall.at[0], nall.at[0], ax_send, ax_recv.at[0, 0], tp=tx).wait_send()
        sent = nall.at[pl.ds(0, 2)]
        remote(sent, sent, ac_send, ac_recv.at[0, 0, 0], tp=tx).wait_send()
        remote(crecv, crecv, rc_send, rc_recv.at[0], tp=tc).wait_send()
        remote(xrecv, xrecv, rx_send, rx_recv.at[0], tp=tx).wait_send()
        remote(zrecv, zrecv, rz_send, rz_recv.at[0], tp=tx).wait_send()


def fused(ns, nt, chunk, nj, resid_in, queries, keys, values, cum_gate, w_out, norm_gain, w_gate, w_up, w_down):
    rows, width = resid_in.shape
    tok, att_w = queries.shape
    depth, units = w_gate.shape
    nheads = att_w // HEAD_DIM
    nu, nd, wide = chunk // UNIT, 4 * nj, width // nj
    vm = pl.BlockSpec(memory_space=pltpu.VMEM)
    hbm = pl.BlockSpec(memory_space=pltpu.HBM)
    dma = pltpu.SemaphoreType.DMA
    return pl.pallas_call(
        functools.partial(layer_kernel, (ns, nt, chunk, nj)),
        out_shape=jax.ShapeDtypeStruct((rows, width), BF16),
        in_specs=[hbm] * 10,
        out_specs=vm,
        scratch_shapes=[
            pltpu.VMEM((rows, width), BF16),
            pltpu.VMEM((tok, att_w), BF16),
            pltpu.VMEM((tok, att_w), BF16),
            pltpu.VMEM((tok, att_w), BF16),
            pltpu.VMEM(cum_gate.shape[::-1], F32),
            pltpu.VMEM((1, width), F32),
            pltpu.VMEM((ns - 1, tok, att_w), BF16),
            pltpu.VMEM((ns - 1, tok, att_w), BF16),
            pltpu.VMEM((nheads, tok, 1), F32),
            pltpu.VMEM((nheads, tok, 1), F32),
            pltpu.VMEM((nheads, tok, HEAD_DIM), F32),
            pltpu.VMEM((tok, att_w), BF16),
            pltpu.VMEM((nt - 1, rows, att_w), BF16),
            pltpu.VMEM(w_out.shape, BF16),
            pltpu.VMEM((rows, width), F32),
            pltpu.VMEM((ns, nt, rows, width), BF16),
            pltpu.VMEM((nu, width, 2 * UNIT), BF16),
            pltpu.VMEM((nj, chunk, wide), BF16),
            pltpu.VMEM((ns, tok, chunk), BF16),
            pltpu.VMEM((nd, 2, 2, rows, wide), BF16),
            pltpu.VMEM((nd, 2, rows, wide), BF16),
            pltpu.VMEM((nd, rows, wide), BF16),
            pltpu.VMEM((nd, rows, wide), F32),
            pltpu.VMEM((nd, rows, wide), BF16),
            pltpu.VMEM((3 * nj, rows, wide), BF16),
            pltpu.VMEM((3 * nj, rows, wide), BF16),
            pltpu.VMEM((nj, rows, wide), BF16),
            dma((6,)),
            dma((1 + 2 * nu + nj,)),
            dma((2,)), dma((2, ns - 1)),
            dma, dma((nu + 1, ns)),
            dma, dma((nu,)),
            dma, dma((nj, ns)),
            dma, dma((nj,)),
            dma, dma((nt - 1,)),
            dma, dma((ns, 2)),
            dma, dma((ns, 2)),
            dma, dma((2, ns, 2)),
            dma, dma((nd,)),
            dma, dma((nd,)),
            dma, dma((3 * nj,)),
            dma((nj,)),
        ],
        compiler_params=pltpu.CompilerParams(
            collective_id=0, has_side_effects=True, vmem_limit_bytes=60 * 2**20
        ),
        name="layer",
    )(
        resid_in, queries, keys, values, cum_gate.T, norm_gain[None, :], w_out, w_gate,
        w_up, w_down,
    )


def pick(mesh):
    ng, ns, nt = (mesh.shape[a] for a in ("grp", "sp", "tp"))

    def step(*args):
        resid_in, queries, cum_gate, w_gate = args[0], args[1], args[4], args[7]
        rows, width = resid_in.shape
        depth, units = w_gate.shape
        chunk = -(-units // (128 * ns)) * 128
        need = 2 * ns * nt * rows * width * 4 + 6 * width * chunk + 2 * args[5].size
        fits = (
            ng == 2 and nt == 4 and ns == 4 and units % UNIT == 0 and chunk >= 2 * UNIT and depth % (128 * PIECES) == 0 and (ns - 1) * chunk < units
            and depth % 256 == 0 and width % 256 == 0 and (chunk - ns * chunk + units) % 32 == 0 and width == ns * depth and rows % 32 == 0
            and queries.shape[0] == rows * nt and queries.shape[0] % 128 == 0
            and cum_gate.shape[0] == ns * nt * rows and queries.shape[1] % 128 == 0
            and need < 40 * 2**20
        )
        if fits:
            return fused(ns, nt, chunk, PIECES, *args)
        return on_device(*args)

    return step


def solution(mesh):
    return jax.shard_map(
        pick(mesh),
        mesh=mesh,
        in_specs=(
            P(("grp", "sp", "tp"), None),
            P(("grp", "sp"), "tp"),
            P(("grp", "sp"), "tp"),
            P(("grp", "sp"), "tp"),
            P("grp", "tp"),
            P(),
            P(),
            P("sp", "tp"),
            P("sp", "tp"),
            P("tp", "sp"),
        ),
        out_specs=P(("grp", "sp", "tp"), None),
        check_vma=False,
    )
```

```python
import functools
import math

import jax
import jax.numpy as jnp
from jax import lax
from jax.experimental import pallas as pl
from jax.experimental.pallas import tpu as pltpu
from jax.sharding import PartitionSpec as P

HEAD_DIM = 64


def on_device(resid_in, queries, keys, values, cum_gate, w_out, norm_gain, w_gate, w_up, w_down):
    tok_rows = queries.shape[0]
    local_heads = queries.shape[1] // HEAD_DIM
    scale = HEAD_DIM ** (-0.5)
    offset = lax.axis_index("sp") * tok_rows
    query_heads = queries.reshape(tok_rows, local_heads, HEAD_DIM)
    own_gate = lax.dynamic_slice_in_dim(cum_gate, offset, tok_rows, 0).T
    query_pos = offset + jnp.arange(tok_rows, dtype=jnp.int32)
    last_pos = offset + tok_rows - 1
    initial = (
        jnp.full((local_heads, tok_rows), -1e30, jnp.float32),
        jnp.zeros((local_heads, tok_rows), jnp.float32),
        jnp.zeros((tok_rows, local_heads, HEAD_DIM), jnp.float32),
    )
    pair = lax.all_gather(jnp.stack([keys, values]), "sp", axis=1, tiled=True)
    key_piece, value_piece = pair[0], pair[1]
    length = key_piece.shape[0]
    span = math.gcd(length, 512)

    def block(index, state):
        begin = index * span

        def work(inner):
            maxima, totals, summed = inner
            key_block = lax.dynamic_slice_in_dim(key_piece, index * span, span, 0).reshape(
                span, local_heads, HEAD_DIM
            )
            value_block_rows = lax.dynamic_slice_in_dim(value_piece, index * span, span, 0).reshape(
                span, local_heads, HEAD_DIM
            )
            key_gate = lax.dynamic_slice_in_dim(cum_gate, begin, span, 0).T
            scores = (
                jnp.einsum(
                    "qhd,khd->hqk", query_heads, key_block, preferred_element_type=jnp.float32
                )
                * scale
            )
            scores = scores + own_gate[:, :, None] - key_gate[:, None, :]
            key_pos = begin + jnp.arange(span, dtype=jnp.int32)
            mask = (key_pos[None, :] <= query_pos[:, None])[None]
            scores = jnp.where(mask, scores, -1e30)
            new_max = jnp.maximum(maxima, jnp.max(scores, axis=-1))
            weights = jnp.where(mask, jnp.exp(scores - new_max[:, :, None]), 0.0)
            rescale = jnp.exp(maxima - new_max)
            totals = totals * rescale + jnp.sum(weights, axis=-1)
            product = jnp.einsum(
                "hqk,khd->qhd",
                weights.astype(jnp.bfloat16),
                value_block_rows,
                preferred_element_type=jnp.float32,
            )
            summed = summed * rescale.T[:, :, None] + product
            return (new_max, totals, summed)

        return lax.cond(begin <= last_pos, work, lambda inner: inner, state)

    maxima, totals, summed = lax.fori_loop(0, length // span, block, initial)
    attended = (
        (summed / totals.T[:, :, None])
        .reshape(tok_rows, local_heads * HEAD_DIM)
        .astype(jnp.bfloat16)
    )
    head_rows = lax.all_to_all(attended, "tp", split_axis=0, concat_axis=1, tiled=True)
    mixed = jnp.dot(head_rows, w_out, preferred_element_type=jnp.float32)
    resid = resid_in.astype(jnp.float32) + mixed
    normed = resid * lax.rsqrt(jnp.mean(resid * resid, axis=-1, keepdims=True) + 1e-06)
    normed = (normed * norm_gain).astype(jnp.bfloat16)
    all_rows = lax.all_gather(normed, ("sp", "tp"), axis=0, tiled=True)
    full_gate, full_up, full_down = (
        lax.all_to_all(w_gate, "sp", split_axis=1, concat_axis=0, tiled=True),
        lax.all_to_all(w_up, "sp", split_axis=1, concat_axis=0, tiled=True),
        lax.all_to_all(w_down, "sp", split_axis=0, concat_axis=1, tiled=True),
    )
    gate = jnp.dot(all_rows, full_gate, preferred_element_type=jnp.float32)
    up = jnp.dot(all_rows, full_up, preferred_element_type=jnp.float32)
    hidden = (jax.nn.silu(gate) * up).astype(jnp.bfloat16)
    terms = jnp.dot(hidden, full_down, preferred_element_type=jnp.float32)
    back = lax.psum_scatter(
        terms.astype(jnp.bfloat16), ("sp", "tp"), scatter_dimension=0, tiled=True
    ).astype(jnp.float32)
    return (resid + back).astype(jnp.bfloat16)


MESH = pl.DeviceIdType.MESH
F32 = jnp.float32
BF16 = jnp.bfloat16
UNIT = 128
PIECES = 4


def layer_kernel(
    dims, resid_hbm, q_hbm, k_hbm, v_hbm, gate_t_hbm, gain_hbm, w_out_ref, w_gate_ref,
    w_up_ref, w_down_ref, out_ref, resid_ref, q_ref, k_ref, v_ref, gate_t_ref, gain_ref, kbuf, vbuf, top, tot, acc, att, heads, w_out, resid, nall, wgu,
    wd, hidden, part, crecv, csend, keep, xrecv, zsend, zrecv, frecv, in_sem, loc_sem, kv_send, kv_recv, wz_send,
    wz_recv, wy_send, wy_recv, dz_send, dz_recv, dy_send, dy_recv, h_send, h_recv, az_send, az_recv,
    ax_send, ax_recv, ac_send, ac_recv, rc_send, rc_recv, rx_send, rx_recv, rz_send, rz_recv,
    rf_recv,
):
    ns, nt, chunk, nj = dims
    g, s, t = lax.axis_index("grp"), lax.axis_index("sp"), lax.axis_index("tp")
    rows, width = resid_hbm.shape
    tok, att_w = q_hbm.shape
    depth, units = w_gate_ref.shape
    nheads = att_w // HEAD_DIM
    half_depth = depth // 2
    dup = ns * chunk - units
    nu, dj = chunk // UNIT, depth // nj
    wide = ns * dj
    x, c = t // 2, t % 2
    tx = (t + 2) % 4
    tc = t + 1 - 2 * c
    scale = HEAD_DIM ** (-0.5)
    sc = jax.named_scope

    def start_of(i):
        return min(i * chunk, units - chunk)

    def first_unit(i):
        return dup // UNIT if i == ns - 1 else 0

    def remote(src, dst, send, recv, **where):
        return pltpu.make_async_remote_copy(
            src_ref=src, dst_ref=dst, send_sem=send, recv_sem=recv, device_id=where,
            device_id_type=MESH,
        )

    def xor(a, b):
        hi, lo, bh, bl = a // 2, a % 2, b // 2, b % 2
        return 2 * (hi + bh - 2 * hi * bh) + lo + bl - 2 * lo * bl

    def on_each_s(body):
        for k in range(ns):
            pl.when(s == k)(lambda k=k: (body(k), None)[1])

    def each(low, high, body):
        lax.fori_loop(low, high, lambda i, z: (body(i), z)[1], 0)

    def unit_band(src, half):
        return pl.ds(pl.multiple_of(src * depth + half * half_depth, half_depth), half_depth)

    def unit_z(mat, u, me, dst):
        src = (w_gate_ref, w_up_ref)[mat].at[
            pl.ds(pl.multiple_of(g * half_depth, half_depth), half_depth),
            pl.ds(start_of(dst) + u * UNIT, UNIT),
        ]
        return remote(
            src, wgu.at[u, unit_band(me, g), pl.ds(mat * UNIT, UNIT)],
            wz_send, wz_recv.at[u + (mat if u == nu - 1 else 0), me], sp=dst,
        )

    def unit_parts(u):
        return ((0, 0, UNIT), (1, UNIT, UNIT)) if u == nu - 1 else ((0, 0, 2 * UNIT),)

    def unit_in(u, src, part):
        i, low, size = part
        block = wgu.at[u, unit_band(src, g), pl.ds(low, size)]
        return remote(block, block, wz_send, wz_recv.at[u + i, src], sp=src)

    def unit_y(u, src, part):
        _, low, size = part
        block = wgu.at[u, unit_band(src, g), pl.ds(low, size)]
        return remote(block, block, wy_send, wy_recv.at[u], grp=1 - g)

    def send_units(me, dst, us):
        for u in us:
            if u >= first_unit(dst):
                for mat in range(2):
                    unit_z(mat, u, me, dst).start()

    def pass_units(me, u, *srcs):
        if u >= first_unit(me):
            for src in srcs:
                with sc(f"y{u}.{src}"):
                    for part in unit_parts(u):
                        unit_in(u, src, part).wait_recv()
                        unit_y(u, src, part).start()

    def down_band(j, src, half, me):
        skip = first_unit(me) * UNIT
        size = (chunk - skip) // 2
        return wd.at[
            j, pl.ds(pl.multiple_of(skip + half * size, math.gcd(128, size)), size),
            pl.ds(src * dj, dj),
        ]

    def down_z(j, me, dst):
        skip = first_unit(dst) * UNIT
        size = (chunk - skip) // 2
        src = w_down_ref.at[
            pl.ds(pl.multiple_of(start_of(dst) + skip + g * size, math.gcd(128, size)), size),
            pl.ds(j * dj, dj),
        ]
        return remote(
            src, down_band(j, me, g, dst), dz_send, dz_recv.at[j, me], sp=dst
        )

    def down_y(j, src, half, me):
        block = down_band(j, src, half, me)
        return remote(block, block, dy_send, dy_recv.at[j], grp=1 - g)

    def send_down(me, j, *dsts):
        for dst in dsts:
            down_z(j, me, dst).start()

    def pass_down(me, j, *srcs):
        for src in srcs:
            block = down_band(j, src, g, me)
            with sc(f"d{j}.{src}"):
                remote(block, block, dz_send, dz_recv.at[j, src], sp=src).wait_recv()
            down_y(j, src, g, me).start()

    inputs = [
        pltpu.make_async_copy(src, dst, in_sem.at[i])
        for i, (src, dst) in enumerate((
            (k_hbm, k_ref), (v_hbm, v_ref), (q_hbm, q_ref), (gate_t_hbm, gate_t_ref),
            (gain_hbm, gain_ref), (resid_hbm, resid_ref),
        ))
    ]
    for copy in inputs:
        copy.start()
    barrier = pltpu.get_barrier_semaphore()

    def greet(i):
        pl.semaphore_signal(barrier, inc=1, device_id={"sp": i}, device_id_type=MESH)

    each(0, s, greet)
    each(s + 1, ns, greet)
    pl.semaphore_signal(barrier, inc=1, device_id={"grp": 1 - g}, device_id_type=MESH)
    for j in range(1, nt):
        pl.semaphore_signal(barrier, inc=1, device_id={"tp": (t + j) % nt}, device_id_type=MESH)
    with sc("bar"):
        pl.semaphore_wait(barrier, ns + nt - 1)
        for copy in inputs[:4]:
            copy.wait()

    def kv_out(i, kk, vv):
        return (
            remote(kk, kbuf.at[i], kv_send.at[0], kv_recv.at[0, i], sp=s + 1),
            remote(vv, vbuf.at[i], kv_send.at[1], kv_recv.at[1, i], sp=s + 1),
        )

    def kv_in(i):
        return (
            remote(kbuf.at[i], kbuf.at[i], kv_send.at[0], kv_recv.at[0, i], sp=s - 1),
            remote(vbuf.at[i], vbuf.at[i], kv_send.at[1], kv_recv.at[1, i], sp=s - 1),
        )

    @pl.when(s + 1 < ns)
    def _():
        for copy in kv_out(0, k_ref, v_ref):
            copy.start()

    w_out_copy = pltpu.make_async_copy(w_out_ref, w_out, loc_sem.at[0])
    w_out_copy.start()

    def locals_(me):
        own = pl.ds(me * depth, depth)
        copies = []
        for mat in range(2):
            for u in range(nu):
                copies.append(
                    pltpu.make_async_copy(
                        (w_gate_ref, w_up_ref)[mat].at[:, pl.ds(start_of(me) + u * UNIT, UNIT)],
                        wgu.at[u, own, pl.ds(mat * UNIT, UNIT)], loc_sem.at[1 + 2 * u + mat],
                    )
                )
        for j in range(nj):
            copies.append(
                pltpu.make_async_copy(
                    w_down_ref.at[pl.ds(start_of(me), chunk), pl.ds(j * dj, dj)],
                    wd.at[j, :, pl.ds(me * dj, dj)], loc_sem.at[1 + 2 * nu + j],
                )
            )
        return copies

    early = range(nu - 1)
    late = range(nu - 1, nu)

    def opening(me):
        for u in early:
            for dst in range(me - 1, -1, -1):
                if u == 0 or dst != 1:
                    send_units(me, dst, (u,))
        if me == 0:
            send_units(0, 1, range(nu))
        for copy in locals_(me):
            copy.start()

    on_each_s(opening)

    if dup:

        @pl.when(s == ns - 1)
        def _():
            for j in range(nj):
                wd[j, :dup, : (ns - 1) * dj] = jnp.zeros((dup, (ns - 1) * dj), BF16)
            for k in range(ns):
                hidden[k, :, :dup] = jnp.zeros((tok, dup), BF16)

    gate_own = gate_t_ref[:, pl.ds(pl.multiple_of(s * tok, tok), tok)].T

    def attend(src, kk, vv, first):
        for h in range(nheads):
            lanes = slice(h * HEAD_DIM, (h + 1) * HEAD_DIM)
            scores = lax.dot_general(
                q_ref[:, lanes], kk[:, lanes], (((1,), (1,)), ((), ())), preferred_element_type=F32
            )
            key_gate = gate_t_ref[h : h + 1, pl.ds(pl.multiple_of(src * tok, tok), tok)]
            scores = scores * scale + gate_own[:, h : h + 1] - key_gate
            if first:
                row = lax.broadcasted_iota(jnp.int32, (tok, tok), 0)
                col = lax.broadcasted_iota(jnp.int32, (tok, tok), 1)
                scores = jnp.where(col <= row, scores, -1e30)
                new = jnp.max(scores, axis=-1, keepdims=True)
                w = jnp.where(col <= row, jnp.exp(scores - new), 0.0)
                tot[h] = jnp.sum(w, axis=-1, keepdims=True)
                acc[h] = jnp.dot(w.astype(BF16), vv[:, lanes], preferred_element_type=F32)
            else:
                old = top[h]
                new = jnp.maximum(old, jnp.max(scores, axis=-1, keepdims=True))
                w = jnp.exp(scores - new)
                shrink = jnp.exp(old - new)
                tot[h] = tot[h] * shrink + jnp.sum(w, axis=-1, keepdims=True)
                acc[h] = acc[h] * shrink + jnp.dot(
                    w.astype(BF16), vv[:, lanes], preferred_element_type=F32
                )
            top[h] = new

    with sc("att0"):
        attend(s, k_ref, v_ref, True)

    def earlier(i):
        for copy in kv_in(i - 1):
            copy.wait_recv()

        @pl.when(s + 1 < ns)
        def _():
            for copy in kv_out(i, kbuf.at[i - 1], vbuf.at[i - 1]):
                copy.start()

        attend(s - i, kbuf.at[i - 1], vbuf.at[i - 1], False)

    with sc("earlier"):
        each(1, s + 1, earlier)

    for h in range(nheads):
        att[:, h * HEAD_DIM : (h + 1) * HEAD_DIM] = (acc[h] / tot[h]).astype(BF16)

    def head_copy(j):
        dst = (t + j) % nt
        return remote(
            att.at[pl.ds(pl.multiple_of(dst * rows, rows), rows)], heads.at[j - 1],
            h_send, h_recv.at[j - 1], tp=dst,
        )

    for j in range(1, nt):
        head_copy(j).start()

    with sc("mix"):
        w_out_copy.wait()
        for copy in inputs[4:]:
            copy.wait()
        resid[...] = resid_ref[...].astype(F32) + jnp.dot(
            att[pl.ds(pl.multiple_of(t * rows, rows), rows), :],
            w_out[pl.ds(pl.multiple_of(t * att_w, att_w), att_w), :], preferred_element_type=F32,
        )

        def mix(j):
            head_copy(j).wait_recv()
            src = (t + nt - j) % nt
            resid[...] += jnp.dot(
                heads[j - 1], w_out[pl.ds(pl.multiple_of(src * att_w, att_w), att_w), :],
                preferred_element_type=F32,
            )

        each(1, nt, mix)
        full = resid[...]
        normed = full * lax.rsqrt(jnp.mean(full * full, axis=-1, keepdims=True) + 1e-06)
        nall[s, t] = (normed * gain_ref[...]).astype(BF16)

    part_rows = rows // 2

    def half_of(src, who, h):
        return nall.at[src, who, pl.ds(h * part_rows, part_rows)]

    def row_z(src, to, h):
        block = half_of(src, t, h)
        return remote(block, block, az_send, az_recv.at[src, h], sp=to)

    def row_x(src, who, h):
        block = half_of(src, who, h)
        return remote(block, block, ax_send, ax_recv.at[src, h], tp=tx)

    def row_c(kind, src, who, h):
        block = half_of(src, who, h)
        return remote(block, block, ac_send, ac_recv.at[kind, src, h], tp=tc)

    def spread(src, h):
        row_x(src, t, h).start()
        row_c(0, src, t, h).start()

    def relay(src):
        for h in range(2):
            row_x(src, tx, h).wait_recv()
            row_c(1, src, tx, h).start()

    def take(me, src):
        for h in range(2):
            with sc(f"take{src}.{h}"):
                row_z(src, me, h).wait_recv()
            if (me, src // 2) in ((1, 1), (2, 0)):
                row_z(src, me ^ 1, h).start()
            spread(src, h)

    def gather(me):
        near, mid = me ^ 1, 2 if me < 2 else 1
        for h in range(2):
            row_z(me, mid, h).start()
        for h in range(2):
            row_z(me, near, h).start()
            spread(me, h)
        last = nu - 1
        if me < 2:
            for u in range(nu):
                send_units(me, 2, (u,))
                send_units(me, 3, (u,))
        if me == 0:
            relay(0)
            for u in early:
                pass_units(0, u, 1, 2, 3)
            for u in late:
                pass_units(0, u, 1)
            take(0, 1)
            relay(1)
            for j in range(nj):
                send_down(0, j, 1)
            take(0, 2)
            for u in late:
                pass_units(0, u, 2, 3)
            take(0, 3)
            relay(2)
            pass_down(0, 0, 1)
            relay(3)
            send_down(0, 0, 2, 3)
        elif me == 1:
            send_units(1, 0, late)
            for j in range(nj):
                send_down(1, j, 0)
            for u in range(nu):
                pass_units(1, u, 0)
            relay(1)
            pass_units(1, 0, 2, 3)
            take(1, 0)
            take(1, 2)
            relay(0)
            take(1, 3)
            relay(2)
            for j in range(nj):
                send_down(1, j, 2, 3)
            pass_units(1, 1, 2)
            relay(3)
            pass_units(1, 1, 3)
            for u in range(2, nu):
                pass_units(1, u, 2, 3)
        elif me == 2:
            send_units(2, 0, late)
            send_units(2, 3, range(last))
            for u in early:
                pass_units(2, u, 3)
            relay(2)
            take(2, 0)
            send_units(2, 3, late)
            take(2, 1)
            pass_units(2, 0, 0)
            relay(0)
            send_units(2, 1, range(1, nu))
            pass_units(2, 1, 0)
            relay(1)
            for u in late:
                pass_units(2, u, 0, 3)
            pass_units(2, 0, 1)
            take(2, 3)
            send_down(2, 0, 0, 1)
            pass_units(2, 1, 1)
            relay(3)
            send_down(2, 0, 3)
            for j in range(1, nj):
                send_down(2, j, 3)
        else:
            send_units(3, 2, late)
            send_units(3, 0, late)
            relay(3)
            take(3, 2)
            pass_units(3, 0, 2, 0)
            pass_units(3, 1, 2, 0)
            relay(2)
            send_units(3, 1, range(1, nu))
            take(3, 0)
            pass_units(3, last, 0)
            send_down(3, 0, 0, 1)
            for j in range(nj):
                send_down(3, j, 2)
            relay(0)
            pass_units(3, 0, 1)
            pass_units(3, 1, 1)
            pass_units(3, last, 2)
            take(3, 1)
            pass_units(3, last, 1)
            relay(1)
            for j in range(1, nj):
                send_down(3, j, 0, 1)

    with sc("gather"):
        on_each_s(gather)

    def between(me, u):
        if u == 0:
            if me == 2:
                for i in late:
                    pass_units(2, i, 1)
                pass_down(2, 0, 3)
            elif me == 3:
                pass_down(3, 0, 2, 1)
            elif me == 1:
                pass_down(1, 0, 0)
            else:
                pass_down(0, 0, 2)
        elif u == 1:
            if me == 2:
                for j in range(1, nj):
                    send_down(2, j, 0, 1)
                pass_down(2, 0, 1, 0)
            elif me == 3:
                pass_down(3, 0, 0)
            elif me == 1:
                pass_down(1, 0, 2, 3)
            else:
                pass_down(0, 0, 3)
        elif u == nu - 1 and me == 0:
            for j in range(1, nj):
                send_down(0, j, 2, 3)
        if (me, u) in ((0, nu - 1), (1, nu - 1), (2, nu - 1), (3, 1)):
            for j in range(1, nj):
                pass_down(me, j, me ^ 1)

    def own_units(u):
        def body(me):
            copies = locals_(me)
            for mat in range(2):
                copies[mat * nu + u].wait()

        on_each_s(body)

    def own_down(j):
        on_each_s(lambda me: locals_(me)[2 * nu + j].wait())

    def twin_units(u):
        def body(me):
            if u >= first_unit(me):
                all_of = wgu.at[u, : (ns - 1) * half_depth]
                remote(all_of, all_of, wy_send, wy_recv.at[u], grp=1 - g).wait_recv()

        on_each_s(body)

    def twin_down(j):
        def body(me):
            all_of = wd.at[j, : (ns - 1) * ((chunk - first_unit(me) * UNIT) // 2) // ns]
            remote(all_of, all_of, dy_send, dy_recv.at[j], grp=1 - g).wait_recv()

        on_each_s(body)

    final = ns - 1 - 2 * (s // (ns - 1))

    def hide(u, low, high):
        def block(i):
            k = jnp.where(i == ns - 1, final, i + jnp.where(i >= final, 1, 0))
            y = jnp.dot(nall[k].reshape(tok, width), wgu[u], preferred_element_type=F32)
            gate, up = y[:, :UNIT], y[:, UNIT:]
            hidden[k, :, u * UNIT : (u + 1) * UNIT] = (gate / (1.0 + jnp.exp(-gate)) * up).astype(BF16)

        def run():
            each(low, high, block)

        if (u + 1) * UNIT <= dup:
            pl.when(s < ns - 1)(run)
        else:
            run()

    def rows_in(i):
        k = jnp.where(i == ns - 1, final, i + jnp.where(i >= final, 1, 0))
        for h in range(2):
            row_c(0, k, tc, h).wait_recv()
            row_c(1, k, (tc + 2) % 4, h).wait_recv()

    with sc("rows"):
        each(0, ns - 1, rows_in)
    for u in range(nu):
        with sc(f"tw{u}"):
            own_units(u)
            twin_units(u)
        with sc(f"hide{u}"):
            hide(u, 0, ns - 1)
        with sc(f"bt{u}"):
            on_each_s(lambda me, u=u: between(me, u))
    with sc("rowl"):
        rows_in(ns - 1)
    with sc("hidel"):
        for u in range(nu):
            hide(u, ns - 1, ns)

    def pass_down_all(j):
        on_each_s(lambda me: pass_down(me, j, me ^ 2, me ^ 3))

    steps = [(0, m) for m in (3, 1, 2, 0)]
    steps += [(j, m) for m in (3, 2, 1, 0) for j in range(1, nj)]
    nd = len(steps)
    at = {step: d for d, step in enumerate(steps)}
    slot = {d: i for i, d in enumerate(d for d in range(nd) if steps[d][1])}

    def sum_c(d):
        return remote(part.at[d, :, 1 - c], crecv.at[d], rc_send, rc_recv.at[d], tp=tc)

    def sum_x(d):
        return remote(csend.at[d], xrecv.at[d], rx_send, rx_recv.at[d], tp=tx)

    def sum_near(d):
        i = slot[d]
        return remote(zsend.at[i], zrecv.at[i], rz_send, rz_recv.at[i], sp=xor(s, 1))

    def sum_on(d):
        j, m = steps[d]
        return remote(zsend.at[slot[d]], frecv.at[j], rz_send, rf_recv.at[j], sp=xor(s, m))

    middle = (s > 0) & (s < ns - 1)

    def stage_x(d):
        sum_c(d).wait_recv()
        csend[d] = (part[d, 1 - x, c].astype(F32) + crecv[d, 1 - x].astype(F32)).astype(BF16)
        sum_x(d).start()
        keep[d] = part[d, x, c].astype(F32) + crecv[d, x].astype(F32)

    def stage_z(d):
        m = steps[d][1]
        if m == 0:
            return
        sum_x(d).wait_recv()
        keep[d] = keep[d] + xrecv[d].astype(F32)

        @pl.when((m == 1) | ~middle)
        def _():
            zsend[slot[d]] = keep[d].astype(BF16)
            sum_near(d).start()

    def stage_on(d):
        j, m = steps[d]

        @pl.when(middle)
        def _():
            other = at[j, 5 - m]
            sum_near(other).wait_recv()
            zsend[slot[d]] = (keep[d] + zrecv[slot[other]].astype(F32)).astype(BF16)
            sum_on(d).start()

    def feed(d):
        j, m = steps[d]
        src = hidden[xor(s, m)]
        piece = math.gcd(wide, 512)

        def down(p):
            cols = pl.ds(pl.multiple_of(p * piece, piece), piece)
            y = jnp.dot(src, wd[j, :, cols], preferred_element_type=F32).astype(BF16)
            part[d, :, :, :, cols] = y.reshape(2, 2, rows, piece)

        each(0, wide // piece, down)
        sum_c(d).start()

    def finish(j):
        d, near = at[j, 0], at[j, 1]
        sum_x(d).wait_recv()
        sum_near(near).wait_recv()
        remote(frecv.at[j], frecv.at[j], rz_send, rf_recv.at[j], sp=xor(s, 1)).wait_recv()
        total = (
            keep[d] + xrecv[d].astype(F32) + zrecv[slot[near]].astype(F32) + frecv[j].astype(F32)
        )
        for p in range(ns):
            cols = slice(p * depth + j * dj, p * depth + (j + 1) * dj)
            out_ref[:, cols] = (resid[:, cols] + total[:, p * dj : (p + 1) * dj]).astype(BF16)

    def on_time(i):
        j, m = steps[i]
        return {2: at[j, 2] + 4, 3: at[j, 2] + 7}.get(m, -1)

    ready = set()
    for d in range(nd):
        j = steps[d][0]
        if j not in ready:
            ready.add(j)
            with sc(f"td{j}"):
                own_down(j)
                twin_down(j)
        with sc(f"f{d}"):
            feed(d)
            if d >= 1:
                stage_x(d - 1)
        ahead = d - 1 if 2 <= d <= nj else nj
        if ahead < nj:
            with sc(f"pd{ahead}"):
                pass_down_all(ahead)
        for i in range(nd):
            if d == i + 4:
                with sc(f"z{i}"):
                    stage_z(i)
        for i in range(nd):
            if d == on_time(i):
                with sc(f"o{i}"):
                    stage_on(i)
    with sc("st"):
        stage_x(nd - 1)
        for d in range(nd, nd + 4):
            stage_z(d - 4)
            for i in range(nd):
                if d == on_time(i):
                    stage_on(i)
    for j in range(nj):
        with sc(f"fin{j}"):
            finish(j)

    def drain(me):
        if me + 1 < ns:
            for kind, buf in enumerate((kbuf, vbuf)):
                sent = buf.at[: me + 1]
                remote(sent, sent, kv_send.at[kind], kv_recv.at[kind, 0], tp=tx).wait_send()
        sent = nall.at[0, : 2 if me in (0, ns - 1) else 4]
        remote(sent, sent, az_send, az_recv.at[0, 0], tp=tx).wait_send()
        others = [i for i in range(ns) if i != me]
        for count, sem in (
            (sum(nu - first_unit(i) for i in others), wz_send),
            ((ns - 1) * (nu - first_unit(me)), wy_send),
        ):
            high = count * half_depth
            all_of = wgu.at[0, :high] if high <= width else wgu.at[:, : high // nu]
            remote(all_of, all_of, sem, wz_recv.at[0, me], grp=1 - g).wait_send()
        halves = [(chunk - first_unit(i) * UNIT) // 2 for i in range(ns)]
        for count, sem in (
            (sum(halves[i] for i in others), dz_send), ((ns - 1) * halves[me], dy_send)
        ):
            all_of = wd.at[:, : count // ns]
            remote(all_of, all_of, sem, dz_recv.at[0, me], grp=1 - g).wait_send()

    with sc("drain"):
        on_each_s(drain)
        remote(heads, heads, h_send, h_recv.at[0], tp=tx).wait_send()

        remote(nall.at[0], nall.at[0], ax_send, ax_recv.at[0, 0], tp=tx).wait_send()
        sent = nall.at[pl.ds(0, 2)]
        remote(sent, sent, ac_send, ac_recv.at[0, 0, 0], tp=tx).wait_send()
        remote(crecv, crecv, rc_send, rc_recv.at[0], tp=tc).wait_send()
        remote(xrecv, xrecv, rx_send, rx_recv.at[0], tp=tx).wait_send()
        remote(zrecv, zrecv, rz_send, rz_recv.at[0], tp=tx).wait_send()


def fused(ns, nt, chunk, nj, resid_in, queries, keys, values, cum_gate, w_out, norm_gain, w_gate, w_up, w_down):
    rows, width = resid_in.shape
    tok, att_w = queries.shape
    depth, units = w_gate.shape
    nheads = att_w // HEAD_DIM
    nu, nd, wide = chunk // UNIT, 4 * nj, width // nj
    vm = pl.BlockSpec(memory_space=pltpu.VMEM)
    hbm = pl.BlockSpec(memory_space=pltpu.HBM)
    dma = pltpu.SemaphoreType.DMA
    return pl.pallas_call(
        functools.partial(layer_kernel, (ns, nt, chunk, nj)),
        out_shape=jax.ShapeDtypeStruct((rows, width), BF16),
        in_specs=[hbm] * 10,
        out_specs=vm,
        scratch_shapes=[
            pltpu.VMEM((rows, width), BF16),
            pltpu.VMEM((tok, att_w), BF16),
            pltpu.VMEM((tok, att_w), BF16),
            pltpu.VMEM((tok, att_w), BF16),
            pltpu.VMEM(cum_gate.shape[::-1], F32),
            pltpu.VMEM((1, width), F32),
            pltpu.VMEM((ns - 1, tok, att_w), BF16),
            pltpu.VMEM((ns - 1, tok, att_w), BF16),
            pltpu.VMEM((nheads, tok, 1), F32),
            pltpu.VMEM((nheads, tok, 1), F32),
            pltpu.VMEM((nheads, tok, HEAD_DIM), F32),
            pltpu.VMEM((tok, att_w), BF16),
            pltpu.VMEM((nt - 1, rows, att_w), BF16),
            pltpu.VMEM(w_out.shape, BF16),
            pltpu.VMEM((rows, width), F32),
            pltpu.VMEM((ns, nt, rows, width), BF16),
            pltpu.VMEM((nu, width, 2 * UNIT), BF16),
            pltpu.VMEM((nj, chunk, wide), BF16),
            pltpu.VMEM((ns, tok, chunk), BF16),
            pltpu.VMEM((nd, 2, 2, rows, wide), BF16),
            pltpu.VMEM((nd, 2, rows, wide), BF16),
            pltpu.VMEM((nd, rows, wide), BF16),
            pltpu.VMEM((nd, rows, wide), F32),
            pltpu.VMEM((nd, rows, wide), BF16),
            pltpu.VMEM((3 * nj, rows, wide), BF16),
            pltpu.VMEM((3 * nj, rows, wide), BF16),
            pltpu.VMEM((nj, rows, wide), BF16),
            dma((6,)),
            dma((1 + 2 * nu + nj,)),
            dma((2,)), dma((2, ns - 1)),
            dma, dma((nu + 1, ns)),
            dma, dma((nu,)),
            dma, dma((nj, ns)),
            dma, dma((nj,)),
            dma, dma((nt - 1,)),
            dma, dma((ns, 2)),
            dma, dma((ns, 2)),
            dma, dma((2, ns, 2)),
            dma, dma((nd,)),
            dma, dma((nd,)),
            dma, dma((3 * nj,)),
            dma((nj,)),
        ],
        compiler_params=pltpu.CompilerParams(
            collective_id=0, has_side_effects=True, vmem_limit_bytes=60 * 2**20
        ),
        name="layer",
    )(
        resid_in, queries, keys, values, cum_gate.T, norm_gain[None, :], w_out, w_gate,
        w_up, w_down,
    )


def pick(mesh):
    ng, ns, nt = (mesh.shape[a] for a in ("grp", "sp", "tp"))

    def step(*args):
        resid_in, queries, cum_gate, w_gate = args[0], args[1], args[4], args[7]
        rows, width = resid_in.shape
        depth, units = w_gate.shape
        chunk = -(-units // (128 * ns)) * 128
        need = 2 * ns * nt * rows * width * 4 + 6 * width * chunk + 2 * args[5].size
        fits = (
            ng == 2 and nt == 4 and ns == 4 and units % UNIT == 0 and chunk >= 2 * UNIT and depth % (128 * PIECES) == 0 and (ns - 1) * chunk < units
            and depth % 256 == 0 and width % 256 == 0 and (chunk - ns * chunk + units) % 32 == 0 and width == ns * depth and rows % 32 == 0
            and queries.shape[0] == rows * nt and queries.shape[0] % 128 == 0
            and cum_gate.shape[0] == ns * nt * rows and queries.shape[1] % 128 == 0
            and need < 40 * 2**20
        )
        if fits:
            return fused(ns, nt, chunk, PIECES, *args)
        return on_device(*args)

    return step


def solution(mesh):
    return jax.shard_map(
        pick(mesh),
        mesh=mesh,
        in_specs=(
            P(("grp", "sp", "tp"), None),
            P(("grp", "sp"), "tp"),
            P(("grp", "sp"), "tp"),
            P(("grp", "sp"), "tp"),
            P("grp", "tp"),
            P(),
            P(),
            P("sp", "tp"),
            P("sp", "tp"),
            P("tp", "sp"),
        ),
        out_specs=P(("grp", "sp", "tp"), None),
        check_vma=False,
    )
```

```python
import functools
import math

import jax
import jax.numpy as jnp
from jax import lax
from jax.experimental import pallas as pl
from jax.experimental.pallas import tpu as pltpu
from jax.sharding import PartitionSpec as P

HEAD_DIM = 64


def on_device(resid_in, queries, keys, values, cum_gate, w_out, norm_gain, w_gate, w_up, w_down):
    tok_rows = queries.shape[0]
    local_heads = queries.shape[1] // HEAD_DIM
    scale = HEAD_DIM ** (-0.5)
    offset = lax.axis_index("sp") * tok_rows
    query_heads = queries.reshape(tok_rows, local_heads, HEAD_DIM)
    own_gate = lax.dynamic_slice_in_dim(cum_gate, offset, tok_rows, 0).T
    query_pos = offset + jnp.arange(tok_rows, dtype=jnp.int32)
    last_pos = offset + tok_rows - 1
    initial = (
        jnp.full((local_heads, tok_rows), -1e30, jnp.float32),
        jnp.zeros((local_heads, tok_rows), jnp.float32),
        jnp.zeros((tok_rows, local_heads, HEAD_DIM), jnp.float32),
    )
    pair = lax.all_gather(jnp.stack([keys, values]), "sp", axis=1, tiled=True)
    key_piece, value_piece = pair[0], pair[1]
    length = key_piece.shape[0]
    span = math.gcd(length, 512)

    def block(index, state):
        begin = index * span

        def work(inner):
            maxima, totals, summed = inner
            key_block = lax.dynamic_slice_in_dim(key_piece, index * span, span, 0).reshape(
                span, local_heads, HEAD_DIM
            )
            value_block_rows = lax.dynamic_slice_in_dim(value_piece, index * span, span, 0).reshape(
                span, local_heads, HEAD_DIM
            )
            key_gate = lax.dynamic_slice_in_dim(cum_gate, begin, span, 0).T
            scores = (
                jnp.einsum(
                    "qhd,khd->hqk", query_heads, key_block, preferred_element_type=jnp.float32
                )
                * scale
            )
            scores = scores + own_gate[:, :, None] - key_gate[:, None, :]
            key_pos = begin + jnp.arange(span, dtype=jnp.int32)
            mask = (key_pos[None, :] <= query_pos[:, None])[None]
            scores = jnp.where(mask, scores, -1e30)
            new_max = jnp.maximum(maxima, jnp.max(scores, axis=-1))
            weights = jnp.where(mask, jnp.exp(scores - new_max[:, :, None]), 0.0)
            rescale = jnp.exp(maxima - new_max)
            totals = totals * rescale + jnp.sum(weights, axis=-1)
            product = jnp.einsum(
                "hqk,khd->qhd",
                weights.astype(jnp.bfloat16),
                value_block_rows,
                preferred_element_type=jnp.float32,
            )
            summed = summed * rescale.T[:, :, None] + product
            return (new_max, totals, summed)

        return lax.cond(begin <= last_pos, work, lambda inner: inner, state)

    maxima, totals, summed = lax.fori_loop(0, length // span, block, initial)
    attended = (
        (summed / totals.T[:, :, None])
        .reshape(tok_rows, local_heads * HEAD_DIM)
        .astype(jnp.bfloat16)
    )
    head_rows = lax.all_to_all(attended, "tp", split_axis=0, concat_axis=1, tiled=True)
    mixed = jnp.dot(head_rows, w_out, preferred_element_type=jnp.float32)
    resid = resid_in.astype(jnp.float32) + mixed
    normed = resid * lax.rsqrt(jnp.mean(resid * resid, axis=-1, keepdims=True) + 1e-06)
    normed = (normed * norm_gain).astype(jnp.bfloat16)
    all_rows = lax.all_gather(normed, ("sp", "tp"), axis=0, tiled=True)
    full_gate, full_up, full_down = (
        lax.all_to_all(w_gate, "sp", split_axis=1, concat_axis=0, tiled=True),
        lax.all_to_all(w_up, "sp", split_axis=1, concat_axis=0, tiled=True),
        lax.all_to_all(w_down, "sp", split_axis=0, concat_axis=1, tiled=True),
    )
    gate = jnp.dot(all_rows, full_gate, preferred_element_type=jnp.float32)
    up = jnp.dot(all_rows, full_up, preferred_element_type=jnp.float32)
    hidden = (jax.nn.silu(gate) * up).astype(jnp.bfloat16)
    terms = jnp.dot(hidden, full_down, preferred_element_type=jnp.float32)
    back = lax.psum_scatter(
        terms.astype(jnp.bfloat16), ("sp", "tp"), scatter_dimension=0, tiled=True
    ).astype(jnp.float32)
    return (resid + back).astype(jnp.bfloat16)


MESH = pl.DeviceIdType.MESH
F32 = jnp.float32
BF16 = jnp.bfloat16
UNIT = 128
PIECES = 4


def layer_kernel(
    dims, resid_hbm, q_hbm, k_hbm, v_hbm, gate_t_hbm, gain_hbm, w_out_ref, w_gate_ref,
    w_up_ref, w_down_ref, out_ref, resid_ref, q_ref, k_ref, v_ref, gate_t_ref, gain_ref, kbuf, vbuf, top, tot, acc, att, heads, w_out, resid, nall, wgu,
    wd, hidden, part, crecv, csend, keep, xrecv, zsend, zrecv, frecv, in_sem, loc_sem, kv_send, kv_recv, wz_send,
    wz_recv, wy_send, wy_recv, dz_send, dz_recv, dy_send, dy_recv, h_send, h_recv, az_send, az_recv,
    ax_send, ax_recv, ac_send, ac_recv, rc_send, rc_recv, rx_send, rx_recv, rz_send, rz_recv,
    rf_recv,
):
    ns, nt, chunk, nj = dims
    g, s, t = lax.axis_index("grp"), lax.axis_index("sp"), lax.axis_index("tp")
    rows, width = resid_hbm.shape
    tok, att_w = q_hbm.shape
    depth, units = w_gate_ref.shape
    nheads = att_w // HEAD_DIM
    half_depth = depth // 2
    dup = ns * chunk - units
    nu, dj = chunk // UNIT, depth // nj
    wide = ns * dj
    x, c = t // 2, t % 2
    tx = (t + 2) % 4
    tc = t + 1 - 2 * c
    scale = HEAD_DIM ** (-0.5)
    sc = jax.named_scope

    def start_of(i):
        return min(i * chunk, units - chunk)

    def first_unit(i):
        return dup // UNIT if i == ns - 1 else 0

    def remote(src, dst, send, recv, **where):
        return pltpu.make_async_remote_copy(
            src_ref=src, dst_ref=dst, send_sem=send, recv_sem=recv, device_id=where,
            device_id_type=MESH,
        )

    def xor(a, b):
        hi, lo, bh, bl = a // 2, a % 2, b // 2, b % 2
        return 2 * (hi + bh - 2 * hi * bh) + lo + bl - 2 * lo * bl

    def on_each_s(body):
        for k in range(ns):
            pl.when(s == k)(lambda k=k: (body(k), None)[1])

    def each(low, high, body):
        lax.fori_loop(low, high, lambda i, z: (body(i), z)[1], 0)

    def unit_band(src, half):
        return pl.ds(pl.multiple_of(src * depth + half * half_depth, half_depth), half_depth)

    def unit_z(mat, u, me, dst):
        src = (w_gate_ref, w_up_ref)[mat].at[
            pl.ds(pl.multiple_of(g * half_depth, half_depth), half_depth),
            pl.ds(start_of(dst) + u * UNIT, UNIT),
        ]
        return remote(
            src, wgu.at[u, unit_band(me, g), pl.ds(mat * UNIT, UNIT)],
            wz_send, wz_recv.at[u + (mat if u == nu - 1 else 0), me], sp=dst,
        )

    def unit_parts(u):
        return ((0, 0, UNIT), (1, UNIT, UNIT)) if u == nu - 1 else ((0, 0, 2 * UNIT),)

    def unit_in(u, src, part):
        i, low, size = part
        block = wgu.at[u, unit_band(src, g), pl.ds(low, size)]
        return remote(block, block, wz_send, wz_recv.at[u + i, src], sp=src)

    def unit_y(u, src, part):
        _, low, size = part
        block = wgu.at[u, unit_band(src, g), pl.ds(low, size)]
        return remote(block, block, wy_send, wy_recv.at[u], grp=1 - g)

    def send_units(me, dst, us):
        for u in us:
            if u >= first_unit(dst):
                for mat in range(2):
                    unit_z(mat, u, me, dst).start()

    def pass_units(me, u, *srcs):
        if u >= first_unit(me):
            for src in srcs:
                with sc(f"y{u}.{src}"):
                    for part in unit_parts(u):
                        unit_in(u, src, part).wait_recv()
                        unit_y(u, src, part).start()

    def down_band(j, src, half, me):
        skip = first_unit(me) * UNIT
        size = (chunk - skip) // 2
        return wd.at[
            j, pl.ds(pl.multiple_of(skip + half * size, math.gcd(128, size)), size),
            pl.ds(src * dj, dj),
        ]

    def down_z(j, me, dst):
        skip = first_unit(dst) * UNIT
        size = (chunk - skip) // 2
        src = w_down_ref.at[
            pl.ds(pl.multiple_of(start_of(dst) + skip + g * size, math.gcd(128, size)), size),
            pl.ds(j * dj, dj),
        ]
        return remote(
            src, down_band(j, me, g, dst), dz_send, dz_recv.at[j, me], sp=dst
        )

    def down_y(j, src, half, me):
        block = down_band(j, src, half, me)
        return remote(block, block, dy_send, dy_recv.at[j], grp=1 - g)

    def send_down(me, j, *dsts):
        for dst in dsts:
            down_z(j, me, dst).start()

    def pass_down(me, j, *srcs):
        for src in srcs:
            block = down_band(j, src, g, me)
            with sc(f"d{j}.{src}"):
                remote(block, block, dz_send, dz_recv.at[j, src], sp=src).wait_recv()
            down_y(j, src, g, me).start()

    inputs = [
        pltpu.make_async_copy(src, dst, in_sem.at[i])
        for i, (src, dst) in enumerate((
            (k_hbm, k_ref), (v_hbm, v_ref), (q_hbm, q_ref), (gate_t_hbm, gate_t_ref),
            (gain_hbm, gain_ref), (resid_hbm, resid_ref),
        ))
    ]
    for copy in inputs:
        copy.start()
    barrier = pltpu.get_barrier_semaphore()

    def greet(i):
        pl.semaphore_signal(barrier, inc=1, device_id={"sp": i}, device_id_type=MESH)

    each(0, s, greet)
    each(s + 1, ns, greet)
    pl.semaphore_signal(barrier, inc=1, device_id={"grp": 1 - g}, device_id_type=MESH)
    for j in range(1, nt):
        pl.semaphore_signal(barrier, inc=1, device_id={"tp": (t + j) % nt}, device_id_type=MESH)
    with sc("bar"):
        pl.semaphore_wait(barrier, ns + nt - 1)
        for copy in inputs[:4]:
            copy.wait()

    def kv_out(i, kk, vv):
        return (
            remote(kk, kbuf.at[i], kv_send.at[0], kv_recv.at[0, i], sp=s + 1),
            remote(vv, vbuf.at[i], kv_send.at[1], kv_recv.at[1, i], sp=s + 1),
        )

    def kv_in(i):
        return (
            remote(kbuf.at[i], kbuf.at[i], kv_send.at[0], kv_recv.at[0, i], sp=s - 1),
            remote(vbuf.at[i], vbuf.at[i], kv_send.at[1], kv_recv.at[1, i], sp=s - 1),
        )

    @pl.when(s + 1 < ns)
    def _():
        for copy in kv_out(0, k_ref, v_ref):
            copy.start()

    w_out_copy = pltpu.make_async_copy(w_out_ref, w_out, loc_sem.at[0])
    w_out_copy.start()

    def locals_(me):
        own = pl.ds(me * depth, depth)
        copies = []
        for mat in range(2):
            for u in range(nu):
                copies.append(
                    pltpu.make_async_copy(
                        (w_gate_ref, w_up_ref)[mat].at[:, pl.ds(start_of(me) + u * UNIT, UNIT)],
                        wgu.at[u, own, pl.ds(mat * UNIT, UNIT)], loc_sem.at[1 + 2 * u + mat],
                    )
                )
        for j in range(nj):
            copies.append(
                pltpu.make_async_copy(
                    w_down_ref.at[pl.ds(start_of(me), chunk), pl.ds(j * dj, dj)],
                    wd.at[j, :, pl.ds(me * dj, dj)], loc_sem.at[1 + 2 * nu + j],
                )
            )
        return copies

    early = range(nu - 1)
    late = range(nu - 1, nu)

    def opening(me):
        for u in early:
            for dst in range(me - 1, -1, -1):
                if u == 0 or dst != 1:
                    send_units(me, dst, (u,))
        if me == 0:
            send_units(0, 1, range(nu))
        for copy in locals_(me):
            copy.start()

    on_each_s(opening)

    if dup:

        @pl.when(s == ns - 1)
        def _():
            for j in range(nj):
                wd[j, :dup, : (ns - 1) * dj] = jnp.zeros((dup, (ns - 1) * dj), BF16)
            for k in range(ns):
                hidden[k, :, :dup] = jnp.zeros((tok, dup), BF16)

    gate_own = gate_t_ref[:, pl.ds(pl.multiple_of(s * tok, tok), tok)].T

    def attend(src, kk, vv, first):
        for h in range(nheads):
            lanes = slice(h * HEAD_DIM, (h + 1) * HEAD_DIM)
            scores = lax.dot_general(
                q_ref[:, lanes], kk[:, lanes], (((1,), (1,)), ((), ())), preferred_element_type=F32
            )
            key_gate = gate_t_ref[h : h + 1, pl.ds(pl.multiple_of(src * tok, tok), tok)]
            scores = scores * scale + gate_own[:, h : h + 1] - key_gate
            if first:
                row = lax.broadcasted_iota(jnp.int32, (tok, tok), 0)
                col = lax.broadcasted_iota(jnp.int32, (tok, tok), 1)
                scores = jnp.where(col <= row, scores, -1e30)
                new = jnp.max(scores, axis=-1, keepdims=True)
                w = jnp.where(col <= row, jnp.exp(scores - new), 0.0)
                tot[h] = jnp.sum(w, axis=-1, keepdims=True)
                acc[h] = jnp.dot(w.astype(BF16), vv[:, lanes], preferred_element_type=F32)
            else:
                old = top[h]
                new = jnp.maximum(old, jnp.max(scores, axis=-1, keepdims=True))
                w = jnp.exp(scores - new)
                shrink = jnp.exp(old - new)
                tot[h] = tot[h] * shrink + jnp.sum(w, axis=-1, keepdims=True)
                acc[h] = acc[h] * shrink + jnp.dot(
                    w.astype(BF16), vv[:, lanes], preferred_element_type=F32
                )
            top[h] = new

    with sc("att0"):
        attend(s, k_ref, v_ref, True)

    def earlier(i):
        for copy in kv_in(i - 1):
            copy.wait_recv()

        @pl.when(s + 1 < ns)
        def _():
            for copy in kv_out(i, kbuf.at[i - 1], vbuf.at[i - 1]):
                copy.start()

        attend(s - i, kbuf.at[i - 1], vbuf.at[i - 1], False)

    with sc("earlier"):
        each(1, s + 1, earlier)

    for h in range(nheads):
        att[:, h * HEAD_DIM : (h + 1) * HEAD_DIM] = (acc[h] / tot[h]).astype(BF16)

    def head_copy(j):
        dst = (t + j) % nt
        return remote(
            att.at[pl.ds(pl.multiple_of(dst * rows, rows), rows)], heads.at[j - 1],
            h_send, h_recv.at[j - 1], tp=dst,
        )

    for j in range(1, nt):
        head_copy(j).start()

    with sc("mix"):
        w_out_copy.wait()
        for copy in inputs[4:]:
            copy.wait()
        resid[...] = resid_ref[...].astype(F32) + jnp.dot(
            att[pl.ds(pl.multiple_of(t * rows, rows), rows), :],
            w_out[pl.ds(pl.multiple_of(t * att_w, att_w), att_w), :], preferred_element_type=F32,
        )

        def mix(j):
            head_copy(j).wait_recv()
            src = (t + nt - j) % nt
            resid[...] += jnp.dot(
                heads[j - 1], w_out[pl.ds(pl.multiple_of(src * att_w, att_w), att_w), :],
                preferred_element_type=F32,
            )

        each(1, nt, mix)
        full = resid[...]
        normed = full * lax.rsqrt(jnp.mean(full * full, axis=-1, keepdims=True) + 1e-06)
        nall[s, t] = (normed * gain_ref[...]).astype(BF16)

    part_rows = rows // 2

    def half_of(src, who, h):
        return nall.at[src, who, pl.ds(h * part_rows, part_rows)]

    def row_z(src, to, h):
        block = half_of(src, t, h)
        return remote(block, block, az_send, az_recv.at[src, h], sp=to)

    def row_x(src, who, h):
        block = half_of(src, who, h)
        return remote(block, block, ax_send, ax_recv.at[src, h], tp=tx)

    def row_c(src, who, h):
        block = half_of(src, who, h)
        return remote(block, block, ac_send, ac_recv.at[src], tp=tc)

    def spread(src, h):
        row_x(src, t, h).start()
        row_c(src, t, h).start()

    def relay(src):
        for h in range(2):
            row_x(src, tx, h).wait_recv()
            row_c(src, tx, h).start()

    def take(me, src):
        for h in range(2):
            with sc(f"take{src}.{h}"):
                row_z(src, me, h).wait_recv()
            if (me, src // 2) in ((1, 1), (2, 0)):
                row_z(src, me ^ 1, h).start()
            spread(src, h)

    def gather(me):
        near, mid = me ^ 1, 2 if me < 2 else 1
        for h in range(2):
            row_z(me, mid, h).start()
        for h in range(2):
            row_z(me, near, h).start()
            spread(me, h)
        last = nu - 1
        if me < 2:
            for u in range(nu):
                send_units(me, 2, (u,))
                send_units(me, 3, (u,))
        if me == 0:
            relay(0)
            for u in early:
                pass_units(0, u, 1, 2, 3)
            for u in late:
                pass_units(0, u, 1)
            take(0, 1)
            relay(1)
            for j in range(nj):
                send_down(0, j, 1)
            take(0, 2)
            for u in late:
                pass_units(0, u, 2, 3)
            take(0, 3)
            relay(2)
            pass_down(0, 0, 1)
            relay(3)
            send_down(0, 0, 2, 3)
        elif me == 1:
            send_units(1, 0, late)
            for j in range(nj):
                send_down(1, j, 0)
            for u in range(nu):
                pass_units(1, u, 0)
            relay(1)
            pass_units(1, 0, 2, 3)
            take(1, 0)
            take(1, 2)
            relay(0)
            take(1, 3)
            relay(2)
            for j in range(nj):
                send_down(1, j, 2, 3)
            pass_units(1, 1, 2)
            relay(3)
            pass_units(1, 1, 3)
            for u in range(2, nu):
                pass_units(1, u, 2, 3)
        elif me == 2:
            send_units(2, 0, late)
            send_units(2, 3, range(last))
            for u in early:
                pass_units(2, u, 3)
            relay(2)
            take(2, 0)
            send_units(2, 3, late)
            take(2, 1)
            pass_units(2, 0, 0)
            relay(0)
            send_units(2, 1, range(1, nu))
            pass_units(2, 1, 0)
            relay(1)
            for u in late:
                pass_units(2, u, 0, 3)
            pass_units(2, 0, 1)
            take(2, 3)
            send_down(2, 0, 0, 1)
            pass_units(2, 1, 1)
            relay(3)
            send_down(2, 0, 3)
            for j in range(1, nj):
                send_down(2, j, 3)
        else:
            send_units(3, 2, late)
            send_units(3, 0, late)
            relay(3)
            take(3, 2)
            pass_units(3, 0, 2, 0)
            pass_units(3, 1, 2, 0)
            relay(2)
            send_units(3, 1, range(1, nu))
            take(3, 0)
            pass_units(3, last, 0)
            send_down(3, 0, 0, 1)
            for j in range(nj):
                send_down(3, j, 2)
            relay(0)
            pass_units(3, 0, 1)
            pass_units(3, 1, 1)
            pass_units(3, last, 2)
            take(3, 1)
            pass_units(3, last, 1)
            relay(1)
            for j in range(1, nj):
                send_down(3, j, 0, 1)

    with sc("gather"):
        on_each_s(gather)

    def between(me, u):
        if u == 0:
            if me == 2:
                for i in late:
                    pass_units(2, i, 1)
                pass_down(2, 0, 3)
            elif me == 3:
                pass_down(3, 0, 2, 1)
            elif me == 1:
                pass_down(1, 0, 0)
            else:
                pass_down(0, 0, 2)
        elif u == 1:
            if me == 2:
                for j in range(1, nj):
                    send_down(2, j, 0, 1)
                pass_down(2, 0, 1, 0)
            elif me == 3:
                pass_down(3, 0, 0)
            elif me == 1:
                pass_down(1, 0, 2, 3)
            else:
                pass_down(0, 0, 3)
        elif u == nu - 1 and me == 0:
            for j in range(1, nj):
                send_down(0, j, 2, 3)
        if (me, u) in ((0, nu - 1), (1, nu - 1), (2, nu - 1), (3, 1)):
            for j in range(1, nj):
                pass_down(me, j, me ^ 1)

    def own_units(u):
        def body(me):
            copies = locals_(me)
            for mat in range(2):
                copies[mat * nu + u].wait()

        on_each_s(body)

    def own_down(j):
        on_each_s(lambda me: locals_(me)[2 * nu + j].wait())

    def twin_units(u):
        def body(me):
            if u >= first_unit(me):
                all_of = wgu.at[u, : (ns - 1) * half_depth]
                remote(all_of, all_of, wy_send, wy_recv.at[u], grp=1 - g).wait_recv()

        on_each_s(body)

    def twin_down(j):
        def body(me):
            all_of = wd.at[j, : (ns - 1) * ((chunk - first_unit(me) * UNIT) // 2) // ns]
            remote(all_of, all_of, dy_send, dy_recv.at[j], grp=1 - g).wait_recv()

        on_each_s(body)

    final = ns - 1 - 2 * (s // (ns - 1))

    def hide(u, low, high):
        def block(i):
            k = jnp.where(i == ns - 1, final, i + jnp.where(i >= final, 1, 0))
            y = jnp.dot(nall[k].reshape(tok, width), wgu[u], preferred_element_type=F32)
            gate, up = y[:, :UNIT], y[:, UNIT:]
            hidden[k, :, u * UNIT : (u + 1) * UNIT] = (gate / (1.0 + jnp.exp(-gate)) * up).astype(BF16)

        def run():
            each(low, high, block)

        if (u + 1) * UNIT <= dup:
            pl.when(s < ns - 1)(run)
        else:
            run()

    def rows_in(i):
        k = jnp.where(i == ns - 1, final, i + jnp.where(i >= final, 1, 0))
        both = nall.at[k, pl.ds(0, 2)]
        remote(both, both, ac_send, ac_recv.at[k], tp=tc).wait_recv()

    with sc("rows"):
        each(0, ns - 1, rows_in)
    for u in range(nu):
        with sc(f"tw{u}"):
            own_units(u)
            twin_units(u)
        with sc(f"hide{u}"):
            hide(u, 0, ns - 1)
        with sc(f"bt{u}"):
            on_each_s(lambda me, u=u: between(me, u))
    with sc("rowl"):
        rows_in(ns - 1)
    with sc("hidel"):
        for u in range(nu):
            hide(u, ns - 1, ns)

    def pass_down_all(j):
        on_each_s(lambda me: pass_down(me, j, me ^ 2, me ^ 3))

    steps = [(0, m) for m in (3, 1, 2, 0)]
    steps += [(j, m) for m in (3, 2, 1, 0) for j in range(1, nj)]
    nd = len(steps)
    at = {step: d for d, step in enumerate(steps)}
    slot = {d: i for i, d in enumerate(d for d in range(nd) if steps[d][1])}

    def sum_c(d):
        return remote(part.at[d, :, 1 - c], crecv.at[d], rc_send, rc_recv.at[d], tp=tc)

    def sum_x(d):
        return remote(csend.at[d], xrecv.at[d], rx_send, rx_recv.at[d], tp=tx)

    def sum_near(d):
        i = slot[d]
        return remote(zsend.at[i], zrecv.at[i], rz_send, rz_recv.at[i], sp=xor(s, 1))

    def sum_on(d):
        j, m = steps[d]
        return remote(zsend.at[slot[d]], frecv.at[j], rz_send, rf_recv.at[j], sp=xor(s, m))

    middle = (s > 0) & (s < ns - 1)

    def stage_x(d):
        sum_c(d).wait_recv()
        csend[d] = (part[d, 1 - x, c].astype(F32) + crecv[d, 1 - x].astype(F32)).astype(BF16)
        sum_x(d).start()
        keep[d] = part[d, x, c].astype(F32) + crecv[d, x].astype(F32)

    def stage_z(d):
        m = steps[d][1]
        if m == 0:
            return
        sum_x(d).wait_recv()
        keep[d] = keep[d] + xrecv[d].astype(F32)

        @pl.when((m == 1) | ~middle)
        def _():
            zsend[slot[d]] = keep[d].astype(BF16)
            sum_near(d).start()

    def stage_on(d):
        j, m = steps[d]

        @pl.when(middle)
        def _():
            other = at[j, 5 - m]
            sum_near(other).wait_recv()
            zsend[slot[d]] = (keep[d] + zrecv[slot[other]].astype(F32)).astype(BF16)
            sum_on(d).start()

    def feed(d):
        j, m = steps[d]
        src = hidden[xor(s, m)]
        piece = math.gcd(wide, 512)

        def down(p):
            cols = pl.ds(pl.multiple_of(p * piece, piece), piece)
            y = jnp.dot(src, wd[j, :, cols], preferred_element_type=F32).astype(BF16)
            part[d, :, :, :, cols] = y.reshape(2, 2, rows, piece)

        each(0, wide // piece, down)
        sum_c(d).start()

    def finish(j):
        d, near = at[j, 0], at[j, 1]
        sum_x(d).wait_recv()
        sum_near(near).wait_recv()
        remote(frecv.at[j], frecv.at[j], rz_send, rf_recv.at[j], sp=xor(s, 1)).wait_recv()
        total = (
            keep[d] + xrecv[d].astype(F32) + zrecv[slot[near]].astype(F32) + frecv[j].astype(F32)
        )
        for p in range(ns):
            cols = slice(p * depth + j * dj, p * depth + (j + 1) * dj)
            out_ref[:, cols] = (resid[:, cols] + total[:, p * dj : (p + 1) * dj]).astype(BF16)

    def on_time(i):
        j, m = steps[i]
        return {2: at[j, 2] + 4, 3: at[j, 2] + 7}.get(m, -1)

    ready = set()
    for d in range(nd):
        j = steps[d][0]
        if j not in ready:
            ready.add(j)
            with sc(f"td{j}"):
                own_down(j)
                twin_down(j)
        with sc(f"f{d}"):
            feed(d)
            if d >= 1:
                stage_x(d - 1)
        ahead = d - 1 if 2 <= d <= nj else nj
        if ahead < nj:
            with sc(f"pd{ahead}"):
                pass_down_all(ahead)
        for i in range(nd):
            if d == i + 4:
                with sc(f"z{i}"):
                    stage_z(i)
        for i in range(nd):
            if d == on_time(i):
                with sc(f"o{i}"):
                    stage_on(i)
    with sc("st"):
        stage_x(nd - 1)
        for d in range(nd, nd + 4):
            stage_z(d - 4)
            for i in range(nd):
                if d == on_time(i):
                    stage_on(i)
    for j in range(nj):
        with sc(f"fin{j}"):
            finish(j)

    def drain(me):
        if me + 1 < ns:
            for kind, buf in enumerate((kbuf, vbuf)):
                sent = buf.at[: me + 1]
                remote(sent, sent, kv_send.at[kind], kv_recv.at[kind, 0], tp=tx).wait_send()
        sent = nall.at[0, : 2 if me in (0, ns - 1) else 4]
        remote(sent, sent, az_send, az_recv.at[0, 0], tp=tx).wait_send()
        others = [i for i in range(ns) if i != me]
        for count, sem in (
            (sum(nu - first_unit(i) for i in others), wz_send),
            ((ns - 1) * (nu - first_unit(me)), wy_send),
        ):
            high = count * half_depth
            all_of = wgu.at[0, :high] if high <= width else wgu.at[:, : high // nu]
            remote(all_of, all_of, sem, wz_recv.at[0, me], grp=1 - g).wait_send()
        halves = [(chunk - first_unit(i) * UNIT) // 2 for i in range(ns)]
        for count, sem in (
            (sum(halves[i] for i in others), dz_send), ((ns - 1) * halves[me], dy_send)
        ):
            all_of = wd.at[:, : count // ns]
            remote(all_of, all_of, sem, dz_recv.at[0, me], grp=1 - g).wait_send()

    with sc("drain"):
        on_each_s(drain)
        remote(heads, heads, h_send, h_recv.at[0], tp=tx).wait_send()

        remote(nall.at[0], nall.at[0], ax_send, ax_recv.at[0, 0], tp=tx).wait_send()
        sent = nall.at[pl.ds(0, 2)]
        remote(sent, sent, ac_send, ac_recv.at[0], tp=tx).wait_send()
        remote(crecv, crecv, rc_send, rc_recv.at[0], tp=tc).wait_send()
        remote(xrecv, xrecv, rx_send, rx_recv.at[0], tp=tx).wait_send()
        remote(zrecv, zrecv, rz_send, rz_recv.at[0], tp=tx).wait_send()


def fused(ns, nt, chunk, nj, resid_in, queries, keys, values, cum_gate, w_out, norm_gain, w_gate, w_up, w_down):
    rows, width = resid_in.shape
    tok, att_w = queries.shape
    depth, units = w_gate.shape
    nheads = att_w // HEAD_DIM
    nu, nd, wide = chunk // UNIT, 4 * nj, width // nj
    vm = pl.BlockSpec(memory_space=pltpu.VMEM)
    hbm = pl.BlockSpec(memory_space=pltpu.HBM)
    dma = pltpu.SemaphoreType.DMA
    return pl.pallas_call(
        functools.partial(layer_kernel, (ns, nt, chunk, nj)),
        out_shape=jax.ShapeDtypeStruct((rows, width), BF16),
        in_specs=[hbm] * 10,
        out_specs=vm,
        scratch_shapes=[
            pltpu.VMEM((rows, width), BF16),
            pltpu.VMEM((tok, att_w), BF16),
            pltpu.VMEM((tok, att_w), BF16),
            pltpu.VMEM((tok, att_w), BF16),
            pltpu.VMEM(cum_gate.shape[::-1], F32),
            pltpu.VMEM((1, width), F32),
            pltpu.VMEM((ns - 1, tok, att_w), BF16),
            pltpu.VMEM((ns - 1, tok, att_w), BF16),
            pltpu.VMEM((nheads, tok, 1), F32),
            pltpu.VMEM((nheads, tok, 1), F32),
            pltpu.VMEM((nheads, tok, HEAD_DIM), F32),
            pltpu.VMEM((tok, att_w), BF16),
            pltpu.VMEM((nt - 1, rows, att_w), BF16),
            pltpu.VMEM(w_out.shape, BF16),
            pltpu.VMEM((rows, width), F32),
            pltpu.VMEM((ns, nt, rows, width), BF16),
            pltpu.VMEM((nu, width, 2 * UNIT), BF16),
            pltpu.VMEM((nj, chunk, wide), BF16),
            pltpu.VMEM((ns, tok, chunk), BF16),
            pltpu.VMEM((nd, 2, 2, rows, wide), BF16),
            pltpu.VMEM((nd, 2, rows, wide), BF16),
            pltpu.VMEM((nd, rows, wide), BF16),
            pltpu.VMEM((nd, rows, wide), F32),
            pltpu.VMEM((nd, rows, wide), BF16),
            pltpu.VMEM((3 * nj, rows, wide), BF16),
            pltpu.VMEM((3 * nj, rows, wide), BF16),
            pltpu.VMEM((nj, rows, wide), BF16),
            dma((6,)),
            dma((1 + 2 * nu + nj,)),
            dma((2,)), dma((2, ns - 1)),
            dma, dma((nu + 1, ns)),
            dma, dma((nu,)),
            dma, dma((nj, ns)),
            dma, dma((nj,)),
            dma, dma((nt - 1,)),
            dma, dma((ns, 2)),
            dma, dma((ns, 2)),
            dma, dma((ns,)),
            dma, dma((nd,)),
            dma, dma((nd,)),
            dma, dma((3 * nj,)),
            dma((nj,)),
        ],
        compiler_params=pltpu.CompilerParams(
            collective_id=0, has_side_effects=True, vmem_limit_bytes=60 * 2**20
        ),
        name="layer",
    )(
        resid_in, queries, keys, values, cum_gate.T, norm_gain[None, :], w_out, w_gate,
        w_up, w_down,
    )


def pick(mesh):
    ng, ns, nt = (mesh.shape[a] for a in ("grp", "sp", "tp"))

    def step(*args):
        resid_in, queries, cum_gate, w_gate = args[0], args[1], args[4], args[7]
        rows, width = resid_in.shape
        depth, units = w_gate.shape
        chunk = -(-units // (128 * ns)) * 128
        need = 2 * ns * nt * rows * width * 4 + 6 * width * chunk + 2 * args[5].size
        fits = (
            ng == 2 and nt == 4 and ns == 4 and units % UNIT == 0 and chunk >= 2 * UNIT and depth % (128 * PIECES) == 0 and (ns - 1) * chunk < units
            and depth % 256 == 0 and width % 256 == 0 and (chunk - ns * chunk + units) % 32 == 0 and width == ns * depth and rows % 32 == 0
            and queries.shape[0] == rows * nt and queries.shape[0] % 128 == 0
            and cum_gate.shape[0] == ns * nt * rows and queries.shape[1] % 128 == 0
            and need < 40 * 2**20
        )
        if fits:
            return fused(ns, nt, chunk, PIECES, *args)
        return on_device(*args)

    return step


def solution(mesh):
    return jax.shard_map(
        pick(mesh),
        mesh=mesh,
        in_specs=(
            P(("grp", "sp", "tp"), None),
            P(("grp", "sp"), "tp"),
            P(("grp", "sp"), "tp"),
            P(("grp", "sp"), "tp"),
            P("grp", "tp"),
            P(),
            P(),
            P("sp", "tp"),
            P("sp", "tp"),
            P("tp", "sp"),
        ),
        out_specs=P(("grp", "sp", "tp"), None),
        check_vma=False,
    )
```
